32 devices in a mesh: row: 8 (over z, core), col: 4 (over y, x).
Axes of the slice: x: 2, y: 2, z: 4, core: 2. Of those that a mesh axis runs over, the one named last changes fastest.
Arguments:
- tokens: bfloat16 [1, 2048, 2048], P(None, 'row'), may hold values from -6 to 6
- w_value: bfloat16 [2048, 1024], P(None, 'col'), may hold values from -0.125 to 0.125
- w_first: bfloat16 [2048, 1024], P(None, 'col'), may hold values from -0.125 to 0.125
- w_second: bfloat16 [2048, 1024], P(None, 'col'), may hold values from -0.125 to 0.125
- w_gate: bfloat16 [2048, 1024], P(None, 'col'), may hold values from -0.125 to 0.125
- conv_taps: float32 [3, 3, 1024], P(None, None, 'col'), may hold values from -3.5 to 3.5
- filter_embed: float32 [33, 64], replicated, may hold values from -48 to 48
- filter_freq: float32 [64], replicated, may hold values from 0.1 to 1.9
- filter_proj: float32 [64, 2, 2, 1024], P(None, None, None, 'col'), may hold values from -0.0234375 to 0.0234375
- filter_decay: float32 [2, 2, 1024], P(None, None, 'col'), may hold values from 0.25 to 32
- skip_gain: float32 [2, 1024], P(None, 'col'), may hold values from -3 to 3
- w_out: bfloat16 [1024, 2048], P('col'), may hold values from -0.1875 to 0.1875
Outputs:
- mixed: bfloat16 [1, 2048, 2048], P(None, ('row', 'col'))
The draws below stay inside these ranges and needn't reach their ends.
All inputs are finite; a program needn't handle non-finite values.
Results may differ from the reference program's by a relative error of at most 0.018.
Values may be sent and summed in bfloat16 or wider, within the bound.
A program may use at most 64 MiB of HBM per device.

```python
import math
import jax
import jax.numpy as jnp
from jax import lax

D = 2048
C = 1024
HID = 64
EMB = 33
SEQS = 1
SEQ_LEN = 2048


def levels(stream_key, shape, pieces, low, largest):
    loudness = 1.0
    for position, parts in pieces:
        steps = jax.random.uniform(jax.random.fold_in(jax.random.fold_in(stream_key, 6), position), (parts,), jnp.float32, low / len(pieces), largest / len(pieces))
        loudness = loudness * jnp.repeat(jnp.exp(steps), shape[position] // parts).reshape((-1,) + (1,) * (len(shape) - 1 - position))
    return loudness


def gaussian(own_key, shape, scale, limit, shards=(), held_as=jnp.bfloat16):
    values = scale * jax.random.normal(own_key, shape, jnp.float32)
    if shards:
        values = values * levels(own_key, shape, shards, -0.22, 0.18)
    return jnp.clip(values, -limit, limit).astype(held_as)


def setup_inputs(seed: int = 0) -> dict:
    key_of = jax.random.split(jax.random.key(seed), 13)
    return {
        "tokens": gaussian(key_of[0], (SEQS, SEQ_LEN, D), 1.0, 6.0, ((1, 8),)),
        "w_value": gaussian(key_of[1], (D, C), D ** -0.5, 0.125, ((1, 4),)),
        "w_first": gaussian(key_of[2], (D, C), D ** -0.5, 0.125, ((1, 4),)),
        "w_second": gaussian(key_of[3], (D, C), D ** -0.5, 0.125, ((1, 4),)),
        "w_gate": gaussian(key_of[4], (D, C), D ** -0.5, 0.125, ((1, 4),)),
        "conv_taps": gaussian(key_of[5], (3, 3, C), 3 ** -0.5, 3.5, ((2, 4),), jnp.float32),
        "filter_embed": gaussian(key_of[6], (EMB, HID), (max(1, SEQ_LEN // 256)), 48.0, (), jnp.float32),
        "filter_freq": jnp.clip(1.0 + 0.18 * jax.random.normal(key_of[7], (HID,), jnp.float32), 0.1, 1.9),
        "filter_proj": gaussian(key_of[8], (HID, 2, 2, C), (HID * SEQ_LEN // 2) ** -0.5, 0.0234375, ((3, 4),), jnp.float32),
        "filter_decay": jnp.clip(jnp.exp(math.log(32.0) - 4.8520303 * jax.random.uniform(key_of[9], (2, 2, C), jnp.float32) ** levels(key_of[9], (2, 2, C), ((2, 4),), -0.2, 0.2)), 0.25, 32.0),
        "skip_gain": gaussian(key_of[10], (2, C), 0.5, 3.0, ((1, 4),), jnp.float32),
        "w_out": gaussian(key_of[11], (C, D), C ** -0.5, 0.1875, ((0, 4),)),
    }


def filter_spectra(length, filter_embed, filter_freq, filter_proj, filter_decay):
    bands = (filter_embed.shape[0] - 1) // 2
    index = jnp.arange(length, dtype=jnp.int32)
    spot = index.astype(jnp.float32) / (length - 1)
    freqs = jnp.arange(1, bands + 1, dtype=jnp.int32)
    phase = ((index[:, None] * freqs[None, :]) % length).astype(jnp.float32) * (2.0 * math.pi / length)
    features = jnp.concatenate([spot[:, None], jnp.cos(phase), jnp.sin(phase)], axis=1)
    hidden = jnp.sin(filter_freq[None, :] * jnp.dot(features, filter_embed, precision=lax.Precision.HIGHEST))
    width = filter_proj.shape[3]
    taps = jnp.dot(hidden, filter_proj.reshape(filter_proj.shape[0], 4 * width), precision=lax.Precision.HIGHEST)
    taps = taps.reshape(length, 2, 2, width) * jnp.exp(-spot[:, None, None, None] * filter_decay[None])
    spectra = []
    for order in range(2):
        ahead = taps[:, order, 0]
        behind = taps[:, order, 1]
        cycle = jnp.concatenate([ahead, jnp.zeros((1, width), jnp.float32), behind[1:][::-1]], axis=0)
        spectra.append(jnp.fft.rfft(cycle, axis=0))
    return spectra


def long_conv(signal, spectrum, gain):
    length = signal.shape[0]
    signal_spec = jnp.fft.rfft(signal, n=2 * length, axis=0)
    result = jnp.fft.irfft(signal_spec * spectrum, n=2 * length, axis=0)[:length]
    return result + gain[None, :] * signal


def one_sequence(sequence, w_value, w_first, w_second, w_gate, conv_taps, spectra, skip_gain, w_out):
    width = w_value.shape[1]
    proj = jnp.concatenate([jnp.dot(sequence, w_value, preferred_element_type=jnp.float32),
                            jnp.dot(sequence, w_first, preferred_element_type=jnp.float32),
                            jnp.dot(sequence, w_second, preferred_element_type=jnp.float32)], axis=1).astype(jnp.bfloat16)
    gate = jnp.dot(sequence, w_gate, preferred_element_type=jnp.float32).astype(jnp.bfloat16)
    padded = jnp.pad(proj, ((1, 1), (0, 0))).astype(jnp.float32)
    weights = conv_taps.reshape(3, 3 * width)
    short = padded[:-2] * weights[0] + padded[1:-1] * weights[1] + padded[2:] * weights[2]
    value = short[:, :width]
    first = short[:, width:2 * width]
    second = short[:, 2 * width:]
    inner = first * long_conv(value, spectra[0], skip_gain[0])
    outer = (second * long_conv(inner, spectra[1], skip_gain[1]) * jax.nn.silu(gate.astype(jnp.float32))).astype(jnp.bfloat16)
    return jnp.dot(outer, w_out, preferred_element_type=jnp.float32).astype(jnp.bfloat16)


def reference(tokens, w_value, w_first, w_second, w_gate, conv_taps, filter_embed, filter_freq, filter_proj, filter_decay, skip_gain, w_out):
    length = tokens.shape[1]
    spectra = filter_spectra(length, filter_embed, filter_freq, filter_proj, filter_decay)
    results = [one_sequence(tokens[number], w_value, w_first, w_second, w_gate, conv_taps, spectra, skip_gain, w_out)
               for number in range(tokens.shape[0])]
    return jnp.stack(results, axis=0)
```

```python
import functools
import math

import jax
import jax.numpy as jnp
import numpy as np
from jax import lax
from jax.experimental import pallas as pl
from jax.experimental.pallas import tpu as pltpu
from jax.sharding import PartitionSpec as P

precise = lax.Precision.HIGHEST


def padded_2(array, sides, width):
    for axis, dim in sides:
        size, length = (lax.axis_size(axis), array.shape[dim])
        up = [(i, (i + 1) % size) for i in range(size - 1)]
        down = [(j, i) for i, j in up]
        last = lax.slice_in_dim(array, length - width, length, axis=dim)
        leading = lax.slice_in_dim(array, 0, width, axis=dim)
        before = lax.ppermute(last, axis, up)
        after = lax.ppermute(leading, axis, down)
        array = jnp.concatenate([before, array, after], axis=dim)
    return array


def split_length(total):
    factor = math.isqrt(total)
    while total % factor != 0:
        factor = factor - 1
    return (factor, total // factor)


def tables(outer, inner, total):
    first_index = jnp.arange(outer, dtype=jnp.int32)
    second_index = jnp.arange(inner, dtype=jnp.int32)
    scale = 2.0 * math.pi
    outer_angle = (first_index[:, None] * first_index[None, :] % outer).astype(jnp.float32) * (
        scale / outer
    )
    inner_angle = (second_index[:, None] * second_index[None, :] % inner).astype(jnp.float32) * (
        scale / inner
    )
    twist_angle = (first_index[:, None] * second_index[None, :] % total).astype(jnp.float32) * (
        scale / total
    )
    return (
        jnp.cos(outer_angle),
        jnp.sin(outer_angle),
        jnp.cos(inner_angle),
        jnp.sin(inner_angle),
        jnp.cos(twist_angle),
        jnp.sin(twist_angle),
    )


def forward_real(signal, table):
    outer_cos, outer_sin, inner_cos, inner_sin, twist_cos, twist_sin = table
    outer = outer_cos.shape[0]
    inner = inner_cos.shape[0]
    grid = signal.reshape(signal.shape[0], outer, inner)
    real_part = jnp.einsum("kq,cqp->ckp", outer_cos, grid, precision=precise)
    imag_part = -jnp.einsum("kq,cqp->ckp", outer_sin, grid, precision=precise)
    turned_real = real_part * twist_cos + imag_part * twist_sin
    turned_imag = imag_part * twist_cos - real_part * twist_sin
    spec_real = jnp.einsum("ckp,pj->ckj", turned_real, inner_cos, precision=precise) + jnp.einsum(
        "ckp,pj->ckj", turned_imag, inner_sin, precision=precise
    )
    spec_imag = jnp.einsum("ckp,pj->ckj", turned_imag, inner_cos, precision=precise) - jnp.einsum(
        "ckp,pj->ckj", turned_real, inner_sin, precision=precise
    )
    return (spec_real, spec_imag)


def inverse_real(spec_real, spec_imag, table):
    outer_cos, outer_sin, inner_cos, inner_sin, twist_cos, twist_sin = table
    total = outer_cos.shape[0] * inner_cos.shape[0]
    back_real = jnp.einsum("ckj,jp->ckp", spec_real, inner_cos, precision=precise) - jnp.einsum(
        "ckj,jp->ckp", spec_imag, inner_sin, precision=precise
    )
    back_imag = jnp.einsum("ckj,jp->ckp", spec_real, inner_sin, precision=precise) + jnp.einsum(
        "ckj,jp->ckp", spec_imag, inner_cos, precision=precise
    )
    turned_real = back_real * twist_cos - back_imag * twist_sin
    turned_imag = back_real * twist_sin + back_imag * twist_cos
    result = jnp.einsum("qk,ckp->cqp", outer_cos, turned_real, precision=precise) - jnp.einsum(
        "qk,ckp->cqp", outer_sin, turned_imag, precision=precise
    )
    return result.reshape(result.shape[0], total) / total


def channel_filters(
    length, row_index, chan_row, filter_embed, filter_freq, filter_proj, filter_decay
):
    bands = (filter_embed.shape[0] - 1) // 2
    index = jnp.arange(length, dtype=jnp.int32)
    spot = index.astype(jnp.float32) / (length - 1)
    freqs = jnp.arange(1, bands + 1, dtype=jnp.int32)
    phase = (index[:, None] * freqs[None, :] % length).astype(jnp.float32) * (
        2.0 * math.pi / length
    )
    features = jnp.concatenate([spot[:, None], jnp.cos(phase), jnp.sin(phase)], axis=1)
    hidden = jnp.sin(filter_freq[None, :] * jnp.dot(features, filter_embed, precision=precise))
    own_proj = lax.dynamic_slice_in_dim(filter_proj, row_index * chan_row, chan_row, 3)
    own_decay = lax.dynamic_slice_in_dim(filter_decay, row_index * chan_row, chan_row, 2)
    taps = jnp.dot(hidden, own_proj.reshape(own_proj.shape[0], 4 * chan_row), precision=precise)
    taps = jnp.transpose(taps).reshape(2, 2, chan_row, length)
    taps = taps * jnp.exp(-spot[None, None, None, :] * own_decay[:, :, :, None])
    cycles = []
    for order in range(2):
        behind = jnp.flip(taps[order, 1, :, 1:], axis=1)
        cycles.append(
            jnp.concatenate([taps[order, 0], jnp.zeros((chan_row, 1), jnp.float32), behind], axis=1)
        )
    return cycles


def body(
    tokens,
    w_value,
    w_first,
    w_second,
    w_gate,
    conv_taps,
    filter_embed,
    filter_freq,
    filter_proj,
    filter_decay,
    skip_gain,
    w_out,
):
    seq_count = tokens.shape[0]
    tok_rows = tokens.shape[1]
    chan_col = w_value.shape[1]
    row_count = lax.axis_size("row")
    chan_row = chan_col // row_count
    length = tok_rows * row_count
    row_index = lax.axis_index("row")
    proj = jnp.concatenate(
        [
            jnp.dot(tokens, w_value, preferred_element_type=jnp.float32),
            jnp.dot(tokens, w_first, preferred_element_type=jnp.float32),
            jnp.dot(tokens, w_second, preferred_element_type=jnp.float32),
        ],
        axis=2,
    ).astype(jnp.bfloat16)
    gate = jnp.dot(tokens, w_gate, preferred_element_type=jnp.float32).astype(jnp.bfloat16)
    padded = padded_2(proj, (("row", 1),), 1).astype(jnp.float32)
    weights = conv_taps.reshape(3, 3 * chan_col)
    short = padded[:, :-2] * weights[0] + padded[:, 1:-1] * weights[1] + padded[:, 2:] * weights[2]
    value_rows = jnp.transpose(short[:, :, :chan_col], (0, 2, 1))
    first_rows = jnp.transpose(short[:, :, chan_col : 2 * chan_col], (0, 2, 1))
    second_rows = jnp.transpose(short[:, :, 2 * chan_col :], (0, 2, 1))
    outer, inner = split_length(2 * length)
    table = tables(outer, inner, 2 * length)
    cycles = channel_filters(
        length, row_index, chan_row, filter_embed, filter_freq, filter_proj, filter_decay
    )
    spectra = [forward_real(cycle, table) for cycle in cycles]
    own_gain = lax.dynamic_slice_in_dim(skip_gain, row_index * chan_row, chan_row, 1)

    def convolve(signal, order):
        flat = signal.reshape(seq_count * chan_row, length)
        padded_signal = jnp.concatenate([flat, jnp.zeros_like(flat)], axis=1)
        sig_real, sig_imag = forward_real(padded_signal, table)
        sig_real = sig_real.reshape(seq_count, chan_row, outer, inner)
        sig_imag = sig_imag.reshape(seq_count, chan_row, outer, inner)
        filt_real, filt_imag = spectra[order]
        prod_real = sig_real * filt_real[None] - sig_imag * filt_imag[None]
        prod_imag = sig_real * filt_imag[None] + sig_imag * filt_real[None]
        result = inverse_real(
            prod_real.reshape(seq_count * chan_row, outer, inner),
            prod_imag.reshape(seq_count * chan_row, outer, inner),
            table,
        )[:, :length]
        return result.reshape(seq_count, chan_row, length) + own_gain[order][None, :, None] * signal

    value_chan, first_chan = (
        lax.all_to_all(value_rows, "row", split_axis=1, concat_axis=2, tiled=True),
        lax.all_to_all(first_rows, "row", split_axis=1, concat_axis=2, tiled=True),
    )
    inner_chan = first_chan * convolve(value_chan, 0)
    second_conv = lax.all_to_all(
        convolve(inner_chan, 1), "row", split_axis=2, concat_axis=1, tiled=True
    )
    outer_rows = (
        jnp.transpose(second_rows * second_conv, (0, 2, 1)) * jax.nn.silu(gate.astype(jnp.float32))
    ).astype(jnp.bfloat16)
    own_rows = tok_rows // lax.axis_size("col")
    flat_rows = jnp.transpose(outer_rows, (1, 0, 2)).reshape(tok_rows * seq_count, chan_col)
    summed = lax.psum_scatter(
        jnp.dot(flat_rows, w_out, preferred_element_type=jnp.float32).astype(jnp.bfloat16),
        "col",
        scatter_dimension=0,
        tiled=True,
    ).astype(jnp.float32)
    summed = jnp.transpose(summed.reshape(own_rows, seq_count, w_out.shape[1]), (1, 0, 2))
    return summed.astype(jnp.bfloat16)


LANES = 128
PACK = 16


def dft_tables(length):
    filled = length // LANES
    outer = 2 * filled
    total = outer * LANES
    half = filled + 1
    eye = np.eye(PACK)
    q, k, p = np.arange(filled), np.arange(half), np.arange(LANES)
    inside = k[1:-1]
    angle = 2.0 * np.pi * (np.outer(k, q) % outer) / outer
    first = np.concatenate([np.kron(np.cos(angle), eye), np.kron(-np.sin(angle)[inside], eye)], axis=0)
    weight = np.where((k == 0) | (k == filled), 1.0, 2.0) / total
    last = np.concatenate(
        [
            np.kron(np.cos(angle).T * weight, eye),
            np.kron((-np.sin(angle).T * weight)[:, inside], eye),
        ],
        axis=1,
    )
    turn = 2.0 * np.pi * np.outer(k, p) / total
    twist = np.stack([np.cos(turn), np.sin(turn)])[:, :, None, :]
    twist = np.broadcast_to(twist, (2, half, 8, LANES))
    angle = 2.0 * np.pi * (np.outer(p, p) % LANES) / LANES
    cos, sin = np.cos(angle), np.sin(angle)
    ahead = np.block([[cos, -sin], [sin, cos]])
    back = np.block([[cos, sin], [-sin, cos]])
    low = lambda array: jnp.asarray(array.astype(np.float32)).astype(jnp.bfloat16)
    return low(first), low(last), jnp.asarray(twist.astype(np.float32)), low(ahead), low(back)


def split_bf16(array):
    high = array.astype(jnp.bfloat16).astype(jnp.float32)
    middle = (array - high).astype(jnp.bfloat16).astype(jnp.float32)
    low = (array - high - middle).astype(jnp.bfloat16).astype(jnp.float32)
    return high, middle, low


def host_split(array):
    low_type = jnp.bfloat16.dtype
    high = array.astype(low_type).astype(np.float64)
    middle = (array - high).astype(low_type).astype(np.float64)
    low = (array - high - middle).astype(low_type).astype(np.float64)
    return high, middle, low


def flip(value, bits):
    bit = 1
    while bit <= bits:
        if bits & bit:
            value = value + bit - 2 * bit * lax.rem(lax.div(value, bit), 2)
        bit *= 2
    return value


def mixer_kernel(
    rows, cols, width, emb,
    tokens_hbm, w_value_hbm, w_first_hbm, w_second_hbm, w_gate_hbm, w_out_hbm, conv_hbm, embed_hbm, freq_hbm,
    proj_hbm, decay_hbm, gain_hbm, features_hbm, first_hbm, last_hbm, twist_hbm, ahead_hbm, back_hbm, perm_hbm,
    out_ref,
    tokens_ref, w_refs, conv_ref, embed_ref, freq_ref, fproj_ref, decay_ref, gain_ref, features_ref, first_ref,
    last_ref, twist_ref, ahead_ref, back_ref, perm_ref,
    send, recv, spectra, taps_ref, stack_ref, coef_ref, gated, gated_in, edge_out, edge_in, piece, final, weights,
    load_sem, row_send, row_recv, edge_send, edge_recv, gate_send, gate_recv, piece_send, piece_recv,
    wide_send, wide_recv, pass_send, pass_recv, mate_send, mate_recv,
):
    my_row = lax.axis_index("row")
    my_col = lax.axis_index("col")
    mesh_id = pl.DeviceIdType.MESH
    groups = recv.shape[2]
    chans = groups * PACK
    tok_rows = tokens_ref.shape[0]
    block_q = tok_rows // LANES
    length_q = rows * block_q
    length = tok_rows * rows
    half = length_q + 1
    hid = freq_ref.shape[1]
    f32, low = jnp.float32, jnp.bfloat16

    def remote(src, dst, send_sem, recv_sem, row, col):
        return pltpu.make_async_remote_copy(
            src_ref=src, dst_ref=dst, send_sem=send_sem, recv_sem=recv_sem,
            device_id=(row, col), device_id_type=mesh_id,
        )

    barrier = pltpu.get_barrier_semaphore()
    for d in range(1, rows):
        pl.semaphore_signal(barrier, inc=1, device_id=(flip(my_row, d), my_col), device_id_type=mesh_id)
    for d in range(1, cols):
        pl.semaphore_signal(barrier, inc=1, device_id=(my_row, flip(my_col, d)), device_id_type=mesh_id)

    loads = {}
    for name, src, dst in (
        ("tokens", tokens_hbm, tokens_ref),
        ("value", w_value_hbm, w_refs.at[0]),
        ("embed", embed_hbm, embed_ref.at[pl.ds(0, emb)]),
        ("freq", freq_hbm, freq_ref),
        ("conv", conv_hbm, conv_ref),
        ("gain", gain_hbm, gain_ref),
        ("decay", decay_hbm, decay_ref),
        ("first", w_first_hbm, w_refs.at[1]),
        ("second", w_second_hbm, w_refs.at[2]),
        ("gate", w_gate_hbm, w_refs.at[3]),
        ("fproj", proj_hbm, fproj_ref),
        ("features", features_hbm, features_ref),
        ("dft_first", first_hbm, first_ref),
        ("twist", twist_hbm, twist_ref),
        ("ahead", ahead_hbm, ahead_ref),
        ("perm", perm_hbm, perm_ref),
        ("back", back_hbm, back_ref),
        ("dft_last", last_hbm, last_ref),
        ("w_out", w_out_hbm, weights.at[0]),
    ):
        loads[name] = pltpu.make_async_copy(src, dst, load_sem.at[len(loads)])
        loads[name].start()

    side = lax.rem(my_row, 2)
    mate = flip(my_row, 1)
    quarter = rows // 4
    rows_of = lambda part: pl.ds(side * (rows // 2) + part * quarter, quarter)

    def wide_copy(index, d, part):
        return remote(
            w_out_hbm.at[rows_of(part)], weights.at[d, rows_of(part)],
            wide_send.at[index], wide_recv.at[index], my_row, flip(my_col, d),
        )

    wide = {(1, 0): wide_copy(0, 1, 0), (2, 1): wide_copy(1, 2, 1), (1, 1): wide_copy(2, 1, 1), (2, 0): wide_copy(3, 2, 0)}
    passed = {
        0: remote(weights.at[1, rows_of(0)], weights.at[3, rows_of(0)], pass_send.at[0], pass_recv.at[0], my_row, flip(my_col, 2)),
        1: remote(weights.at[2, rows_of(1)], weights.at[3, rows_of(1)], pass_send.at[1], pass_recv.at[1], my_row, flip(my_col, 1)),
    }
    mates = {}
    for d in range(1, cols):
        for part in range(2):
            index = 2 * (d - 1) + part
            mates[d, part] = remote(
                weights.at[d, rows_of(part)], weights.at[d, rows_of(part)],
                mate_send.at[index], mate_recv.at[index], mate, my_col,
            )

    far_first = sorted(range(1, rows), key=lambda d: -(d & (rows // 2)))

    def row_copies(role):
        return [
            remote(
                send.at[role, flip(my_row, d)], recv.at[role, my_row],
                row_send.at[role, d - 1], row_recv.at[role, d - 1], flip(my_row, d), my_col,
            )
            for d in far_first
        ]

    def project(role):
        return jnp.dot(tokens_ref[...], w_refs[role], preferred_element_type=f32)

    def project_turned(role):
        result = project(role).T
        for q in range(block_q):
            send[role, :, :, q] = (
                result[:, q * LANES : (q + 1) * LANES].reshape(rows, groups, PACK, LANES).astype(low)
            )

    value_copies, first_copies = row_copies(0), row_copies(1)

    loads["tokens"].wait()
    loads["value"].wait()
    project_turned(0)
    pl.semaphore_wait(barrier, rows + cols - 2)
    for copy in value_copies:
        copy.start()
    wide[1, 0].start()
    wide[2, 1].start()
    recv[0, my_row] = send[0, my_row]

    loads["first"].wait()
    project_turned(1)
    for copy in first_copies:
        copy.start()
    recv[1, my_row] = send[1, my_row]

    loads["second"].wait()
    second = project(2).astype(low).astype(f32)
    edge_out[0] = jnp.broadcast_to(second[tok_rows - 1 :], edge_out.shape[1:])
    edge_out[1] = jnp.broadcast_to(second[:1], edge_out.shape[1:])
    edges = [
        remote(edge_out.at[0], edge_in.at[0], edge_send.at[0], edge_recv.at[0], lax.rem(my_row + 1, rows), my_col),
        remote(edge_out.at[1], edge_in.at[1], edge_send.at[1], edge_recv.at[1], lax.rem(my_row + rows - 1, rows), my_col),
    ]
    for copy in edges:
        copy.start()
    loads["gate"].wait()
    gate = project(3).astype(low).astype(f32)
    loads["conv"].wait()

    loads["gain"].wait()
    loads["decay"].wait()
    stack_ref[...] = jnp.zeros_like(stack_ref)
    for j in range(3):
        stack_ref[j : j + 1] = conv_ref[j, 0:1]
        stack_ref[3 + j : 4 + j] = conv_ref[j, 1:2]
    stack_ref[6:8] = gain_ref[...]
    stack_ref[8:10] = decay_ref[0]
    stack_ref[10:12] = decay_ref[1]
    shape = (chans, stack_ref.shape[1])
    picks = lax.broadcasted_iota(jnp.int32, shape, 1) == lax.broadcasted_iota(jnp.int32, shape, 0) + my_row * chans
    picks = jnp.where(picks, 1.0, 0.0)
    contract_last = (((1,), (1,)), ((), ()))
    own = lax.dot_general(picks, stack_ref[...], contract_last, precision=precise, preferred_element_type=f32)
    for k in range(8):
        coef_ref[k] = jnp.broadcast_to(own[:, k : k + 1], (chans, LANES)).reshape(groups, PACK, LANES)

    loads["embed"].wait()
    loads["freq"].wait()
    embed = embed_ref[...] * (freq_ref[...] * (1.0 / math.pi))
    embed = jnp.where(lax.broadcasted_iota(jnp.int32, embed.shape, 0) < emb, embed, 0.0)
    high, middle, least = split_bf16(embed)
    stacked = jnp.concatenate([high, high, middle, high, middle, least], axis=0).astype(low)
    loads["features"].wait()
    turns = lax.dot_general(stacked, features_ref[...], (((0,), (0,)), ((), ())), preferred_element_type=f32)
    whole = jnp.floor(turns + 0.5)
    rest = turns - whole
    sign = 1.0 - 2.0 * (whole - 2.0 * jnp.floor(whole * 0.5))
    square = rest * rest
    series = jnp.full_like(square, -(math.pi**11) / math.factorial(11))
    for n in (9, 7, 5, 3, 1):
        series = series * square + (-1) ** (n // 2) * math.pi**n / math.factorial(n)
    hidden = (series * (rest * sign)).astype(low)
    loads["fproj"].wait()
    pieces = []
    picks_low = picks.astype(low)
    halves = 2
    for od in range(4):
        parts = [
            fproj_ref[pl.ds((od // 2) * 2 * halves + j * 2 + od % 2, hid, stride=4 * halves), :]
            for j in range(halves)
        ]
        block = jnp.concatenate(parts, axis=1).astype(low)
        pieces.append(lax.dot_general(picks_low, block, contract_last, preferred_element_type=f32).astype(low))
    taps = jnp.dot(jnp.concatenate(pieces, axis=0), hidden, preferred_element_type=f32)
    lag = lax.broadcasted_iota(jnp.int32, (1, length), 1)
    spot = lag.astype(f32) / (length - 1)
    for od in range(4):
        block = taps[od * chans : (od + 1) * chans] * jnp.exp(-own[:, 8 + od : 9 + od] * spot)
        if od % 2 == 1:
            block = jnp.where(lag == 0, 0.0, block)
        taps_ref[od] = block.astype(low)

    def wide_twist(index):
        return twist_ref[index].reshape(half, 1, 8, LANES)

    def ahead(signal):
        mid = jnp.dot(first_ref[...], signal, preferred_element_type=f32)
        blank = jnp.zeros((PACK, LANES), f32)
        blocks = []
        for g in range(groups):
            lanes = slice(g * LANES, (g + 1) * LANES)
            real = mid[: half * PACK, lanes].reshape(half, 2, 8, LANES)
            imag = jnp.concatenate([blank, mid[half * PACK :, lanes], blank], axis=0).reshape(half, 2, 8, LANES)
            cos, sin = wide_twist(0), wide_twist(1)
            blocks.append(
                jnp.concatenate(
                    [
                        (real * cos + imag * sin).reshape(half * PACK, LANES),
                        (imag * cos - real * sin).reshape(half * PACK, LANES),
                    ],
                    axis=1,
                ).astype(low)
            )
        return jnp.dot(jnp.concatenate(blocks, axis=0), ahead_ref[...], preferred_element_type=f32)

    def convolve(signal, order):
        spec = ahead(signal.astype(low))
        real, imag = spec[:, :LANES], spec[:, LANES:]
        filt_real, filt_imag = spectra[order, 0], spectra[order, 1]
        prod = jnp.concatenate(
            [real * filt_real - imag * filt_imag, real * filt_imag + imag * filt_real], axis=1
        ).astype(low)
        mid = jnp.dot(prod, back_ref[...], preferred_element_type=f32)
        blocks = []
        for g in range(groups):
            span = slice(g * half * PACK, (g + 1) * half * PACK)
            real = mid[span, :LANES].reshape(half, 2, 8, LANES)
            imag = mid[span, LANES:].reshape(half, 2, 8, LANES)
            cos, sin = wide_twist(0), wide_twist(1)
            turned_real = (real * cos - imag * sin).reshape(half * PACK, LANES)
            turned_imag = (real * sin + imag * cos)[1:-1].reshape((half - 2) * PACK, LANES)
            blocks.append(jnp.concatenate([turned_real, turned_imag], axis=0).astype(low))
        result = jnp.dot(last_ref[...], jnp.concatenate(blocks, axis=1), preferred_element_type=f32)
        gain = jnp.concatenate([coef_ref[6 + order, g] for g in range(groups)], axis=1)
        shape = (length_q, PACK, groups * LANES)
        return (result.reshape(shape) + gain[None] * signal.reshape(shape)).reshape(signal.shape)

    loads["dft_first"].wait()
    loads["twist"].wait()
    loads["ahead"].wait()
    for order in range(2):
        for direction in range(2):
            od = 2 * order + direction
            signal = jnp.concatenate(
                [
                    jnp.concatenate(
                        [
                            taps_ref[od, g * PACK : (g + 1) * PACK, q * LANES : (q + 1) * LANES]
                            for q in range(length_q)
                        ],
                        axis=0,
                    )
                    for g in range(groups)
                ],
                axis=1,
            )
            spec = ahead(signal)
            if direction == 0:
                spectra[order, 0] = spec[:, :LANES]
                spectra[order, 1] = spec[:, LANES:]
            else:
                spectra[order, 0] += spec[:, :LANES]
                spectra[order, 1] -= spec[:, LANES:]

    for copy in edges:
        copy.wait_recv()
    line = lax.broadcasted_iota(jnp.int32, second.shape, 0)
    above = jnp.where(my_row == 0, 0.0, edge_in[0, 0:1])
    below = jnp.where(my_row == rows - 1, 0.0, edge_in[1, 0:1])
    before = jnp.where(line == 0, above, pltpu.roll(second, 1, 0))
    after = jnp.where(line == tok_rows - 1, below, pltpu.roll(second, tok_rows - 1, 0))
    short_second = before * conv_ref[0, 2:3] + second * conv_ref[1, 2:3] + after * conv_ref[2, 2:3]
    both = (short_second * (gate / (1.0 + jnp.exp(-gate)))).astype(low)
    loads["perm"].wait()
    both = jnp.dot(both, perm_ref[...], preferred_element_type=f32).astype(low)
    per_group = rows * PACK
    for g in range(groups):
        gated[:, g] = both[:, g * per_group : (g + 1) * per_group].reshape(cols, width, per_group)
    gate_copies = [
        remote(
            gated.at[flip(my_col, d)], gated_in.at[d], gate_send.at[d - 1], gate_recv.at[d - 1], my_row, flip(my_col, d)
        )
        for d in range(1, cols)
    ]
    for copy in gate_copies:
        copy.start()
    gated_in[0] = gated[my_col]
    wide[1, 1].start()
    wide[2, 0].start()

    def short(role):
        blocks = []
        for g in range(groups):
            here = recv[role, :, g].reshape(length_q * PACK, LANES).astype(f32)
            size = here.shape[0]
            lane = lax.broadcasted_iota(jnp.int32, here.shape, 1)
            blank = jnp.zeros((PACK, LANES), f32)
            before = pltpu.roll(here, 1, 1)
            before = jnp.where(lane == 0, jnp.concatenate([blank, before[: size - PACK]], axis=0), before)
            after = pltpu.roll(here, LANES - 1, 1)
            after = jnp.where(lane == LANES - 1, jnp.concatenate([after[PACK:], blank], axis=0), after)
            shape = (length_q, PACK, LANES)
            w = lambda j: coef_ref[3 * role + j, g][None]
            result = before.reshape(shape) * w(0) + here.reshape(shape) * w(1) + after.reshape(shape) * w(2)
            blocks.append(result.reshape(size, LANES))
        return jnp.concatenate(blocks, axis=1)

    loads["back"].wait()
    loads["dft_last"].wait()
    for copy in value_copies:
        copy.wait_recv()
    conv = convolve(short(0), 0)
    for copy in first_copies:
        copy.wait_recv()
    conv = convolve(short(1) * conv, 1)

    left = conv[:, :LANES].reshape(length_q, PACK, LANES)
    right = conv[:, LANES:].reshape(length_q, PACK, LANES)
    lane = lax.broadcasted_iota(jnp.int32, left.shape, 2)
    piece[:, 0] = jnp.where(lane < width, left, pltpu.roll(right, width, 2)).astype(low)
    piece[:, 1] = jnp.where(lane < width, pltpu.roll(left, width, 2), right).astype(low)
    piece_copies = []
    for dr in far_first + [0]:
        for dc in range(cols):
            if dr == 0 and dc == 0:
                continue
            row, col = flip(my_row, dr), flip(my_col, dc)
            index = dr * cols + dc - 1
            piece_copies.append(
                remote(
                    piece.at[row * block_q + lax.div(col, 2), lax.rem(col, 2)], final.at[dc, my_row],
                    piece_send.at[index], piece_recv.at[index], row, col,
                )
            )
    for copy in piece_copies:
        copy.start()
    final[0, my_row] = piece[my_row * block_q + lax.div(my_col, 2), lax.rem(my_col, 2)]

    wide[1, 0].wait_recv()
    passed[0].start()
    mates[1, 0].start()
    wide[2, 1].wait_recv()
    passed[1].start()
    mates[2, 1].start()
    wide[1, 1].wait_recv()
    mates[1, 1].start()
    wide[2, 0].wait_recv()
    mates[2, 0].start()
    for part in range(2):
        passed[part].wait_recv()
        mates[3, part].start()

    for copy in gate_copies:
        copy.wait_recv()
    for copy in piece_copies:
        copy.wait_recv()
    loads["w_out"].wait()
    picked = []
    for d in range(cols):
        outer = final[d].reshape(rows * PACK, LANES).astype(f32).T
        outer = (outer * gated_in[d].reshape(groups * width, per_group).astype(f32)).astype(low)
        for g in range(groups):
            picked.append(outer[g * width : (g + 1) * width])
    for copy in mates.values():
        copy.wait_recv()
    depth = weights.shape[4]
    full = jnp.concatenate(
        [weights[d, :, g].reshape(per_group, depth) for d in range(cols) for g in range(groups)], axis=0
    )
    out_ref[...] = jnp.dot(jnp.concatenate(picked, axis=1), full, preferred_element_type=f32).astype(low)
    for copy in value_copies + first_copies + edges + gate_copies + piece_copies:
        copy.wait_send()
    for group in (wide, passed, mates):
        for copy in group.values():
            copy.wait_send()


def fast_body(
    tokens, w_value, w_first, w_second, w_gate, conv_taps, filter_embed, filter_freq, filter_proj,
    filter_decay, skip_gain, w_out,
):
    rows, cols = lax.axis_size("row"), lax.axis_size("col")
    tok_rows = tokens.shape[1]
    chan_col = w_value.shape[1]
    chans = chan_col // rows
    groups = chans // PACK
    length = tok_rows * rows
    block_q = tok_rows // LANES
    length_q = length // LANES
    width = tok_rows // cols
    depth = w_out.shape[1]
    emb, hid = filter_embed.shape
    half = length_q + 1

    flat = tokens.reshape(tok_rows, tokens.shape[2])
    bands = (emb - 1) // 2
    index = np.arange(length)
    spot = index.astype(np.float32) / np.float32(length - 1)
    phase = 2.0 * np.pi * (np.outer(np.arange(1, bands + 1), index) % length) / length
    features = np.concatenate([spot[None, :], np.cos(phase), np.sin(phase)])
    emb_pad = -(-emb // 8) * 8
    features = np.concatenate([features, np.zeros((emb_pad - emb, length))]).astype(np.float32).astype(np.float64)
    high, middle, least = host_split(features)
    features = np.concatenate([high, middle, high, least, middle, high]).astype(jnp.bfloat16.dtype)
    own = np.arange(chan_col).reshape(rows, groups, PACK).transpose(1, 0, 2).reshape(-1)
    perm = np.zeros((chan_col, chan_col), np.float32)
    perm[own, np.arange(chan_col)] = 1.0
    lanes = chan_col // LANES
    fproj = filter_proj.reshape(hid, 2, 2, lanes, LANES).transpose(0, 1, 3, 2, 4).reshape(hid * 4 * lanes, LANES)
    w_rows = w_out.reshape(rows, groups, PACK, depth)

    first, last, twist, ahead, back = dft_tables(length)
    operands = (
        flat, w_value, w_first, w_second, w_gate, w_rows, conv_taps, filter_embed, filter_freq.reshape(1, hid),
        fproj, filter_decay, skip_gain, jnp.asarray(features), first, last, twist, ahead, back,
        jnp.asarray(perm).astype(jnp.bfloat16),
    )
    dma = pltpu.SemaphoreType.DMA
    f32, low = jnp.float32, jnp.bfloat16
    like = lambda array: pltpu.VMEM(array.shape, array.dtype)
    mixed = pl.pallas_call(
        functools.partial(mixer_kernel, rows, cols, width, emb),
        out_shape=jax.ShapeDtypeStruct((width, depth), low),
        in_specs=[pl.BlockSpec(memory_space=pl.ANY)] * len(operands),
        out_specs=pl.BlockSpec(memory_space=pltpu.VMEM),
        scratch_shapes=[
            like(flat),
            pltpu.VMEM((4,) + w_value.shape, low),
            like(conv_taps),
            pltpu.VMEM((emb_pad, hid), f32),
            pltpu.VMEM((1, hid), f32),
            like(fproj),
            like(filter_decay),
            like(skip_gain),
            pltpu.VMEM(features.shape, low),
            like(first),
            like(last),
            like(twist),
            like(ahead),
            like(back),
            pltpu.VMEM(perm.shape, low),
            pltpu.VMEM((2, rows, groups, block_q, PACK, LANES), low),
            pltpu.VMEM((2, rows, groups, block_q, PACK, LANES), low),
            pltpu.VMEM((2, 2, groups * half * PACK, LANES), f32),
            pltpu.VMEM((4, chans, length), low),
            pltpu.VMEM((16, chan_col), f32),
            pltpu.VMEM((8, groups, PACK, LANES), f32),
            pltpu.VMEM((cols, groups, width, rows * PACK), low),
            pltpu.VMEM((cols, groups, width, rows * PACK), low),
            pltpu.VMEM((2, 8, chan_col), f32),
            pltpu.VMEM((2, 8, chan_col), f32),
            pltpu.VMEM((length_q, groups, PACK, LANES), low),
            pltpu.VMEM((cols, rows, PACK, LANES), low),
            pltpu.VMEM((cols, rows, groups, PACK, depth), low),
            dma((len(operands),)),
            dma((2, rows - 1)),
            dma((2, rows - 1)),
            dma((2,)),
            dma((2,)),
            dma((cols - 1,)),
            dma((cols - 1,)),
            dma((rows * cols - 1,)),
            dma((rows * cols - 1,)),
            dma((4,)),
            dma((4,)),
            dma((2,)),
            dma((2,)),
            dma((2 * cols - 2,)),
            dma((2 * cols - 2,)),
        ],
        compiler_params=pltpu.CompilerParams(
            collective_id=0, has_side_effects=True, vmem_limit_bytes=60 * 1024 * 1024
        ),
        cost_estimate=pl.CostEstimate(flops=12_000_000_000, bytes_accessed=8_000_000, transcendentals=0),
    )(*operands)
    return mixed[None]


def shaped_body(tokens, w_value, *rest):
    rows, cols = lax.axis_size("row"), lax.axis_size("col")
    seqs, tok_rows = tokens.shape[:2]
    chan_col = w_value.shape[1]
    chans = chan_col // rows
    width = tok_rows // cols
    fits = (
        seqs == 1
        and cols == 4
        and rows == 8
        and chans == 2 * PACK
        and tok_rows % LANES == 0
        and LANES == 2 * width
        and chan_col == 2 * LANES
        and rows * PACK == LANES
    )
    return (fast_body if fits else body)(tokens, w_value, *rest)


def solution(mesh):
    in_specs = (
        P(None, "row", None),
        P(None, "col"),
        P(None, "col"),
        P(None, "col"),
        P(None, "col"),
        P(None, None, "col"),
        P(),
        P(),
        P(None, None, None, "col"),
        P(None, None, "col"),
        P(None, "col"),
        P("col", None),
    )
    out_specs = P(None, ("row", "col"), None)
    return jax.shard_map(shaped_body, mesh=mesh, in_specs=in_specs, out_specs=out_specs, check_vma=False)
```

```python
import functools
import math

import jax
import jax.numpy as jnp
import numpy as np
from jax import lax
from jax.experimental import pallas as pl
from jax.experimental.pallas import tpu as pltpu
from jax.sharding import PartitionSpec as P

precise = lax.Precision.HIGHEST


def padded_2(array, sides, width):
    for axis, dim in sides:
        size, length = (lax.axis_size(axis), array.shape[dim])
        up = [(i, (i + 1) % size) for i in range(size - 1)]
        down = [(j, i) for i, j in up]
        last = lax.slice_in_dim(array, length - width, length, axis=dim)
        leading = lax.slice_in_dim(array, 0, width, axis=dim)
        before = lax.ppermute(last, axis, up)
        after = lax.ppermute(leading, axis, down)
        array = jnp.concatenate([before, array, after], axis=dim)
    return array


def split_length(total):
    factor = math.isqrt(total)
    while total % factor != 0:
        factor = factor - 1
    return (factor, total // factor)


def tables(outer, inner, total):
    first_index = jnp.arange(outer, dtype=jnp.int32)
    second_index = jnp.arange(inner, dtype=jnp.int32)
    scale = 2.0 * math.pi
    outer_angle = (first_index[:, None] * first_index[None, :] % outer).astype(jnp.float32) * (
        scale / outer
    )
    inner_angle = (second_index[:, None] * second_index[None, :] % inner).astype(jnp.float32) * (
        scale / inner
    )
    twist_angle = (first_index[:, None] * second_index[None, :] % total).astype(jnp.float32) * (
        scale / total
    )
    return (
        jnp.cos(outer_angle),
        jnp.sin(outer_angle),
        jnp.cos(inner_angle),
        jnp.sin(inner_angle),
        jnp.cos(twist_angle),
        jnp.sin(twist_angle),
    )


def forward_real(signal, table):
    outer_cos, outer_sin, inner_cos, inner_sin, twist_cos, twist_sin = table
    outer = outer_cos.shape[0]
    inner = inner_cos.shape[0]
    grid = signal.reshape(signal.shape[0], outer, inner)
    real_part = jnp.einsum("kq,cqp->ckp", outer_cos, grid, precision=precise)
    imag_part = -jnp.einsum("kq,cqp->ckp", outer_sin, grid, precision=precise)
    turned_real = real_part * twist_cos + imag_part * twist_sin
    turned_imag = imag_part * twist_cos - real_part * twist_sin
    spec_real = jnp.einsum("ckp,pj->ckj", turned_real, inner_cos, precision=precise) + jnp.einsum(
        "ckp,pj->ckj", turned_imag, inner_sin, precision=precise
    )
    spec_imag = jnp.einsum("ckp,pj->ckj", turned_imag, inner_cos, precision=precise) - jnp.einsum(
        "ckp,pj->ckj", turned_real, inner_sin, precision=precise
    )
    return (spec_real, spec_imag)


def inverse_real(spec_real, spec_imag, table):
    outer_cos, outer_sin, inner_cos, inner_sin, twist_cos, twist_sin = table
    total = outer_cos.shape[0] * inner_cos.shape[0]
    back_real = jnp.einsum("ckj,jp->ckp", spec_real, inner_cos, precision=precise) - jnp.einsum(
        "ckj,jp->ckp", spec_imag, inner_sin, precision=precise
    )
    back_imag = jnp.einsum("ckj,jp->ckp", spec_real, inner_sin, precision=precise) + jnp.einsum(
        "ckj,jp->ckp", spec_imag, inner_cos, precision=precise
    )
    turned_real = back_real * twist_cos - back_imag * twist_sin
    turned_imag = back_real * twist_sin + back_imag * twist_cos
    result = jnp.einsum("qk,ckp->cqp", outer_cos, turned_real, precision=precise) - jnp.einsum(
        "qk,ckp->cqp", outer_sin, turned_imag, precision=precise
    )
    return result.reshape(result.shape[0], total) / total


def channel_filters(
    length, row_index, chan_row, filter_embed, filter_freq, filter_proj, filter_decay
):
    bands = (filter_embed.shape[0] - 1) // 2
    index = jnp.arange(length, dtype=jnp.int32)
    spot = index.astype(jnp.float32) / (length - 1)
    freqs = jnp.arange(1, bands + 1, dtype=jnp.int32)
    phase = (index[:, None] * freqs[None, :] % length).astype(jnp.float32) * (
        2.0 * math.pi / length
    )
    features = jnp.concatenate([spot[:, None], jnp.cos(phase), jnp.sin(phase)], axis=1)
    hidden = jnp.sin(filter_freq[None, :] * jnp.dot(features, filter_embed, precision=precise))
    own_proj = lax.dynamic_slice_in_dim(filter_proj, row_index * chan_row, chan_row, 3)
    own_decay = lax.dynamic_slice_in_dim(filter_decay, row_index * chan_row, chan_row, 2)
    taps = jnp.dot(hidden, own_proj.reshape(own_proj.shape[0], 4 * chan_row), precision=precise)
    taps = jnp.transpose(taps).reshape(2, 2, chan_row, length)
    taps = taps * jnp.exp(-spot[None, None, None, :] * own_decay[:, :, :, None])
    cycles = []
    for order in range(2):
        behind = jnp.flip(taps[order, 1, :, 1:], axis=1)
        cycles.append(
            jnp.concatenate([taps[order, 0], jnp.zeros((chan_row, 1), jnp.float32), behind], axis=1)
        )
    return cycles


def body(
    tokens,
    w_value,
    w_first,
    w_second,
    w_gate,
    conv_taps,
    filter_embed,
    filter_freq,
    filter_proj,
    filter_decay,
    skip_gain,
    w_out,
):
    seq_count = tokens.shape[0]
    tok_rows = tokens.shape[1]
    chan_col = w_value.shape[1]
    row_count = lax.axis_size("row")
    chan_row = chan_col // row_count
    length = tok_rows * row_count
    row_index = lax.axis_index("row")
    proj = jnp.concatenate(
        [
            jnp.dot(tokens, w_value, preferred_element_type=jnp.float32),
            jnp.dot(tokens, w_first, preferred_element_type=jnp.float32),
            jnp.dot(tokens, w_second, preferred_element_type=jnp.float32),
        ],
        axis=2,
    ).astype(jnp.bfloat16)
    gate = jnp.dot(tokens, w_gate, preferred_element_type=jnp.float32).astype(jnp.bfloat16)
    padded = padded_2(proj, (("row", 1),), 1).astype(jnp.float32)
    weights = conv_taps.reshape(3, 3 * chan_col)
    short = padded[:, :-2] * weights[0] + padded[:, 1:-1] * weights[1] + padded[:, 2:] * weights[2]
    value_rows = jnp.transpose(short[:, :, :chan_col], (0, 2, 1))
    first_rows = jnp.transpose(short[:, :, chan_col : 2 * chan_col], (0, 2, 1))
    second_rows = jnp.transpose(short[:, :, 2 * chan_col :], (0, 2, 1))
    outer, inner = split_length(2 * length)
    table = tables(outer, inner, 2 * length)
    cycles = channel_filters(
        length, row_index, chan_row, filter_embed, filter_freq, filter_proj, filter_decay
    )
    spectra = [forward_real(cycle, table) for cycle in cycles]
    own_gain = lax.dynamic_slice_in_dim(skip_gain, row_index * chan_row, chan_row, 1)

    def convolve(signal, order):
        flat = signal.reshape(seq_count * chan_row, length)
        padded_signal = jnp.concatenate([flat, jnp.zeros_like(flat)], axis=1)
        sig_real, sig_imag = forward_real(padded_signal, table)
        sig_real = sig_real.reshape(seq_count, chan_row, outer, inner)
        sig_imag = sig_imag.reshape(seq_count, chan_row, outer, inner)
        filt_real, filt_imag = spectra[order]
        prod_real = sig_real * filt_real[None] - sig_imag * filt_imag[None]
        prod_imag = sig_real * filt_imag[None] + sig_imag * filt_real[None]
        result = inverse_real(
            prod_real.reshape(seq_count * chan_row, outer, inner),
            prod_imag.reshape(seq_count * chan_row, outer, inner),
            table,
        )[:, :length]
        return result.reshape(seq_count, chan_row, length) + own_gain[order][None, :, None] * signal

    value_chan, first_chan = (
        lax.all_to_all(value_rows, "row", split_axis=1, concat_axis=2, tiled=True),
        lax.all_to_all(first_rows, "row", split_axis=1, concat_axis=2, tiled=True),
    )
    inner_chan = first_chan * convolve(value_chan, 0)
    second_conv = lax.all_to_all(
        convolve(inner_chan, 1), "row", split_axis=2, concat_axis=1, tiled=True
    )
    outer_rows = (
        jnp.transpose(second_rows * second_conv, (0, 2, 1)) * jax.nn.silu(gate.astype(jnp.float32))
    ).astype(jnp.bfloat16)
    own_rows = tok_rows // lax.axis_size("col")
    flat_rows = jnp.transpose(outer_rows, (1, 0, 2)).reshape(tok_rows * seq_count, chan_col)
    summed = lax.psum_scatter(
        jnp.dot(flat_rows, w_out, preferred_element_type=jnp.float32).astype(jnp.bfloat16),
        "col",
        scatter_dimension=0,
        tiled=True,
    ).astype(jnp.float32)
    summed = jnp.transpose(summed.reshape(own_rows, seq_count, w_out.shape[1]), (1, 0, 2))
    return summed.astype(jnp.bfloat16)


LANES = 128
PACK = 16


def dft_tables(length):
    filled = length // LANES
    outer = 2 * filled
    total = outer * LANES
    half = filled + 1
    eye = np.eye(PACK)
    q, k, p = np.arange(filled), np.arange(half), np.arange(LANES)
    inside = k[1:-1]
    angle = 2.0 * np.pi * (np.outer(k, q) % outer) / outer
    first = np.concatenate([np.kron(np.cos(angle), eye), np.kron(-np.sin(angle)[inside], eye)], axis=0)
    weight = np.where((k == 0) | (k == filled), 1.0, 2.0) / total
    last = np.concatenate(
        [
            np.kron(np.cos(angle).T * weight, eye),
            np.kron((-np.sin(angle).T * weight)[:, inside], eye),
        ],
        axis=1,
    )
    turn = 2.0 * np.pi * np.outer(k, p) / total
    twist = np.stack([np.cos(turn), np.sin(turn)])[:, :, None, :]
    twist = np.broadcast_to(twist, (2, half, 8, LANES))
    angle = 2.0 * np.pi * (np.outer(p, p) % LANES) / LANES
    cos, sin = np.cos(angle), np.sin(angle)
    ahead = np.block([[cos, -sin], [sin, cos]])
    back = np.block([[cos, sin], [-sin, cos]])
    low = lambda array: jnp.asarray(array.astype(np.float32)).astype(jnp.bfloat16)
    return low(first), low(last), jnp.asarray(twist.astype(np.float32)), low(ahead), low(back)


def split_bf16(array):
    high = array.astype(jnp.bfloat16).astype(jnp.float32)
    middle = (array - high).astype(jnp.bfloat16).astype(jnp.float32)
    low = (array - high - middle).astype(jnp.bfloat16).astype(jnp.float32)
    return high, middle, low


def host_split(array):
    low_type = jnp.bfloat16.dtype
    high = array.astype(low_type).astype(np.float64)
    middle = (array - high).astype(low_type).astype(np.float64)
    low = (array - high - middle).astype(low_type).astype(np.float64)
    return high, middle, low


def flip(value, bits):
    bit = 1
    while bit <= bits:
        if bits & bit:
            value = value + bit - 2 * bit * lax.rem(lax.div(value, bit), 2)
        bit *= 2
    return value


def mixer_kernel(
    rows, cols, width, emb,
    tokens_hbm, w_value_hbm, w_first_hbm, w_second_hbm, w_gate_hbm, w_out_hbm, conv_hbm, embed_hbm, freq_hbm,
    proj_hbm, decay_hbm, gain_hbm, features_hbm, first_hbm, last_hbm, twist_hbm, ahead_hbm, back_hbm, perm_hbm,
    out_ref,
    tokens_ref, w_refs, conv_ref, embed_ref, freq_ref, fproj_ref, decay_ref, gain_ref, features_ref, first_ref,
    last_ref, twist_ref, ahead_ref, back_ref, perm_ref,
    send, recv, spectra, taps_ref, stack_ref, coef_ref, gated, gated_in, edge_out, edge_in, piece, final, weights, total,
    load_sem, row_send, row_recv, edge_send, edge_recv, gate_send, gate_recv, piece_send, piece_recv,
    wide_send, wide_recv, level_send, level_recv, pass_send, pass_recv, mate_send, mate_recv, told,
):
    my_row = lax.axis_index("row")
    my_col = lax.axis_index("col")
    mesh_id = pl.DeviceIdType.MESH
    groups = recv.shape[2]
    chans = groups * PACK
    tok_rows = tokens_ref.shape[0]
    block_q = tok_rows // LANES
    length_q = rows * block_q
    length = tok_rows * rows
    half = length_q + 1
    hid = freq_ref.shape[1]
    f32, low = jnp.float32, jnp.bfloat16

    def remote(src, dst, send_sem, recv_sem, row, col):
        return pltpu.make_async_remote_copy(
            src_ref=src, dst_ref=dst, send_sem=send_sem, recv_sem=recv_sem,
            device_id=(row, col), device_id_type=mesh_id,
        )

    side = lax.rem(my_row, 2)
    mate = flip(my_row, 1)
    low_row = my_row - side
    barrier = pltpu.get_barrier_semaphore()

    def greet(row, col):
        pl.semaphore_signal(barrier, inc=1, device_id=(row, col), device_id_type=mesh_id)

    greet(mate, my_col)
    for d in range(1, cols):
        greet(low_row, flip(my_col, d))
    for d in range(1, rows // 2):
        greet(flip(low_row, 2 * d) + 1, my_col)

    def heard(own_side):
        others = 2 * cols - 1 if own_side == 0 else rows - 1

        @pl.when(side == own_side)
        def _():
            pl.semaphore_wait(barrier, others)
            pl.semaphore_signal(told, inc=1, device_id=(mate, my_col), device_id_type=mesh_id)

        @pl.when(side != own_side)
        def _():
            pl.semaphore_wait(told, 1)

    loads = {}
    for name, src, dst in (
        ("tokens", tokens_hbm, tokens_ref),
        ("value", w_value_hbm, w_refs.at[0]),
        ("embed", embed_hbm, embed_ref.at[pl.ds(0, emb)]),
        ("freq", freq_hbm, freq_ref),
        ("conv", conv_hbm, conv_ref),
        ("gain", gain_hbm, gain_ref),
        ("decay", decay_hbm, decay_ref),
        ("first", w_first_hbm, w_refs.at[1]),
        ("second", w_second_hbm, w_refs.at[2]),
        ("gate", w_gate_hbm, w_refs.at[3]),
        ("fproj", proj_hbm, fproj_ref),
        ("features", features_hbm, features_ref),
        ("dft_first", first_hbm, first_ref),
        ("twist", twist_hbm, twist_ref),
        ("ahead", ahead_hbm, ahead_ref),
        ("perm", perm_hbm, perm_ref),
        ("back", back_hbm, back_ref),
        ("dft_last", last_hbm, last_ref),
        ("w_out", w_out_hbm, weights.at[0]),
    ):
        loads[name] = pltpu.make_async_copy(src, dst, load_sem.at[len(loads)])
        loads[name].start()

    plane = lax.rem(lax.div(my_row, 2), 2)
    subs = rows // 2
    row_of = lambda sub: side * subs + sub

    def wide_copy(index, d, sub):
        return remote(
            w_out_hbm.at[row_of(sub)], weights.at[d, row_of(sub)],
            wide_send.at[index], wide_recv.at[index], my_row, flip(my_col, d),
        )

    wide = {
        (d, sub): wide_copy(index, d, sub + plane if sub == mixed else sub)
        for index, (d, sub, mixed) in enumerate(
            ((1, 0, 0), (2, 2, 2), (1, 2, 0), (2, 0, 2), (1, 3, 0), (2, 1, 2))
        )
    }

    def level_copy(index, d, sub):
        part = weights.at[d, row_of(sub + plane)]
        return remote(part, part, level_send.at[index], level_recv.at[index], flip(my_row, 2), my_col)

    level = {1: level_copy(0, 1, 0), 2: level_copy(1, 2, 2)}

    def pass_copy(index, d, sub):
        return remote(
            weights.at[d, row_of(sub)], weights.at[3, row_of(sub)],
            pass_send.at[index], pass_recv.at[index], my_row, flip(my_col, 3 - d),
        )

    passed = {(d, sub): pass_copy(i, d, sub) for i, (d, sub) in enumerate(((1, 2), (2, 0), (1, 3), (2, 1)))}

    def mate_copy(index, d, sub):
        part = weights.at[d, row_of(sub)]
        return remote(part, part, mate_send.at[index], mate_recv.at[index], mate, my_col)

    mates = {}
    for d in range(1, cols):
        for sub in range(subs):
            here = sub
            if d == 1 and sub < 2:
                here = plane if sub == 0 else 1 - plane
            if d == 2 and sub >= 2:
                here = 2 + plane if sub == 2 else 3 - plane
            mates[d, sub] = mate_copy(subs * (d - 1) + sub, d, here)

    far_first = sorted(range(1, rows), key=lambda d: -(d & (rows // 2)))

    def row_copies(role):
        return [
            remote(
                send.at[role, flip(my_row, d)], recv.at[role, my_row],
                row_send.at[role, d - 1], row_recv.at[role, d - 1], flip(my_row, d), my_col,
            )
            for d in far_first
        ]

    def project(role):
        return jnp.dot(tokens_ref[...], w_refs[role], preferred_element_type=f32)

    def project_turned(role):
        result = project(role).T
        for q in range(block_q):
            send[role, :, :, q] = (
                result[:, q * LANES : (q + 1) * LANES].reshape(rows, groups, PACK, LANES).astype(low)
            )

    value_copies, first_copies = row_copies(0), row_copies(1)

    heard(0)
    for copy in wide.values():
        copy.start()
    loads["tokens"].wait()
    loads["value"].wait()
    project_turned(0)
    heard(1)
    for copy in value_copies:
        copy.start()
    recv[0, my_row] = send[0, my_row]

    loads["second"].wait()
    second = project(2).astype(low).astype(f32)
    edge_out[0] = jnp.broadcast_to(second[tok_rows - 1 :], edge_out.shape[1:])
    edge_out[1] = jnp.broadcast_to(second[:1], edge_out.shape[1:])
    edges = [
        remote(edge_out.at[0], edge_in.at[0], edge_send.at[0], edge_recv.at[0], lax.rem(my_row + 1, rows), my_col),
        remote(edge_out.at[1], edge_in.at[1], edge_send.at[1], edge_recv.at[1], lax.rem(my_row + rows - 1, rows), my_col),
    ]
    for copy in edges:
        copy.start()
    loads["first"].wait()
    project_turned(1)
    for copy in first_copies:
        copy.start()
    recv[1, my_row] = send[1, my_row]
    loads["gate"].wait()
    gate = project(3).astype(low).astype(f32)
    loads["conv"].wait()

    loads["gain"].wait()
    loads["decay"].wait()
    stack_ref[...] = jnp.zeros_like(stack_ref)
    for j in range(3):
        stack_ref[j : j + 1] = conv_ref[j, 0:1]
        stack_ref[3 + j : 4 + j] = conv_ref[j, 1:2]
    stack_ref[6:8] = gain_ref[...]
    stack_ref[8:10] = decay_ref[0]
    stack_ref[10:12] = decay_ref[1]
    shape = (chans, stack_ref.shape[1])
    picks = lax.broadcasted_iota(jnp.int32, shape, 1) == lax.broadcasted_iota(jnp.int32, shape, 0) + my_row * chans
    picks = jnp.where(picks, 1.0, 0.0)
    contract_last = (((1,), (1,)), ((), ()))
    own = lax.dot_general(picks, stack_ref[...], contract_last, precision=precise, preferred_element_type=f32)
    for k in range(8):
        coef_ref[k] = jnp.broadcast_to(own[:, k : k + 1], (chans, LANES)).reshape(groups, PACK, LANES)

    loads["embed"].wait()
    loads["freq"].wait()
    embed = embed_ref[...] * (freq_ref[...] * (1.0 / math.pi))
    embed = jnp.where(lax.broadcasted_iota(jnp.int32, embed.shape, 0) < emb, embed, 0.0)
    high, middle, least = split_bf16(embed)
    stacked = jnp.concatenate([high, high, middle, high, middle, least], axis=0).astype(low)
    loads["features"].wait()
    turns = lax.dot_general(stacked, features_ref[...], (((0,), (0,)), ((), ())), preferred_element_type=f32)
    whole = jnp.floor(turns + 0.5)
    rest = turns - whole
    sign = 1.0 - 2.0 * (whole - 2.0 * jnp.floor(whole * 0.5))
    square = rest * rest
    series = jnp.full_like(square, -(math.pi**11) / math.factorial(11))
    for n in (9, 7, 5, 3, 1):
        series = series * square + (-1) ** (n // 2) * math.pi**n / math.factorial(n)
    hidden = (series * (rest * sign)).astype(low)
    loads["fproj"].wait()
    pieces = []
    picks_low = picks.astype(low)
    halves = 2
    for od in range(4):
        parts = [
            fproj_ref[pl.ds((od // 2) * 2 * halves + j * 2 + od % 2, hid, stride=4 * halves), :]
            for j in range(halves)
        ]
        block = jnp.concatenate(parts, axis=1).astype(low)
        pieces.append(lax.dot_general(picks_low, block, contract_last, preferred_element_type=f32).astype(low))
    taps = jnp.dot(jnp.concatenate(pieces, axis=0), hidden, preferred_element_type=f32)
    lag = lax.broadcasted_iota(jnp.int32, (1, length), 1)
    spot = lag.astype(f32) / (length - 1)
    for od in range(4):
        block = taps[od * chans : (od + 1) * chans] * jnp.exp(-own[:, 8 + od : 9 + od] * spot)
        if od % 2 == 1:
            block = jnp.where(lag == 0, 0.0, block)
        taps_ref[od] = block.astype(low)

    def wide_twist(index):
        return twist_ref[index].reshape(half, 1, 8, LANES)

    def ahead(signal):
        mid = jnp.dot(first_ref[...], signal, preferred_element_type=f32)
        blank = jnp.zeros((PACK, LANES), f32)
        blocks = []
        for g in range(groups):
            lanes = slice(g * LANES, (g + 1) * LANES)
            real = mid[: half * PACK, lanes].reshape(half, 2, 8, LANES)
            imag = jnp.concatenate([blank, mid[half * PACK :, lanes], blank], axis=0).reshape(half, 2, 8, LANES)
            cos, sin = wide_twist(0), wide_twist(1)
            blocks.append(
                jnp.concatenate(
                    [
                        (real * cos + imag * sin).reshape(half * PACK, LANES),
                        (imag * cos - real * sin).reshape(half * PACK, LANES),
                    ],
                    axis=1,
                ).astype(low)
            )
        return jnp.dot(jnp.concatenate(blocks, axis=0), ahead_ref[...], preferred_element_type=f32)

    def convolve(signal, order):
        spec = ahead(signal.astype(low))
        real, imag = spec[:, :LANES], spec[:, LANES:]
        filt_real, filt_imag = spectra[order, 0], spectra[order, 1]
        prod = jnp.concatenate(
            [real * filt_real - imag * filt_imag, real * filt_imag + imag * filt_real], axis=1
        ).astype(low)
        mid = jnp.dot(prod, back_ref[...], preferred_element_type=f32)
        blocks = []
        for g in range(groups):
            span = slice(g * half * PACK, (g + 1) * half * PACK)
            real = mid[span, :LANES].reshape(half, 2, 8, LANES)
            imag = mid[span, LANES:].reshape(half, 2, 8, LANES)
            cos, sin = wide_twist(0), wide_twist(1)
            turned_real = (real * cos - imag * sin).reshape(half * PACK, LANES)
            turned_imag = (real * sin + imag * cos)[1:-1].reshape((half - 2) * PACK, LANES)
            blocks.append(jnp.concatenate([turned_real, turned_imag], axis=0).astype(low))
        result = jnp.dot(last_ref[...], jnp.concatenate(blocks, axis=1), preferred_element_type=f32)
        gain = jnp.concatenate([coef_ref[6 + order, g] for g in range(groups)], axis=1)
        shape = (length_q, PACK, groups * LANES)
        return (result.reshape(shape) + gain[None] * signal.reshape(shape)).reshape(signal.shape)

    loads["dft_first"].wait()
    loads["twist"].wait()
    loads["ahead"].wait()
    for order in range(2):
        for direction in range(2):
            od = 2 * order + direction
            signal = jnp.concatenate(
                [
                    jnp.concatenate(
                        [
                            taps_ref[od, g * PACK : (g + 1) * PACK, q * LANES : (q + 1) * LANES]
                            for q in range(length_q)
                        ],
                        axis=0,
                    )
                    for g in range(groups)
                ],
                axis=1,
            )
            spec = ahead(signal)
            if direction == 0:
                spectra[order, 0] = spec[:, :LANES]
                spectra[order, 1] = spec[:, LANES:]
            else:
                spectra[order, 0] += spec[:, :LANES]
                spectra[order, 1] -= spec[:, LANES:]

    for d in (1, 2):
        wide[d, 2 * d - 2].wait_recv()
        level[d].start()
        mates[d, 2 * d - 2].start()

    def short(role):
        blocks = []
        for g in range(groups):
            here = recv[role, :, g].reshape(length_q * PACK, LANES).astype(f32)
            size = here.shape[0]
            lane = lax.broadcasted_iota(jnp.int32, here.shape, 1)
            blank = jnp.zeros((PACK, LANES), f32)
            before = pltpu.roll(here, 1, 1)
            before = jnp.where(lane == 0, jnp.concatenate([blank, before[: size - PACK]], axis=0), before)
            after = pltpu.roll(here, LANES - 1, 1)
            after = jnp.where(lane == LANES - 1, jnp.concatenate([after[PACK:], blank], axis=0), after)
            shape = (length_q, PACK, LANES)
            w = lambda j: coef_ref[3 * role + j, g][None]
            result = before.reshape(shape) * w(0) + here.reshape(shape) * w(1) + after.reshape(shape) * w(2)
            blocks.append(result.reshape(size, LANES))
        return jnp.concatenate(blocks, axis=1)

    loads["back"].wait()
    loads["dft_last"].wait()
    for copy in value_copies:
        copy.wait_recv()
    conv = convolve(short(0), 0)

    for copy in edges:
        copy.wait_recv()
    line = lax.broadcasted_iota(jnp.int32, second.shape, 0)
    above = jnp.where(my_row == 0, 0.0, edge_in[0, 0:1])
    below = jnp.where(my_row == rows - 1, 0.0, edge_in[1, 0:1])
    before = jnp.where(line == 0, above, pltpu.roll(second, 1, 0))
    after = jnp.where(line == tok_rows - 1, below, pltpu.roll(second, tok_rows - 1, 0))
    short_second = before * conv_ref[0, 2:3] + second * conv_ref[1, 2:3] + after * conv_ref[2, 2:3]
    both = (short_second * (gate / (1.0 + jnp.exp(-gate)))).astype(low)
    loads["perm"].wait()
    both = jnp.dot(both, perm_ref[...], preferred_element_type=f32).astype(low)
    per_group = rows * PACK
    for g in range(groups):
        gated[:, g] = both[:, g * per_group : (g + 1) * per_group].reshape(cols, width, per_group)
    gate_copies = [
        remote(
            gated.at[flip(my_col, d)], gated_in.at[d], gate_send.at[d - 1], gate_recv.at[d - 1], my_row, flip(my_col, d)
        )
        for d in range(1, cols)
    ]
    for copy in gate_copies:
        copy.start()
    gated_in[0] = gated[my_col]

    for copy in first_copies:
        copy.wait_recv()
    conv = convolve(short(1) * conv, 1)

    left = conv[:, :LANES].reshape(length_q, PACK, LANES)
    right = conv[:, LANES:].reshape(length_q, PACK, LANES)
    lane = lax.broadcasted_iota(jnp.int32, left.shape, 2)
    piece[:, 0] = jnp.where(lane < width, left, pltpu.roll(right, width, 2)).astype(low)
    piece[:, 1] = jnp.where(lane < width, pltpu.roll(left, width, 2), right).astype(low)
    piece_copies = []
    for dr in far_first + [0]:
        for dc in range(cols):
            if dr == 0 and dc == 0:
                continue
            row, col = flip(my_row, dr), flip(my_col, dc)
            index = dr * cols + dc - 1
            piece_copies.append(
                remote(
                    piece.at[row * block_q + lax.div(col, 2), lax.rem(col, 2)], final.at[dc, my_row],
                    piece_send.at[index], piece_recv.at[index], row, col,
                )
            )
    for copy in piece_copies:
        copy.start()
    final[0, my_row] = piece[my_row * block_q + lax.div(my_col, 2), lax.rem(my_col, 2)]

    for key, copy in passed.items():
        wide[key].wait_recv()
        copy.start()
        mates[key].start()
    for d in (1, 2):
        level[d].wait_recv()
        mates[d, 2 * d - 1].start()

    for copy in gate_copies:
        copy.wait_recv()
    for copy in piece_copies:
        copy.wait_recv()
    loads["w_out"].wait()
    depth = weights.shape[4]

    def share(d):
        outer = final[d].reshape(rows * PACK, LANES).astype(f32).T
        outer = (outer * gated_in[d].reshape(groups * width, per_group).astype(f32)).astype(low)
        left = jnp.concatenate([outer[g * width : (g + 1) * width] for g in range(groups)], axis=1)
        right = jnp.concatenate([weights[d, :, g].reshape(per_group, depth) for g in range(groups)], axis=0)
        return jnp.dot(left, right, preferred_element_type=f32)

    for d in (1, 2):
        for sub in range(subs):
            mates[d, sub].wait_recv()
    total[...] = share(0) + share(1) + share(2)
    for d, sub in ((2, 0), (1, 2), (2, 1), (1, 3)):
        passed[d, sub].wait_recv()
        mates[3, sub].start()
    for sub in range(subs):
        mates[3, sub].wait_recv()
    out_ref[...] = (total[...] + share(3)).astype(low)
    for copy in value_copies + first_copies + edges + gate_copies + piece_copies:
        copy.wait_send()
    for group in (wide, level, passed, mates):
        for copy in group.values():
            copy.wait_send()


def fast_body(
    tokens, w_value, w_first, w_second, w_gate, conv_taps, filter_embed, filter_freq, filter_proj,
    filter_decay, skip_gain, w_out,
):
    rows, cols = lax.axis_size("row"), lax.axis_size("col")
    tok_rows = tokens.shape[1]
    chan_col = w_value.shape[1]
    chans = chan_col // rows
    groups = chans // PACK
    length = tok_rows * rows
    block_q = tok_rows // LANES
    length_q = length // LANES
    width = tok_rows // cols
    depth = w_out.shape[1]
    emb, hid = filter_embed.shape
    half = length_q + 1

    flat = tokens.reshape(tok_rows, tokens.shape[2])
    bands = (emb - 1) // 2
    index = np.arange(length)
    spot = index.astype(np.float32) / np.float32(length - 1)
    phase = 2.0 * np.pi * (np.outer(np.arange(1, bands + 1), index) % length) / length
    features = np.concatenate([spot[None, :], np.cos(phase), np.sin(phase)])
    emb_pad = -(-emb // 8) * 8
    features = np.concatenate([features, np.zeros((emb_pad - emb, length))]).astype(np.float32).astype(np.float64)
    high, middle, least = host_split(features)
    features = np.concatenate([high, middle, high, least, middle, high]).astype(jnp.bfloat16.dtype)
    own = np.arange(chan_col).reshape(rows, groups, PACK).transpose(1, 0, 2).reshape(-1)
    perm = np.zeros((chan_col, chan_col), np.float32)
    perm[own, np.arange(chan_col)] = 1.0
    lanes = chan_col // LANES
    fproj = filter_proj.reshape(hid, 2, 2, lanes, LANES).transpose(0, 1, 3, 2, 4).reshape(hid * 4 * lanes, LANES)
    w_rows = w_out.reshape(rows, groups, PACK, depth)

    first, last, twist, ahead, back = dft_tables(length)
    operands = (
        flat, w_value, w_first, w_second, w_gate, w_rows, conv_taps, filter_embed, filter_freq.reshape(1, hid),
        fproj, filter_decay, skip_gain, jnp.asarray(features), first, last, twist, ahead, back,
        jnp.asarray(perm).astype(jnp.bfloat16),
    )
    dma = pltpu.SemaphoreType.DMA
    f32, low = jnp.float32, jnp.bfloat16
    like = lambda array: pltpu.VMEM(array.shape, array.dtype)
    mixed = pl.pallas_call(
        functools.partial(mixer_kernel, rows, cols, width, emb),
        out_shape=pltpu.VMEM((width, depth), low),
        in_specs=[pl.BlockSpec(memory_space=pl.ANY)] * len(operands),
        out_specs=pl.BlockSpec(memory_space=pltpu.VMEM),
        scratch_shapes=[
            like(flat),
            pltpu.VMEM((4,) + w_value.shape, low),
            like(conv_taps),
            pltpu.VMEM((emb_pad, hid), f32),
            pltpu.VMEM((1, hid), f32),
            like(fproj),
            like(filter_decay),
            like(skip_gain),
            pltpu.VMEM(features.shape, low),
            like(first),
            like(last),
            like(twist),
            like(ahead),
            like(back),
            pltpu.VMEM(perm.shape, low),
            pltpu.VMEM((2, rows, groups, block_q, PACK, LANES), low),
            pltpu.VMEM((2, rows, groups, block_q, PACK, LANES), low),
            pltpu.VMEM((2, 2, groups * half * PACK, LANES), f32),
            pltpu.VMEM((4, chans, length), low),
            pltpu.VMEM((16, chan_col), f32),
            pltpu.VMEM((8, groups, PACK, LANES), f32),
            pltpu.VMEM((cols, groups, width, rows * PACK), low),
            pltpu.VMEM((cols, groups, width, rows * PACK), low),
            pltpu.VMEM((2, 8, chan_col), f32),
            pltpu.VMEM((2, 8, chan_col), f32),
            pltpu.VMEM((length_q, groups, PACK, LANES), low),
            pltpu.VMEM((cols, rows, PACK, LANES), low),
            pltpu.VMEM((cols, rows, groups, PACK, depth), low),
            pltpu.VMEM((width, depth), f32),
            dma((len(operands),)),
            dma((2, rows - 1)),
            dma((2, rows - 1)),
            dma((2,)),
            dma((2,)),
            dma((cols - 1,)),
            dma((cols - 1,)),
            dma((rows * cols - 1,)),
            dma((rows * cols - 1,)),
            dma((6,)),
            dma((6,)),
            dma((2,)),
            dma((2,)),
            dma((4,)),
            dma((4,)),
            dma(((cols - 1) * rows // 2,)),
            dma(((cols - 1) * rows // 2,)),
            pltpu.SemaphoreType.REGULAR,
        ],
        compiler_params=pltpu.CompilerParams(
            collective_id=0, has_side_effects=True, vmem_limit_bytes=40 * 1024 * 1024
        ),
        cost_estimate=pl.CostEstimate(flops=12_000_000_000, bytes_accessed=8_000_000, transcendentals=0),
    )(*[pltpu.with_memory_space_constraint(array, pltpu.HBM) for array in operands])
    return mixed[None]


def shaped_body(tokens, w_value, *rest):
    rows, cols = lax.axis_size("row"), lax.axis_size("col")
    seqs, tok_rows = tokens.shape[:2]
    chan_col = w_value.shape[1]
    chans = chan_col // rows
    width = tok_rows // cols
    fits = (
        seqs == 1
        and cols == 4
        and rows == 8
        and chans == 2 * PACK
        and tok_rows % LANES == 0
        and LANES == 2 * width
        and chan_col == 2 * LANES
        and rows * PACK == LANES
    )
    return (fast_body if fits else body)(tokens, w_value, *rest)


def solution(mesh):
    in_specs = (
        P(None, "row", None),
        P(None, "col"),
        P(None, "col"),
        P(None, "col"),
        P(None, "col"),
        P(None, None, "col"),
        P(),
        P(),
        P(None, None, None, "col"),
        P(None, None, "col"),
        P(None, "col"),
        P("col", None),
    )
    out_specs = P(None, ("row", "col"), None)
    return jax.shard_map(shaped_body, mesh=mesh, in_specs=in_specs, out_specs=out_specs, check_vma=False)
```

```python
import functools
import math

import jax
import jax.numpy as jnp
import numpy as np
from jax import lax
from jax.experimental import pallas as pl
from jax.experimental.pallas import tpu as pltpu
from jax.sharding import PartitionSpec as P

precise = lax.Precision.HIGHEST


def padded_2(array, sides, width):
    for axis, dim in sides:
        size, length = (lax.axis_size(axis), array.shape[dim])
        up = [(i, (i + 1) % size) for i in range(size - 1)]
        down = [(j, i) for i, j in up]
        last = lax.slice_in_dim(array, length - width, length, axis=dim)
        leading = lax.slice_in_dim(array, 0, width, axis=dim)
        before = lax.ppermute(last, axis, up)
        after = lax.ppermute(leading, axis, down)
        array = jnp.concatenate([before, array, after], axis=dim)
    return array


def split_length(total):
    factor = math.isqrt(total)
    while total % factor != 0:
        factor = factor - 1
    return (factor, total // factor)


def tables(outer, inner, total):
    first_index = jnp.arange(outer, dtype=jnp.int32)
    second_index = jnp.arange(inner, dtype=jnp.int32)
    scale = 2.0 * math.pi
    outer_angle = (first_index[:, None] * first_index[None, :] % outer).astype(jnp.float32) * (
        scale / outer
    )
    inner_angle = (second_index[:, None] * second_index[None, :] % inner).astype(jnp.float32) * (
        scale / inner
    )
    twist_angle = (first_index[:, None] * second_index[None, :] % total).astype(jnp.float32) * (
        scale / total
    )
    return (
        jnp.cos(outer_angle),
        jnp.sin(outer_angle),
        jnp.cos(inner_angle),
        jnp.sin(inner_angle),
        jnp.cos(twist_angle),
        jnp.sin(twist_angle),
    )


def forward_real(signal, table):
    outer_cos, outer_sin, inner_cos, inner_sin, twist_cos, twist_sin = table
    outer = outer_cos.shape[0]
    inner = inner_cos.shape[0]
    grid = signal.reshape(signal.shape[0], outer, inner)
    real_part = jnp.einsum("kq,cqp->ckp", outer_cos, grid, precision=precise)
    imag_part = -jnp.einsum("kq,cqp->ckp", outer_sin, grid, precision=precise)
    turned_real = real_part * twist_cos + imag_part * twist_sin
    turned_imag = imag_part * twist_cos - real_part * twist_sin
    spec_real = jnp.einsum("ckp,pj->ckj", turned_real, inner_cos, precision=precise) + jnp.einsum(
        "ckp,pj->ckj", turned_imag, inner_sin, precision=precise
    )
    spec_imag = jnp.einsum("ckp,pj->ckj", turned_imag, inner_cos, precision=precise) - jnp.einsum(
        "ckp,pj->ckj", turned_real, inner_sin, precision=precise
    )
    return (spec_real, spec_imag)


def inverse_real(spec_real, spec_imag, table):
    outer_cos, outer_sin, inner_cos, inner_sin, twist_cos, twist_sin = table
    total = outer_cos.shape[0] * inner_cos.shape[0]
    back_real = jnp.einsum("ckj,jp->ckp", spec_real, inner_cos, precision=precise) - jnp.einsum(
        "ckj,jp->ckp", spec_imag, inner_sin, precision=precise
    )
    back_imag = jnp.einsum("ckj,jp->ckp", spec_real, inner_sin, precision=precise) + jnp.einsum(
        "ckj,jp->ckp", spec_imag, inner_cos, precision=precise
    )
    turned_real = back_real * twist_cos - back_imag * twist_sin
    turned_imag = back_real * twist_sin + back_imag * twist_cos
    result = jnp.einsum("qk,ckp->cqp", outer_cos, turned_real, precision=precise) - jnp.einsum(
        "qk,ckp->cqp", outer_sin, turned_imag, precision=precise
    )
    return result.reshape(result.shape[0], total) / total


def channel_filters(
    length, row_index, chan_row, filter_embed, filter_freq, filter_proj, filter_decay
):
    bands = (filter_embed.shape[0] - 1) // 2
    index = jnp.arange(length, dtype=jnp.int32)
    spot = index.astype(jnp.float32) / (length - 1)
    freqs = jnp.arange(1, bands + 1, dtype=jnp.int32)
    phase = (index[:, None] * freqs[None, :] % length).astype(jnp.float32) * (
        2.0 * math.pi / length
    )
    features = jnp.concatenate([spot[:, None], jnp.cos(phase), jnp.sin(phase)], axis=1)
    hidden = jnp.sin(filter_freq[None, :] * jnp.dot(features, filter_embed, precision=precise))
    own_proj = lax.dynamic_slice_in_dim(filter_proj, row_index * chan_row, chan_row, 3)
    own_decay = lax.dynamic_slice_in_dim(filter_decay, row_index * chan_row, chan_row, 2)
    taps = jnp.dot(hidden, own_proj.reshape(own_proj.shape[0], 4 * chan_row), precision=precise)
    taps = jnp.transpose(taps).reshape(2, 2, chan_row, length)
    taps = taps * jnp.exp(-spot[None, None, None, :] * own_decay[:, :, :, None])
    cycles = []
    for order in range(2):
        behind = jnp.flip(taps[order, 1, :, 1:], axis=1)
        cycles.append(
            jnp.concatenate([taps[order, 0], jnp.zeros((chan_row, 1), jnp.float32), behind], axis=1)
        )
    return cycles


def body(
    tokens,
    w_value,
    w_first,
    w_second,
    w_gate,
    conv_taps,
    filter_embed,
    filter_freq,
    filter_proj,
    filter_decay,
    skip_gain,
    w_out,
):
    seq_count = tokens.shape[0]
    tok_rows = tokens.shape[1]
    chan_col = w_value.shape[1]
    row_count = lax.axis_size("row")
    chan_row = chan_col // row_count
    length = tok_rows * row_count
    row_index = lax.axis_index("row")
    proj = jnp.concatenate(
        [
            jnp.dot(tokens, w_value, preferred_element_type=jnp.float32),
            jnp.dot(tokens, w_first, preferred_element_type=jnp.float32),
            jnp.dot(tokens, w_second, preferred_element_type=jnp.float32),
        ],
        axis=2,
    ).astype(jnp.bfloat16)
    gate = jnp.dot(tokens, w_gate, preferred_element_type=jnp.float32).astype(jnp.bfloat16)
    padded = padded_2(proj, (("row", 1),), 1).astype(jnp.float32)
    weights = conv_taps.reshape(3, 3 * chan_col)
    short = padded[:, :-2] * weights[0] + padded[:, 1:-1] * weights[1] + padded[:, 2:] * weights[2]
    value_rows = jnp.transpose(short[:, :, :chan_col], (0, 2, 1))
    first_rows = jnp.transpose(short[:, :, chan_col : 2 * chan_col], (0, 2, 1))
    second_rows = jnp.transpose(short[:, :, 2 * chan_col :], (0, 2, 1))
    outer, inner = split_length(2 * length)
    table = tables(outer, inner, 2 * length)
    cycles = channel_filters(
        length, row_index, chan_row, filter_embed, filter_freq, filter_proj, filter_decay
    )
    spectra = [forward_real(cycle, table) for cycle in cycles]
    own_gain = lax.dynamic_slice_in_dim(skip_gain, row_index * chan_row, chan_row, 1)

    def convolve(signal, order):
        flat = signal.reshape(seq_count * chan_row, length)
        padded_signal = jnp.concatenate([flat, jnp.zeros_like(flat)], axis=1)
        sig_real, sig_imag = forward_real(padded_signal, table)
        sig_real = sig_real.reshape(seq_count, chan_row, outer, inner)
        sig_imag = sig_imag.reshape(seq_count, chan_row, outer, inner)
        filt_real, filt_imag = spectra[order]
        prod_real = sig_real * filt_real[None] - sig_imag * filt_imag[None]
        prod_imag = sig_real * filt_imag[None] + sig_imag * filt_real[None]
        result = inverse_real(
            prod_real.reshape(seq_count * chan_row, outer, inner),
            prod_imag.reshape(seq_count * chan_row, outer, inner),
            table,
        )[:, :length]
        return result.reshape(seq_count, chan_row, length) + own_gain[order][None, :, None] * signal

    value_chan, first_chan = (
        lax.all_to_all(value_rows, "row", split_axis=1, concat_axis=2, tiled=True),
        lax.all_to_all(first_rows, "row", split_axis=1, concat_axis=2, tiled=True),
    )
    inner_chan = first_chan * convolve(value_chan, 0)
    second_conv = lax.all_to_all(
        convolve(inner_chan, 1), "row", split_axis=2, concat_axis=1, tiled=True
    )
    outer_rows = (
        jnp.transpose(second_rows * second_conv, (0, 2, 1)) * jax.nn.silu(gate.astype(jnp.float32))
    ).astype(jnp.bfloat16)
    own_rows = tok_rows // lax.axis_size("col")
    flat_rows = jnp.transpose(outer_rows, (1, 0, 2)).reshape(tok_rows * seq_count, chan_col)
    summed = lax.psum_scatter(
        jnp.dot(flat_rows, w_out, preferred_element_type=jnp.float32).astype(jnp.bfloat16),
        "col",
        scatter_dimension=0,
        tiled=True,
    ).astype(jnp.float32)
    summed = jnp.transpose(summed.reshape(own_rows, seq_count, w_out.shape[1]), (1, 0, 2))
    return summed.astype(jnp.bfloat16)


LANES = 128
PACK = 16


def dft_tables(length):
    filled = length // LANES
    outer = 2 * filled
    total = outer * LANES
    half = filled + 1
    eye = np.eye(PACK)
    q, k, p = np.arange(filled), np.arange(half), np.arange(LANES)
    inside = k[1:-1]
    angle = 2.0 * np.pi * (np.outer(k, q) % outer) / outer
    first = np.concatenate([np.kron(np.cos(angle), eye), np.kron(-np.sin(angle)[inside], eye)], axis=0)
    weight = np.where((k == 0) | (k == filled), 1.0, 2.0) / total
    last = np.concatenate(
        [
            np.kron(np.cos(angle).T * weight, eye),
            np.kron((-np.sin(angle).T * weight)[:, inside], eye),
        ],
        axis=1,
    )
    turn = 2.0 * np.pi * np.outer(k, p) / total
    twist = np.stack([np.cos(turn), np.sin(turn)])[:, :, None, :]
    twist = np.broadcast_to(twist, (2, half, 8, LANES))
    angle = 2.0 * np.pi * (np.outer(p, p) % LANES) / LANES
    cos, sin = np.cos(angle), np.sin(angle)
    ahead = np.block([[cos, -sin], [sin, cos]])
    back = np.block([[cos, sin], [-sin, cos]])
    return first, last, jnp.asarray(twist.astype(np.float32)), ahead, back


def split_bf16(array):
    high = array.astype(jnp.bfloat16).astype(jnp.float32)
    middle = (array - high).astype(jnp.bfloat16).astype(jnp.float32)
    low = (array - high - middle).astype(jnp.bfloat16).astype(jnp.float32)
    return high, middle, low


def host_split(array):
    low_type = jnp.bfloat16.dtype
    high = array.astype(low_type).astype(np.float64)
    middle = (array - high).astype(low_type).astype(np.float64)
    low = (array - high - middle).astype(low_type).astype(np.float64)
    return high, middle, low


def flip(value, bits):
    bit = 1
    while bit <= bits:
        if bits & bit:
            value = value + bit - 2 * bit * lax.rem(lax.div(value, bit), 2)
        bit *= 2
    return value


def mixer_kernel(
    rows, cols, width, emb,
    tokens_hbm, w_value_hbm, w_first_hbm, w_second_hbm, w_gate_hbm, w_out_hbm, conv_hbm, embed_hbm, freq_hbm,
    proj_hbm, decay_hbm, gain_hbm, features_hbm, tables_hbm, twist_hbm,
    out_ref,
    tokens_ref, w_refs, conv_ref, embed_ref, freq_ref, fproj_ref, decay_ref, gain_ref, features_ref, tables_ref,
    twist_ref,
    send, recv, spectra, taps_ref, stack_ref, coef_ref, gated, gated_in, edge_out, edge_in, piece, final, weights, total,
    load_sem, row_send, row_recv, edge_send, edge_recv, gate_send, gate_recv, piece_send, piece_recv,
    wide_send, wide_recv, level_send, level_recv, pass_send, pass_recv, mate_send, mate_recv, told, ready,
):
    my_row = lax.axis_index("row")
    my_col = lax.axis_index("col")
    mesh_id = pl.DeviceIdType.MESH
    groups = recv.shape[2]
    chans = groups * PACK
    tok_rows = tokens_ref.shape[0]
    block_q = tok_rows // LANES
    length_q = rows * block_q
    length = tok_rows * rows
    half = length_q + 1
    hid = freq_ref.shape[1]
    depth = weights.shape[4]
    f32, low = jnp.float32, jnp.bfloat16

    def remote(src, dst, send_sem, recv_sem, row, col):
        return pltpu.make_async_remote_copy(
            src_ref=src, dst_ref=dst, send_sem=send_sem, recv_sem=recv_sem,
            device_id=(row, col), device_id_type=mesh_id,
        )

    side = lax.rem(my_row, 2)
    mate = flip(my_row, 1)
    low_row = my_row - side
    barrier = pltpu.get_barrier_semaphore()

    def greet(row, col):
        pl.semaphore_signal(barrier, inc=1, device_id=(row, col), device_id_type=mesh_id)

    near = (1, 2)
    greet(mate, my_col)
    for d in near:
        greet(low_row, flip(my_col, d))
    for d in range(1, rows // 2):
        greet(flip(low_row, 2 * d) + 1, my_col)

    def heard(own_side):
        others = 2 * len(near) + 1 if own_side == 0 else rows - 1

        @pl.when(side == own_side)
        def _():
            pl.semaphore_wait(barrier, others)
            pl.semaphore_signal(told, inc=1, device_id=(mate, my_col), device_id_type=mesh_id)

        @pl.when(side != own_side)
        def _():
            pl.semaphore_wait(told, 1)

    def await_bytes(ref, sem):
        pltpu.make_async_copy(ref, ref, sem).wait()

    token_sem, weight_sem = load_sem.at[0], load_sem.at[1]
    pltpu.make_async_copy(tokens_hbm, tokens_ref, token_sem).start()
    pltpu.make_async_copy(w_value_hbm, w_refs.at[0], token_sem).start()
    loads = {}
    for name, src, dst in (
        ("embed", embed_hbm, embed_ref.at[pl.ds(0, emb)]),
        ("freq", freq_hbm, freq_ref),
        ("conv", conv_hbm, conv_ref),
        ("gain", gain_hbm, gain_ref),
        ("decay", decay_hbm, decay_ref),
        ("fproj", proj_hbm, fproj_ref),
        ("features", features_hbm, features_ref),
        ("tables", tables_hbm, tables_ref),
        ("twist", twist_hbm, twist_ref),
        ("w_out", w_out_hbm, weights.at[0]),
    ):
        loads[name] = pltpu.make_async_copy(src, dst, load_sem.at[2 + len(loads)])
    for role, w_hbm in ((2, w_second_hbm), (1, w_first_hbm), (3, w_gate_hbm)):
        pltpu.make_async_copy(w_hbm, w_refs.at[role], weight_sem).start()
    for copy in loads.values():
        copy.start()

    plane = lax.rem(lax.div(my_row, 2), 2)
    subs = rows // 2
    row_of = lambda sub: side * subs + sub

    def wide_copy(index, d, sub):
        return remote(
            w_out_hbm.at[row_of(sub)], weights.at[d, row_of(sub)],
            wide_send, wide_recv.at[index // 2], my_row, flip(my_col, d),
        )

    wide = {
        (d, sub): wide_copy(index, d, sub + plane if sub == mixed else sub)
        for index, (d, sub, mixed) in enumerate(
            ((1, 0, 0), (2, 2, 2), (1, 3, 0), (2, 1, 2), (1, 2, 0), (2, 0, 2))
        )
    }

    def there(part, send_sem, recv_sem, row):
        return remote(part, part, send_sem, recv_sem, row, my_col)

    own_half, far_half = pl.ds(plane, 1), pl.ds(1 - plane, 1)
    all_of = pl.ds(0, groups)
    level_row = flip(my_row, 2)
    level = {
        d: there(weights.at[d, row_of(2 * d - 2 + plane)], level_send, level_recv.at[0], level_row) for d in (1, 2)
    }
    level_late = {
        sub: there(weights.at[3, row_of(sub), own_half, pl.ds(0, PACK), pl.ds(0, depth // 2)], level_send, level_recv.at[1], level_row) for sub in (3, 1)
    }

    shared, unshared = pl.ds(0, depth // 2), pl.ds(depth // 2, depth // 2)
    every_row, every_lane = pl.ds(0, PACK), pl.ds(0, depth)

    def pass_copy(index, d, sub, span, lanes):
        return remote(
            weights.at[d, row_of(sub), span, every_row, lanes], weights.at[3, row_of(sub), span, every_row, lanes],
            pass_send, pass_recv.at[index], my_row, flip(my_col, 3 - d),
        )

    passed = {
        (1, 3): [pass_copy(0, 1, 3, own_half, shared), pass_copy(3, 1, 3, all_of, unshared)],
        (2, 1): [pass_copy(0, 2, 1, own_half, shared), pass_copy(3, 2, 1, all_of, unshared)],
        (1, 2): [pass_copy(1, 1, 2, all_of, every_lane)],
        (2, 0): [pass_copy(2, 2, 0, all_of, every_lane)],
    }

    def to_mate(d, sub, span=all_of, lanes=every_lane):
        there(weights.at[d, row_of(sub), span, every_row, lanes], mate_send, mate_recv.at[d // 3], mate).start()

    far_first = sorted(range(1, rows), key=lambda d: -(d & (rows // 2)))

    def row_copies(role):
        return [
            remote(
                send.at[role, flip(my_row, d)], recv.at[role, my_row],
                row_send.at[role], row_recv.at[role], flip(my_row, d), my_col,
            )
            for d in far_first
        ]

    def project(role):
        return jnp.dot(tokens_ref[...], w_refs[role], preferred_element_type=f32)

    def project_turned(role):
        result = project(role).T
        for q in range(block_q):
            send[role, :, :, q] = (
                result[:, q * LANES : (q + 1) * LANES].reshape(rows, groups, PACK, LANES).astype(low)
            )

    value_copies, first_copies = row_copies(0), row_copies(1)

    heard(0)
    for copy in wide.values():
        copy.start()
    await_bytes(w_refs.at[pl.ds(0, 2)], token_sem)
    project_turned(0)
    heard(1)
    for copy in value_copies:
        copy.start()
    recv[0, my_row] = send[0, my_row]

    await_bytes(w_refs.at[pl.ds(1, 3)], weight_sem)
    second = project(2).astype(low).astype(f32)
    edge_out[0] = jnp.broadcast_to(second[tok_rows - 1 :], edge_out.shape[1:])
    edge_out[1] = jnp.broadcast_to(second[:1], edge_out.shape[1:])
    def edge_copy(index, step):
        return remote(edge_out.at[index], edge_in.at[index], edge_send.at[index], edge_recv.at[index], my_row + step, my_col)

    has_above, has_below = my_row > 0, my_row < rows - 1

    @pl.when(has_below)
    def _():
        edge_copy(0, 1).start()

    @pl.when(has_above)
    def _():
        edge_copy(1, -1).start()

    project_turned(1)
    for copy in first_copies:
        copy.start()
    recv[1, my_row] = send[1, my_row]
    gate = project(3).astype(low).astype(f32)
    loads["conv"].wait()

    loads["gain"].wait()
    loads["decay"].wait()
    stack_ref[...] = jnp.zeros_like(stack_ref)
    for j in range(3):
        stack_ref[j : j + 1] = conv_ref[j, 0:1]
        stack_ref[3 + j : 4 + j] = conv_ref[j, 1:2]
    stack_ref[6:8] = gain_ref[...]
    stack_ref[8:10] = decay_ref[0]
    stack_ref[10:12] = decay_ref[1]
    shape = (chans, stack_ref.shape[1])
    picks = lax.broadcasted_iota(jnp.int32, shape, 1) == lax.broadcasted_iota(jnp.int32, shape, 0) + my_row * chans
    picks = jnp.where(picks, 1.0, 0.0)
    contract_last = (((1,), (1,)), ((), ()))
    own = lax.dot_general(picks, stack_ref[...], contract_last, precision=precise, preferred_element_type=f32)
    for k in range(8):
        coef_ref[k] = jnp.broadcast_to(own[:, k : k + 1], (chans, LANES)).reshape(groups, PACK, LANES)

    loads["embed"].wait()
    loads["freq"].wait()
    embed = embed_ref[...] * (freq_ref[...] * (1.0 / math.pi))
    embed = jnp.where(lax.broadcasted_iota(jnp.int32, embed.shape, 0) < emb, embed, 0.0)
    high, middle, least = split_bf16(embed)
    stacked = jnp.concatenate([high, high, middle, high, middle, least], axis=0).astype(low)
    loads["features"].wait()
    turns = lax.dot_general(stacked, features_ref[...], (((0,), (0,)), ((), ())), preferred_element_type=f32)
    whole = jnp.floor(turns + 0.5)
    rest = turns - whole
    sign = 1.0 - 2.0 * (whole - 2.0 * jnp.floor(whole * 0.5))
    square = rest * rest
    series = jnp.full_like(square, -(math.pi**11) / math.factorial(11))
    for n in (9, 7, 5, 3, 1):
        series = series * square + (-1) ** (n // 2) * math.pi**n / math.factorial(n)
    hidden = (series * (rest * sign)).astype(low)
    loads["fproj"].wait()
    pieces = []
    picks_low = picks.astype(low)
    halves = 2
    for od in range(4):
        parts = [
            fproj_ref[pl.ds((od // 2) * 2 * halves + j * 2 + od % 2, hid, stride=4 * halves), :]
            for j in range(halves)
        ]
        block = jnp.concatenate(parts, axis=1).astype(low)
        pieces.append(lax.dot_general(picks_low, block, contract_last, preferred_element_type=f32).astype(low))
    taps = jnp.dot(jnp.concatenate(pieces, axis=0), hidden, preferred_element_type=f32)
    lag = lax.broadcasted_iota(jnp.int32, (1, length), 1)
    spot = lag.astype(f32) / (length - 1)
    for od in range(4):
        block = taps[od * chans : (od + 1) * chans] * jnp.exp(-own[:, 8 + od : 9 + od] * spot)
        if od % 2 == 1:
            block = jnp.where(lag == 0, 0.0, block)
        taps_ref[od] = block.astype(low)

    size = LANES * groups
    first_ref, last_ref, ahead_ref, back_ref, perm_ref = (
        tables_ref.at[pl.ds(start * size, count * size)]
        for start, count in ((0, 2), (2, 2), (4, 1), (5, 1), (6, 1))
    )

    def wide_twist(index):
        return twist_ref[index].reshape(half, 1, 8, LANES)

    def ahead(signal):
        mid = jnp.dot(first_ref[...], signal, preferred_element_type=f32)
        blank = jnp.zeros((PACK, LANES), f32)
        blocks = []
        for g in range(groups):
            lanes = slice(g * LANES, (g + 1) * LANES)
            real = mid[: half * PACK, lanes].reshape(half, 2, 8, LANES)
            imag = jnp.concatenate([blank, mid[half * PACK :, lanes], blank], axis=0).reshape(half, 2, 8, LANES)
            cos, sin = wide_twist(0), wide_twist(1)
            blocks.append(
                jnp.concatenate(
                    [
                        (real * cos + imag * sin).reshape(half * PACK, LANES),
                        (imag * cos - real * sin).reshape(half * PACK, LANES),
                    ],
                    axis=1,
                ).astype(low)
            )
        return jnp.dot(jnp.concatenate(blocks, axis=0), ahead_ref[...], preferred_element_type=f32)

    def convolve(signal, order):
        spec = ahead(signal.astype(low))
        real, imag = spec[:, :LANES], spec[:, LANES:]
        filt_real, filt_imag = spectra[order, 0], spectra[order, 1]
        prod = jnp.concatenate(
            [real * filt_real - imag * filt_imag, real * filt_imag + imag * filt_real], axis=1
        ).astype(low)
        mid = jnp.dot(prod, back_ref[...], preferred_element_type=f32)
        blocks = []
        for g in range(groups):
            span = slice(g * half * PACK, (g + 1) * half * PACK)
            real = mid[span, :LANES].reshape(half, 2, 8, LANES)
            imag = mid[span, LANES:].reshape(half, 2, 8, LANES)
            cos, sin = wide_twist(0), wide_twist(1)
            turned_real = (real * cos - imag * sin).reshape(half * PACK, LANES)
            turned_imag = (real * sin + imag * cos)[1:-1].reshape((half - 2) * PACK, LANES)
            blocks.append(jnp.concatenate([turned_real, turned_imag], axis=0).astype(low))
        last = jnp.concatenate([last_ref[:size], last_ref[size:]], axis=1)
        result = jnp.dot(last, jnp.concatenate(blocks, axis=1), preferred_element_type=f32)
        gain = jnp.concatenate([coef_ref[6 + order, g] for g in range(groups)], axis=1)
        shape = (length_q, PACK, groups * LANES)
        return (result.reshape(shape) + gain[None] * signal.reshape(shape)).reshape(signal.shape)

    loads["tables"].wait()
    loads["twist"].wait()
    for order in range(2):
        for direction in range(2):
            od = 2 * order + direction
            signal = jnp.concatenate(
                [
                    jnp.concatenate(
                        [
                            taps_ref[od, g * PACK : (g + 1) * PACK, q * LANES : (q + 1) * LANES]
                            for q in range(length_q)
                        ],
                        axis=0,
                    )
                    for g in range(groups)
                ],
                axis=1,
            )
            spec = ahead(signal)
            if direction == 0:
                spectra[order, 0] = spec[:, :LANES]
                spectra[order, 1] = spec[:, LANES:]
            else:
                spectra[order, 0] += spec[:, :LANES]
                spectra[order, 1] -= spec[:, LANES:]

    await_bytes(weights.at[0, pl.ds(0, 2)], wide_recv.at[0])
    for d in (1, 2):
        level[d].start()
        to_mate(d, 2 * d - 2 + plane)


    @pl.when(has_above)
    def _():
        await_bytes(edge_in.at[0], edge_recv.at[0])

    @pl.when(has_below)
    def _():
        await_bytes(edge_in.at[1], edge_recv.at[1])

    line = lax.broadcasted_iota(jnp.int32, second.shape, 0)
    above = jnp.where(has_above, edge_in[0, 0:1], 0.0)
    below = jnp.where(has_below, edge_in[1, 0:1], 0.0)
    before = jnp.where(line == 0, above, pltpu.roll(second, 1, 0))
    after = jnp.where(line == tok_rows - 1, below, pltpu.roll(second, tok_rows - 1, 0))
    short_second = before * conv_ref[0, 2:3] + second * conv_ref[1, 2:3] + after * conv_ref[2, 2:3]
    both = (short_second * (gate / (1.0 + jnp.exp(-gate)))).astype(low)
    both = jnp.dot(both, perm_ref[...], preferred_element_type=f32).astype(low)
    per_group = rows * PACK
    for g in range(groups):
        gated[:, g] = both[:, g * per_group : (g + 1) * per_group].reshape(cols, width, per_group)
    gate_copies = [
        remote(
            gated.at[flip(my_col, d)], gated_in.at[d], gate_send, gate_recv, my_row, flip(my_col, d)
        )
        for d in range(1, cols)
    ]
    for copy in gate_copies:
        copy.start()
    gated_in[0] = gated[my_col]

    def pass_on(index, keys):
        await_bytes(weights.at[0, pl.ds(0, 2)], wide_recv.at[1 + index])
        for key in keys:
            for copy in passed[key]:
                copy.start()
            to_mate(*key)

    def short(role):
        blocks = []
        for g in range(groups):
            here = recv[role, :, g].reshape(length_q * PACK, LANES).astype(f32)
            size = here.shape[0]
            lane = lax.broadcasted_iota(jnp.int32, here.shape, 1)
            blank = jnp.zeros((PACK, LANES), f32)
            before = pltpu.roll(here, 1, 1)
            before = jnp.where(lane == 0, jnp.concatenate([blank, before[: size - PACK]], axis=0), before)
            after = pltpu.roll(here, LANES - 1, 1)
            after = jnp.where(lane == LANES - 1, jnp.concatenate([after[PACK:], blank], axis=0), after)
            shape = (length_q, PACK, LANES)
            w = lambda j: coef_ref[3 * role + j, g][None]
            result = before.reshape(shape) * w(0) + here.reshape(shape) * w(1) + after.reshape(shape) * w(2)
            blocks.append(result.reshape(size, LANES))
        return jnp.concatenate(blocks, axis=1)

    others = pl.ds(0, rows - 1)
    await_bytes(recv.at[0, others], row_recv.at[0])
    pl.semaphore_signal(ready, inc=1, device_id=(my_row, flip(my_col, 1)), device_id_type=mesh_id)
    conv = convolve(short(0), 0)

    pass_on(0, ((1, 3), (2, 1)))
    await_bytes(recv.at[1, others], row_recv.at[1])
    conv = convolve(short(1) * conv, 1)

    left = conv[:, :LANES].reshape(length_q, PACK, LANES)
    right = conv[:, LANES:].reshape(length_q, PACK, LANES)
    lane = lax.broadcasted_iota(jnp.int32, left.shape, 2)
    piece[:, 0] = jnp.where(lane < width, left, pltpu.roll(right, width, 2)).astype(low)
    piece[:, 1] = jnp.where(lane < width, pltpu.roll(left, width, 2), right).astype(low)
    piece_copies = []
    for dr in far_first + [0]:
        for dc in range(cols):
            if dr == 0 and dc == 0:
                continue
            row, col = flip(my_row, dr), flip(my_col, dc)
            piece_copies.append(
                remote(
                    piece.at[row * block_q + lax.div(col, 2), lax.rem(col, 2)], final.at[dc * rows + my_row],
                    piece_send, piece_recv, row, col,
                )
            )
    pl.semaphore_wait(ready, 1)
    for copy in piece_copies:
        copy.start()
    final[my_row] = piece[my_row * block_q + lax.div(my_col, 2), lax.rem(my_col, 2)]

    pass_on(1, ((1, 2), (2, 0)))
    await_bytes(weights.at[0, 0, 0], pass_recv.at[0])
    for sub in (3, 1):
        level_late[sub].start()
        to_mate(3, sub, own_half, shared)
    await_bytes(weights.at[0, 0], pass_recv.at[3])
    for sub in (3, 1):
        to_mate(3, sub, all_of, unshared)
    await_bytes(weights.at[0, pl.ds(0, 2)], level_recv.at[0])
    for d in (1, 2):
        to_mate(d, 2 * d - 1 - plane)
    for index, sub in ((1, 2), (2, 0)):
        await_bytes(weights.at[0, 0], pass_recv.at[index])
        to_mate(3, sub)
    await_bytes(weights.at[0, 0, 0], level_recv.at[1])
    for sub in (3, 1):
        to_mate(3, sub, far_half, shared)

    await_bytes(gated_in.at[pl.ds(1, cols - 1)], gate_recv)
    await_bytes(final.at[pl.ds(0, rows * cols - 1)], piece_recv)
    loads["w_out"].wait()

    def share(d):
        outer = final[d * rows : (d + 1) * rows].reshape(rows * PACK, LANES).astype(f32).T
        outer = (outer * gated_in[d].reshape(groups * width, per_group).astype(f32)).astype(low)
        left = jnp.concatenate([outer[g * width : (g + 1) * width] for g in range(groups)], axis=1)
        right = jnp.concatenate([weights[d, :, g].reshape(per_group, depth) for g in range(groups)], axis=0)
        return jnp.dot(left, right, preferred_element_type=f32)

    await_bytes(weights.at[0], mate_recv.at[0])
    total[...] = share(0) + share(1) + share(2)
    await_bytes(weights.at[0, pl.ds(0, subs)], mate_recv.at[1])
    out_ref[...] = (total[...] + share(3)).astype(low)
    for role in range(2):
        await_bytes(send.at[role, others], row_send.at[role])

    @pl.when(has_below)
    def _():
        await_bytes(edge_out.at[0], edge_send.at[0])

    @pl.when(has_above)
    def _():
        await_bytes(edge_out.at[1], edge_send.at[1])

    await_bytes(gated.at[pl.ds(1, cols - 1)], gate_send)
    await_bytes(final.at[pl.ds(0, rows * cols - 1)], piece_send)
    await_bytes(weights.at[0, pl.ds(0, 6)], wide_send)
    await_bytes(weights.at[0, pl.ds(0, 5), 0], level_send)
    await_bytes(weights.at[0, pl.ds(0, 7), 0], pass_send)
    await_bytes(weights.at[pl.ds(0, 3), pl.ds(0, 4)], mate_send)


def fast_body(
    tokens, w_value, w_first, w_second, w_gate, conv_taps, filter_embed, filter_freq, filter_proj,
    filter_decay, skip_gain, w_out,
):
    rows, cols = lax.axis_size("row"), lax.axis_size("col")
    tok_rows = tokens.shape[1]
    chan_col = w_value.shape[1]
    chans = chan_col // rows
    groups = chans // PACK
    length = tok_rows * rows
    block_q = tok_rows // LANES
    length_q = length // LANES
    width = tok_rows // cols
    depth = w_out.shape[1]
    emb, hid = filter_embed.shape
    half = length_q + 1

    flat = tokens.reshape(tok_rows, tokens.shape[2])
    bands = (emb - 1) // 2
    index = np.arange(length)
    spot = index.astype(np.float32) / np.float32(length - 1)
    phase = 2.0 * np.pi * (np.outer(np.arange(1, bands + 1), index) % length) / length
    features = np.concatenate([spot[None, :], np.cos(phase), np.sin(phase)])
    emb_pad = -(-emb // 8) * 8
    features = np.concatenate([features, np.zeros((emb_pad - emb, length))]).astype(np.float32).astype(np.float64)
    high, middle, least = host_split(features)
    features = np.concatenate([high, middle, high, least, middle, high]).astype(jnp.bfloat16.dtype)
    own = np.arange(chan_col).reshape(rows, groups, PACK).transpose(1, 0, 2).reshape(-1)
    perm = np.zeros((chan_col, chan_col), np.float32)
    perm[own, np.arange(chan_col)] = 1.0
    lanes = chan_col // LANES
    fproj = filter_proj.reshape(hid, 2, 2, lanes, LANES).transpose(0, 1, 3, 2, 4).reshape(hid * 4 * lanes, LANES)
    w_rows = w_out.reshape(rows, groups, PACK, depth)

    first, last, twist, ahead, back = dft_tables(length)
    size = groups * LANES
    tables = jnp.asarray(
        np.concatenate([first, last[:, :size], last[:, size:], ahead, back, perm]).astype(np.float32)
    ).astype(jnp.bfloat16)
    operands = (
        flat, w_value, w_first, w_second, w_gate, w_rows, conv_taps, filter_embed, filter_freq.reshape(1, hid),
        fproj, filter_decay, skip_gain, jnp.asarray(features), tables, twist,
    )
    dma = pltpu.SemaphoreType.DMA
    f32, low = jnp.float32, jnp.bfloat16
    like = lambda array: pltpu.VMEM(array.shape, array.dtype)
    mixed = pl.pallas_call(
        functools.partial(mixer_kernel, rows, cols, width, emb),
        out_shape=pltpu.VMEM((width, depth), low),
        in_specs=[pl.BlockSpec(memory_space=pl.ANY)] * len(operands),
        out_specs=pl.BlockSpec(memory_space=pltpu.VMEM),
        scratch_shapes=[
            like(flat),
            pltpu.VMEM((4,) + w_value.shape, low),
            like(conv_taps),
            pltpu.VMEM((emb_pad, hid), f32),
            pltpu.VMEM((1, hid), f32),
            like(fproj),
            like(filter_decay),
            like(skip_gain),
            pltpu.VMEM(features.shape, low),
            like(tables),
            like(twist),
            pltpu.VMEM((2, rows, groups, block_q, PACK, LANES), low),
            pltpu.VMEM((2, rows, groups, block_q, PACK, LANES), low),
            pltpu.VMEM((2, 2, groups * half * PACK, LANES), f32),
            pltpu.VMEM((4, chans, length), low),
            pltpu.VMEM((16, chan_col), f32),
            pltpu.VMEM((8, groups, PACK, LANES), f32),
            pltpu.VMEM((cols, groups, width, rows * PACK), low),
            pltpu.VMEM((cols, groups, width, rows * PACK), low),
            pltpu.VMEM((2, 8, chan_col), f32),
            pltpu.VMEM((2, 8, chan_col), f32),
            pltpu.VMEM((length_q, groups, PACK, LANES), low),
            pltpu.VMEM((cols * rows, PACK, LANES), low),
            pltpu.VMEM((cols, rows, groups, PACK, depth), low),
            pltpu.VMEM((width, depth), f32),
            dma((len(operands) - 3,)),
            dma((2,)),
            dma((2,)),
            dma((2,)),
            dma((2,)),
            dma,
            dma,
            dma,
            dma,
            dma,
            dma((3,)),
            dma,
            dma((2,)),
            dma,
            dma((4,)),
            dma,
            dma((2,)),
            pltpu.SemaphoreType.REGULAR,
            pltpu.SemaphoreType.REGULAR,
        ],
        compiler_params=pltpu.CompilerParams(
            collective_id=0, has_side_effects=True, vmem_limit_bytes=40 * 1024 * 1024
        ),
        cost_estimate=pl.CostEstimate(flops=12_000_000_000, bytes_accessed=8_000_000, transcendentals=0),
    )(*[pltpu.with_memory_space_constraint(array, pltpu.HBM) for array in operands])
    return mixed[None]


def shaped_body(tokens, w_value, *rest):
    rows, cols = lax.axis_size("row"), lax.axis_size("col")
    seqs, tok_rows = tokens.shape[:2]
    chan_col = w_value.shape[1]
    chans = chan_col // rows
    width = tok_rows // cols
    fits = (
        seqs == 1
        and cols == 4
        and rows == 8
        and chans == 2 * PACK
        and tok_rows % LANES == 0
        and LANES == 2 * width
        and chan_col == 2 * LANES
        and rows * PACK == LANES
    )
    return (fast_body if fits else body)(tokens, w_value, *rest)


def solution(mesh):
    in_specs = (
        P(None, "row", None),
        P(None, "col"),
        P(None, "col"),
        P(None, "col"),
        P(None, "col"),
        P(None, None, "col"),
        P(),
        P(),
        P(None, None, None, "col"),
        P(None, None, "col"),
        P(None, "col"),
        P("col", None),
    )
    out_specs = P(None, ("row", "col"), None)
    return jax.shard_map(shaped_body, mesh=mesh, in_specs=in_specs, out_specs=out_specs, check_vma=False)
```

```python
import functools
import math

import jax
import jax.numpy as jnp
import numpy as np
from jax import lax
from jax.experimental import pallas as pl
from jax.experimental.pallas import tpu as pltpu
from jax.sharding import PartitionSpec as P

precise = lax.Precision.HIGHEST


def padded_2(array, sides, width):
    for axis, dim in sides:
        size, length = (lax.axis_size(axis), array.shape[dim])
        up = [(i, (i + 1) % size) for i in range(size - 1)]
        down = [(j, i) for i, j in up]
        last = lax.slice_in_dim(array, length - width, length, axis=dim)
        leading = lax.slice_in_dim(array, 0, width, axis=dim)
        before = lax.ppermute(last, axis, up)
        after = lax.ppermute(leading, axis, down)
        array = jnp.concatenate([before, array, after], axis=dim)
    return array


def split_length(total):
    factor = math.isqrt(total)
    while total % factor != 0:
        factor = factor - 1
    return (factor, total // factor)


def tables(outer, inner, total):
    first_index = jnp.arange(outer, dtype=jnp.int32)
    second_index = jnp.arange(inner, dtype=jnp.int32)
    scale = 2.0 * math.pi
    outer_angle = (first_index[:, None] * first_index[None, :] % outer).astype(jnp.float32) * (
        scale / outer
    )
    inner_angle = (second_index[:, None] * second_index[None, :] % inner).astype(jnp.float32) * (
        scale / inner
    )
    twist_angle = (first_index[:, None] * second_index[None, :] % total).astype(jnp.float32) * (
        scale / total
    )
    return (
        jnp.cos(outer_angle),
        jnp.sin(outer_angle),
        jnp.cos(inner_angle),
        jnp.sin(inner_angle),
        jnp.cos(twist_angle),
        jnp.sin(twist_angle),
    )


def forward_real(signal, table):
    outer_cos, outer_sin, inner_cos, inner_sin, twist_cos, twist_sin = table
    outer = outer_cos.shape[0]
    inner = inner_cos.shape[0]
    grid = signal.reshape(signal.shape[0], outer, inner)
    real_part = jnp.einsum("kq,cqp->ckp", outer_cos, grid, precision=precise)
    imag_part = -jnp.einsum("kq,cqp->ckp", outer_sin, grid, precision=precise)
    turned_real = real_part * twist_cos + imag_part * twist_sin
    turned_imag = imag_part * twist_cos - real_part * twist_sin
    spec_real = jnp.einsum("ckp,pj->ckj", turned_real, inner_cos, precision=precise) + jnp.einsum(
        "ckp,pj->ckj", turned_imag, inner_sin, precision=precise
    )
    spec_imag = jnp.einsum("ckp,pj->ckj", turned_imag, inner_cos, precision=precise) - jnp.einsum(
        "ckp,pj->ckj", turned_real, inner_sin, precision=precise
    )
    return (spec_real, spec_imag)


def inverse_real(spec_real, spec_imag, table):
    outer_cos, outer_sin, inner_cos, inner_sin, twist_cos, twist_sin = table
    total = outer_cos.shape[0] * inner_cos.shape[0]
    back_real = jnp.einsum("ckj,jp->ckp", spec_real, inner_cos, precision=precise) - jnp.einsum(
        "ckj,jp->ckp", spec_imag, inner_sin, precision=precise
    )
    back_imag = jnp.einsum("ckj,jp->ckp", spec_real, inner_sin, precision=precise) + jnp.einsum(
        "ckj,jp->ckp", spec_imag, inner_cos, precision=precise
    )
    turned_real = back_real * twist_cos - back_imag * twist_sin
    turned_imag = back_real * twist_sin + back_imag * twist_cos
    result = jnp.einsum("qk,ckp->cqp", outer_cos, turned_real, precision=precise) - jnp.einsum(
        "qk,ckp->cqp", outer_sin, turned_imag, precision=precise
    )
    return result.reshape(result.shape[0], total) / total


def channel_filters(
    length, row_index, chan_row, filter_embed, filter_freq, filter_proj, filter_decay
):
    bands = (filter_embed.shape[0] - 1) // 2
    index = jnp.arange(length, dtype=jnp.int32)
    spot = index.astype(jnp.float32) / (length - 1)
    freqs = jnp.arange(1, bands + 1, dtype=jnp.int32)
    phase = (index[:, None] * freqs[None, :] % length).astype(jnp.float32) * (
        2.0 * math.pi / length
    )
    features = jnp.concatenate([spot[:, None], jnp.cos(phase), jnp.sin(phase)], axis=1)
    hidden = jnp.sin(filter_freq[None, :] * jnp.dot(features, filter_embed, precision=precise))
    own_proj = lax.dynamic_slice_in_dim(filter_proj, row_index * chan_row, chan_row, 3)
    own_decay = lax.dynamic_slice_in_dim(filter_decay, row_index * chan_row, chan_row, 2)
    taps = jnp.dot(hidden, own_proj.reshape(own_proj.shape[0], 4 * chan_row), precision=precise)
    taps = jnp.transpose(taps).reshape(2, 2, chan_row, length)
    taps = taps * jnp.exp(-spot[None, None, None, :] * own_decay[:, :, :, None])
    cycles = []
    for order in range(2):
        behind = jnp.flip(taps[order, 1, :, 1:], axis=1)
        cycles.append(
            jnp.concatenate([taps[order, 0], jnp.zeros((chan_row, 1), jnp.float32), behind], axis=1)
        )
    return cycles


def body(
    tokens,
    w_value,
    w_first,
    w_second,
    w_gate,
    conv_taps,
    filter_embed,
    filter_freq,
    filter_proj,
    filter_decay,
    skip_gain,
    w_out,
):
    seq_count = tokens.shape[0]
    tok_rows = tokens.shape[1]
    chan_col = w_value.shape[1]
    row_count = lax.axis_size("row")
    chan_row = chan_col // row_count
    length = tok_rows * row_count
    row_index = lax.axis_index("row")
    proj = jnp.concatenate(
        [
            jnp.dot(tokens, w_value, preferred_element_type=jnp.float32),
            jnp.dot(tokens, w_first, preferred_element_type=jnp.float32),
            jnp.dot(tokens, w_second, preferred_element_type=jnp.float32),
        ],
        axis=2,
    ).astype(jnp.bfloat16)
    gate = jnp.dot(tokens, w_gate, preferred_element_type=jnp.float32).astype(jnp.bfloat16)
    padded = padded_2(proj, (("row", 1),), 1).astype(jnp.float32)
    weights = conv_taps.reshape(3, 3 * chan_col)
    short = padded[:, :-2] * weights[0] + padded[:, 1:-1] * weights[1] + padded[:, 2:] * weights[2]
    value_rows = jnp.transpose(short[:, :, :chan_col], (0, 2, 1))
    first_rows = jnp.transpose(short[:, :, chan_col : 2 * chan_col], (0, 2, 1))
    second_rows = jnp.transpose(short[:, :, 2 * chan_col :], (0, 2, 1))
    outer, inner = split_length(2 * length)
    table = tables(outer, inner, 2 * length)
    cycles = channel_filters(
        length, row_index, chan_row, filter_embed, filter_freq, filter_proj, filter_decay
    )
    spectra = [forward_real(cycle, table) for cycle in cycles]
    own_gain = lax.dynamic_slice_in_dim(skip_gain, row_index * chan_row, chan_row, 1)

    def convolve(signal, order):
        flat = signal.reshape(seq_count * chan_row, length)
        padded_signal = jnp.concatenate([flat, jnp.zeros_like(flat)], axis=1)
        sig_real, sig_imag = forward_real(padded_signal, table)
        sig_real = sig_real.reshape(seq_count, chan_row, outer, inner)
        sig_imag = sig_imag.reshape(seq_count, chan_row, outer, inner)
        filt_real, filt_imag = spectra[order]
        prod_real = sig_real * filt_real[None] - sig_imag * filt_imag[None]
        prod_imag = sig_real * filt_imag[None] + sig_imag * filt_real[None]
        result = inverse_real(
            prod_real.reshape(seq_count * chan_row, outer, inner),
            prod_imag.reshape(seq_count * chan_row, outer, inner),
            table,
        )[:, :length]
        return result.reshape(seq_count, chan_row, length) + own_gain[order][None, :, None] * signal

    value_chan, first_chan = (
        lax.all_to_all(value_rows, "row", split_axis=1, concat_axis=2, tiled=True),
        lax.all_to_all(first_rows, "row", split_axis=1, concat_axis=2, tiled=True),
    )
    inner_chan = first_chan * convolve(value_chan, 0)
    second_conv = lax.all_to_all(
        convolve(inner_chan, 1), "row", split_axis=2, concat_axis=1, tiled=True
    )
    outer_rows = (
        jnp.transpose(second_rows * second_conv, (0, 2, 1)) * jax.nn.silu(gate.astype(jnp.float32))
    ).astype(jnp.bfloat16)
    own_rows = tok_rows // lax.axis_size("col")
    flat_rows = jnp.transpose(outer_rows, (1, 0, 2)).reshape(tok_rows * seq_count, chan_col)
    summed = lax.psum_scatter(
        jnp.dot(flat_rows, w_out, preferred_element_type=jnp.float32).astype(jnp.bfloat16),
        "col",
        scatter_dimension=0,
        tiled=True,
    ).astype(jnp.float32)
    summed = jnp.transpose(summed.reshape(own_rows, seq_count, w_out.shape[1]), (1, 0, 2))
    return summed.astype(jnp.bfloat16)


LANES = 128
PACK = 16


def dft_tables(length):
    filled = length // LANES
    outer = 2 * filled
    total = outer * LANES
    half = filled + 1
    eye = np.eye(PACK)
    q, k, p = np.arange(filled), np.arange(half), np.arange(LANES)
    inside = k[1:-1]
    angle = 2.0 * np.pi * (np.outer(k, q) % outer) / outer
    first = np.concatenate([np.kron(np.cos(angle), eye), np.kron(-np.sin(angle)[inside], eye)], axis=0)
    weight = np.where((k == 0) | (k == filled), 1.0, 2.0) / total
    last = np.concatenate(
        [
            np.kron(np.cos(angle).T * weight, eye),
            np.kron((-np.sin(angle).T * weight)[:, inside], eye),
        ],
        axis=1,
    )
    turn = 2.0 * np.pi * np.outer(k, p) / total
    twist = np.stack([np.cos(turn), np.sin(turn)])[:, :, None, :]
    twist = np.broadcast_to(twist, (2, half, 8, LANES))
    angle = 2.0 * np.pi * (np.outer(p, p) % LANES) / LANES
    cos, sin = np.cos(angle), np.sin(angle)
    ahead = np.block([[cos, -sin], [sin, cos]])
    back = np.block([[cos, sin], [-sin, cos]])
    return first, last, jnp.asarray(twist.astype(np.float32)), ahead, back


def split_bf16(array):
    high = array.astype(jnp.bfloat16).astype(jnp.float32)
    middle = (array - high).astype(jnp.bfloat16).astype(jnp.float32)
    low = (array - high - middle).astype(jnp.bfloat16).astype(jnp.float32)
    return high, middle, low


def host_split(array):
    low_type = jnp.bfloat16.dtype
    high = array.astype(low_type).astype(np.float64)
    middle = (array - high).astype(low_type).astype(np.float64)
    low = (array - high - middle).astype(low_type).astype(np.float64)
    return high, middle, low


def flip(value, bits):
    bit = 1
    while bit <= bits:
        if bits & bit:
            value = value + bit - 2 * bit * lax.rem(lax.div(value, bit), 2)
        bit *= 2
    return value


def mixer_kernel(
    rows, cols, width, emb,
    tokens_hbm, w_value_hbm, w_first_hbm, w_second_hbm, w_gate_hbm, w_out_hbm, conv_hbm, embed_hbm, freq_hbm,
    proj_hbm, decay_hbm, gain_hbm, features_hbm, tables_hbm, twist_hbm,
    out_ref,
    tokens_ref, w_refs, conv_ref, embed_ref, freq_ref, fproj_ref, decay_ref, gain_ref, features_ref, tables_ref,
    twist_ref,
    send, recv, spectra, taps_ref, stack_ref, coef_ref, gated, edge_out, edge_in, back_send, back_in, outer_send, outer_in, weights, total,
    load_sem, row_send, row_recv, edge_send, edge_recv, piece_send, piece_recv, outer_sem,
    wide_send, wide_recv, level_send, level_recv, pass_send, pass_recv, mate_send, mate_recv, told,
):
    my_row = lax.axis_index("row")
    my_col = lax.axis_index("col")
    mesh_id = pl.DeviceIdType.MESH
    groups = recv.shape[2]
    chans = groups * PACK
    tok_rows = tokens_ref.shape[0]
    block_q = tok_rows // LANES
    length_q = rows * block_q
    length = tok_rows * rows
    half = length_q + 1
    hid = freq_ref.shape[1]
    depth = weights.shape[4]
    f32, low = jnp.float32, jnp.bfloat16

    def remote(src, dst, send_sem, recv_sem, row, col):
        return pltpu.make_async_remote_copy(
            src_ref=src, dst_ref=dst, send_sem=send_sem, recv_sem=recv_sem,
            device_id=(row, col), device_id_type=mesh_id,
        )

    side = lax.rem(my_row, 2)
    mate = flip(my_row, 1)
    low_row = my_row - side
    barrier = pltpu.get_barrier_semaphore()

    def greet(row, col):
        pl.semaphore_signal(barrier, inc=1, device_id=(row, col), device_id_type=mesh_id)

    near = (1, 2)
    greet(mate, my_col)
    for d in near:
        greet(low_row, flip(my_col, d))
    for d in range(1, rows // 2):
        greet(flip(low_row, 2 * d) + 1, my_col)

    def heard(own_side):
        others = 2 * len(near) + 1 if own_side == 0 else rows - 1

        @pl.when(side == own_side)
        def _():
            pl.semaphore_wait(barrier, others)
            pl.semaphore_signal(told, inc=1, device_id=(mate, my_col), device_id_type=mesh_id)

        @pl.when(side != own_side)
        def _():
            pl.semaphore_wait(told, 1)

    def await_bytes(ref, sem):
        pltpu.make_async_copy(ref, ref, sem).wait()

    token_sem, weight_sem, half_sem = load_sem.at[0], load_sem.at[1], load_sem.at[2]
    half_rows = lambda half: pl.ds(half * (rows // 2), rows // 2)
    own_rows = pltpu.make_async_copy(w_out_hbm.at[half_rows(side)], weights.at[0, half_rows(side)], half_sem)
    own_rows.start()
    pltpu.make_async_copy(tokens_hbm, tokens_ref, token_sem).start()
    pltpu.make_async_copy(w_value_hbm, w_refs.at[0], token_sem).start()
    loads = {}
    for name, src, dst in (
        ("embed", embed_hbm, embed_ref.at[pl.ds(0, emb)]),
        ("freq", freq_hbm, freq_ref),
        ("conv", conv_hbm, conv_ref),
        ("gain", gain_hbm, gain_ref),
        ("decay", decay_hbm, decay_ref),
        ("fproj", proj_hbm, fproj_ref),
        ("features", features_hbm, features_ref),
        ("tables", tables_hbm, tables_ref),
        ("twist", twist_hbm, twist_ref),
        ("w_out", w_out_hbm.at[half_rows(1 - side)], weights.at[0, half_rows(1 - side)]),
    ):
        loads[name] = pltpu.make_async_copy(src, dst, load_sem.at[3 + len(loads)])
    for role, w_hbm in ((2, w_second_hbm), (1, w_first_hbm), (3, w_gate_hbm)):
        pltpu.make_async_copy(w_hbm, w_refs.at[role], weight_sem).start()
    for copy in loads.values():
        copy.start()

    plane = lax.rem(lax.div(my_row, 2), 2)
    subs = rows // 2
    row_of = lambda sub: side * subs + sub

    def wide_copy(group, d, sub):
        return remote(
            weights.at[0, row_of(sub)], weights.at[d, row_of(sub)],
            wide_send, wide_recv.at[group], my_row, flip(my_col, d),
        )

    wide = {
        (d, sub): wide_copy(group, d, sub + plane if group == 0 else sub)
        for group, d, sub in ((0, 1, 0), (0, 2, 2), (1, 1, 3), (1, 2, 0), (2, 1, 2), (2, 2, 1))
    }

    def there(part, send_sem, recv_sem, row):
        return remote(part, part, send_sem, recv_sem, row, my_col)

    levels = [
        there(weights.at[d, row_of(2 * d - 2 + plane)], level_send, level_recv.at[d - 1], flip(my_row, 2)) for d in (1, 2)
    ]
    def pass_copy(index, d, sub):
        return remote(
            weights.at[d, row_of(sub)], weights.at[3, row_of(sub)],
            pass_send, pass_recv.at[index], my_row, flip(my_col, 3 - d),
        )

    passed = {(d, sub): pass_copy(index, d, sub) for index, d, sub in ((0, 1, 3), (0, 2, 0), (1, 1, 2), (1, 2, 1))}

    def to_mate(d, sub):
        there(weights.at[d, row_of(sub)], mate_send, mate_recv.at[d // 3], mate).start()

    def chunk(count):
        return weights.at[0, pl.ds(0, count)]

    def wide_arrived(group, keys):
        await_bytes(chunk(len(keys)), wide_recv.at[group])
        for d, sub in keys:
            if (d, sub) in passed:
                passed[d, sub].start()
            to_mate(d, sub + plane if group == 0 else sub)

    far_first = sorted(range(1, rows), key=lambda d: -(d & (rows // 2)))

    def row_copies(role):
        return [
            remote(
                send.at[role, flip(my_row, d)], recv.at[role, my_row],
                row_send.at[role], row_recv.at[role], flip(my_row, d), my_col,
            )
            for d in far_first
        ]

    def project(role):
        return jnp.dot(tokens_ref[...], w_refs[role], preferred_element_type=f32)

    def project_turned(role):
        result = project(role).T
        for q in range(block_q):
            send[role, :, :, q] = (
                result[:, q * LANES : (q + 1) * LANES].reshape(rows, groups, PACK, LANES).astype(low)
            )

    value_copies, first_copies = row_copies(0), row_copies(1)

    own_rows.wait()
    heard(0)
    for copy in wide.values():
        copy.start()
    await_bytes(w_refs.at[pl.ds(0, 2)], token_sem)
    project_turned(0)
    heard(1)
    for copy in value_copies:
        copy.start()
    recv[0, my_row] = send[0, my_row]

    await_bytes(w_refs.at[pl.ds(1, 3)], weight_sem)
    second = project(2).astype(low).astype(f32)
    edge_out[0] = jnp.broadcast_to(second[tok_rows - 1 :], edge_out.shape[1:])
    edge_out[1] = jnp.broadcast_to(second[:1], edge_out.shape[1:])
    def edge_copy(index, step):
        return remote(edge_out.at[index], edge_in.at[index], edge_send.at[index], edge_recv.at[index], my_row + step, my_col)

    has_above, has_below = my_row > 0, my_row < rows - 1

    @pl.when(has_below)
    def _():
        edge_copy(0, 1).start()

    @pl.when(has_above)
    def _():
        edge_copy(1, -1).start()

    project_turned(1)
    for copy in first_copies:
        copy.start()
    recv[1, my_row] = send[1, my_row]
    gate = project(3).astype(low).astype(f32)
    loads["conv"].wait()

    loads["gain"].wait()
    loads["decay"].wait()
    stack_ref[...] = jnp.zeros_like(stack_ref)
    for j in range(3):
        stack_ref[j : j + 1] = conv_ref[j, 0:1]
        stack_ref[3 + j : 4 + j] = conv_ref[j, 1:2]
    stack_ref[6:8] = gain_ref[...]
    stack_ref[8:10] = decay_ref[0]
    stack_ref[10:12] = decay_ref[1]
    shape = (chans, stack_ref.shape[1])
    picks = lax.broadcasted_iota(jnp.int32, shape, 1) == lax.broadcasted_iota(jnp.int32, shape, 0) + my_row * chans
    picks = jnp.where(picks, 1.0, 0.0)
    contract_last = (((1,), (1,)), ((), ()))
    own = lax.dot_general(picks, stack_ref[...], contract_last, precision=precise, preferred_element_type=f32)
    for k in range(8):
        coef_ref[k] = jnp.broadcast_to(own[:, k : k + 1], (chans, LANES)).reshape(groups, PACK, LANES)

    loads["embed"].wait()
    loads["freq"].wait()
    embed = embed_ref[...] * (freq_ref[...] * (1.0 / math.pi))
    embed = jnp.where(lax.broadcasted_iota(jnp.int32, embed.shape, 0) < emb, embed, 0.0)
    high, middle, least = split_bf16(embed)
    stacked = jnp.concatenate([high, high, middle, high, middle, least], axis=0).astype(low)
    loads["features"].wait()
    turns = lax.dot_general(stacked, features_ref[...], (((0,), (0,)), ((), ())), preferred_element_type=f32)
    whole = jnp.floor(turns + 0.5)
    rest = turns - whole
    sign = 1.0 - 2.0 * (whole - 2.0 * jnp.floor(whole * 0.5))
    square = rest * rest
    series = jnp.full_like(square, -(math.pi**11) / math.factorial(11))
    for n in (9, 7, 5, 3, 1):
        series = series * square + (-1) ** (n // 2) * math.pi**n / math.factorial(n)
    hidden = (series * (rest * sign)).astype(low)
    loads["fproj"].wait()
    pieces = []
    picks_low = picks.astype(low)
    halves = 2
    for od in range(4):
        parts = [
            fproj_ref[pl.ds((od // 2) * 2 * halves + j * 2 + od % 2, hid, stride=4 * halves), :]
            for j in range(halves)
        ]
        block = jnp.concatenate(parts, axis=1).astype(low)
        pieces.append(lax.dot_general(picks_low, block, contract_last, preferred_element_type=f32).astype(low))
    taps = jnp.dot(jnp.concatenate(pieces, axis=0), hidden, preferred_element_type=f32)
    lag = lax.broadcasted_iota(jnp.int32, (1, length), 1)
    spot = lag.astype(f32) / (length - 1)
    for od in range(4):
        block = taps[od * chans : (od + 1) * chans] * jnp.exp(-own[:, 8 + od : 9 + od] * spot)
        if od % 2 == 1:
            block = jnp.where(lag == 0, 0.0, block)
        taps_ref[od] = block.astype(low)

    size = LANES * groups
    first_ref, last_ref, ahead_ref, back_ref = (
        tables_ref.at[pl.ds(start * size, count * size)]
        for start, count in ((0, 2), (2, 2), (4, 1), (5, 1))
    )

    def wide_twist(index):
        return twist_ref[index].reshape(half, 1, 8, LANES)

    def ahead(signal):
        mid = jnp.dot(first_ref[...], signal, preferred_element_type=f32)
        blank = jnp.zeros((PACK, LANES), f32)
        blocks = []
        for g in range(groups):
            lanes = slice(g * LANES, (g + 1) * LANES)
            real = mid[: half * PACK, lanes].reshape(half, 2, 8, LANES)
            imag = jnp.concatenate([blank, mid[half * PACK :, lanes], blank], axis=0).reshape(half, 2, 8, LANES)
            cos, sin = wide_twist(0), wide_twist(1)
            blocks.append(
                jnp.concatenate(
                    [
                        (real * cos + imag * sin).reshape(half * PACK, LANES),
                        (imag * cos - real * sin).reshape(half * PACK, LANES),
                    ],
                    axis=1,
                ).astype(low)
            )
        return jnp.dot(jnp.concatenate(blocks, axis=0), ahead_ref[...], preferred_element_type=f32)

    def convolve(signal, order):
        spec = ahead(signal.astype(low))
        real, imag = spec[:, :LANES], spec[:, LANES:]
        filt_real, filt_imag = spectra[order, 0], spectra[order, 1]
        prod = jnp.concatenate(
            [real * filt_real - imag * filt_imag, real * filt_imag + imag * filt_real], axis=1
        ).astype(low)
        mid = jnp.dot(prod, back_ref[...], preferred_element_type=f32)
        blocks = []
        for g in range(groups):
            span = slice(g * half * PACK, (g + 1) * half * PACK)
            real = mid[span, :LANES].reshape(half, 2, 8, LANES)
            imag = mid[span, LANES:].reshape(half, 2, 8, LANES)
            cos, sin = wide_twist(0), wide_twist(1)
            turned_real = (real * cos - imag * sin).reshape(half * PACK, LANES)
            turned_imag = (real * sin + imag * cos)[1:-1].reshape((half - 2) * PACK, LANES)
            blocks.append(jnp.concatenate([turned_real, turned_imag], axis=0).astype(low))
        last = jnp.concatenate([last_ref[:size], last_ref[size:]], axis=1)
        result = jnp.dot(last, jnp.concatenate(blocks, axis=1), preferred_element_type=f32)
        gain = jnp.concatenate([coef_ref[6 + order, g] for g in range(groups)], axis=1)
        shape = (length_q, PACK, groups * LANES)
        return (result.reshape(shape) + gain[None] * signal.reshape(shape)).reshape(signal.shape)

    loads["tables"].wait()
    loads["twist"].wait()
    for order in range(2):
        for direction in range(2):
            od = 2 * order + direction
            signal = jnp.concatenate(
                [
                    jnp.concatenate(
                        [
                            taps_ref[od, g * PACK : (g + 1) * PACK, q * LANES : (q + 1) * LANES]
                            for q in range(length_q)
                        ],
                        axis=0,
                    )
                    for g in range(groups)
                ],
                axis=1,
            )
            spec = ahead(signal)
            if direction == 0:
                spectra[order, 0] = spec[:, :LANES]
                spectra[order, 1] = spec[:, LANES:]
            else:
                spectra[order, 0] += spec[:, :LANES]
                spectra[order, 1] -= spec[:, LANES:]

    wide_arrived(0, ((1, 0), (2, 2)))
    levels[0].start()


    @pl.when(has_above)
    def _():
        await_bytes(edge_in.at[0], edge_recv.at[0])

    @pl.when(has_below)
    def _():
        await_bytes(edge_in.at[1], edge_recv.at[1])

    line = lax.broadcasted_iota(jnp.int32, second.shape, 0)
    above = jnp.where(has_above, edge_in[0, 0:1], 0.0)
    below = jnp.where(has_below, edge_in[1, 0:1], 0.0)
    before = jnp.where(line == 0, above, pltpu.roll(second, 1, 0))
    after = jnp.where(line == tok_rows - 1, below, pltpu.roll(second, tok_rows - 1, 0))
    short_second = before * conv_ref[0, 2:3] + second * conv_ref[1, 2:3] + after * conv_ref[2, 2:3]
    both = short_second * (gate / (1.0 + jnp.exp(-gate)))
    for tile in range(halves):
        gated[tile] = both[:, tile * LANES : (tile + 1) * LANES]

    def short(role):
        blocks = []
        for g in range(groups):
            here = recv[role, :, g].reshape(length_q * PACK, LANES).astype(f32)
            size = here.shape[0]
            lane = lax.broadcasted_iota(jnp.int32, here.shape, 1)
            blank = jnp.zeros((PACK, LANES), f32)
            before = pltpu.roll(here, 1, 1)
            before = jnp.where(lane == 0, jnp.concatenate([blank, before[: size - PACK]], axis=0), before)
            after = pltpu.roll(here, LANES - 1, 1)
            after = jnp.where(lane == LANES - 1, jnp.concatenate([after[PACK:], blank], axis=0), after)
            shape = (length_q, PACK, LANES)
            w = lambda j: coef_ref[3 * role + j, g][None]
            result = before.reshape(shape) * w(0) + here.reshape(shape) * w(1) + after.reshape(shape) * w(2)
            blocks.append(result.reshape(size, LANES))
        return jnp.concatenate(blocks, axis=1)

    others = pl.ds(0, rows - 1)
    await_bytes(recv.at[0, others], row_recv.at[0])
    conv = convolve(short(0), 0)

    wide_arrived(1, ((1, 3), (2, 0)))
    await_bytes(recv.at[1, others], row_recv.at[1])
    conv = convolve(short(1) * conv, 1)

    for g in range(groups):
        back_send[:, :, g] = (
            conv[:, g * LANES : (g + 1) * LANES].reshape(rows, block_q, PACK, LANES).astype(low)
        )
    for d in far_first:
        peer = flip(my_row, d)
        remote(back_send.at[peer], back_in.at[my_row], piece_send, piece_recv.at[2 * d // rows], peer, my_col).start()
    levels[1].start()
    back_in[my_row] = back_send[my_row]

    wide_arrived(2, ((1, 2), (2, 1)))

    per_tile = rows // halves
    near_tile = lax.div(my_row, per_tile)

    def finish(tile, far):
        count = per_tile if far else per_tile - 1
        await_bytes(back_in.at[pl.ds(0, count)], piece_recv.at[far])
        for q in range(block_q):
            block = back_in[pl.ds(tile * per_tile, per_tile), q].reshape(LANES, LANES).astype(f32).T
            block = (block * gated[tile, q * LANES : (q + 1) * LANES]).astype(low)
            spots = LANES // width
            outer_send[far, q * spots : (q + 1) * spots] = block.reshape(spots, width, LANES)
        for d in (3, 1, 2):
            peer = flip(my_col, d)
            remote(
                outer_send.at[far, peer], outer_in.at[far, d], outer_sem.at[0], outer_sem.at[1 + far], my_row, peer
            ).start()
        outer_in[far, 0] = outer_send[far, my_col]

    def share(tile, far):
        await_bytes(outer_in.at[far, pl.ds(1, cols - 1)], outer_sem.at[1 + far])
        left = jnp.concatenate([outer_in[far, d] for d in range(cols)], axis=1)
        right = jnp.concatenate(
            [weights[d, pl.ds(tile * per_tile, per_tile)].reshape(LANES, depth) for d in range(cols)], axis=0
        )
        return jnp.dot(left, right, preferred_element_type=f32)

    finish(near_tile, 0)
    await_bytes(chunk(2), pass_recv.at[0])
    to_mate(3, 0)
    to_mate(3, 3)
    await_bytes(chunk(1), level_recv.at[0])
    to_mate(1, 1 - plane)
    finish(1 - near_tile, 1)
    await_bytes(chunk(2), pass_recv.at[1])
    to_mate(3, 2)
    to_mate(3, 1)
    await_bytes(chunk(1), level_recv.at[1])
    to_mate(2, 3 - plane)

    loads["w_out"].wait()
    await_bytes(weights.at[0], mate_recv.at[0])
    await_bytes(chunk(subs), mate_recv.at[1])
    total[...] = share(near_tile, 0)
    out_ref[...] = (total[...] + share(1 - near_tile, 1)).astype(low)

    for role in range(2):
        await_bytes(send.at[role, others], row_send.at[role])

    @pl.when(has_below)
    def _():
        await_bytes(edge_out.at[0], edge_send.at[0])

    @pl.when(has_above)
    def _():
        await_bytes(edge_out.at[1], edge_send.at[1])

    await_bytes(back_send.at[others], piece_send)
    await_bytes(outer_send.at[pl.ds(0, 2), pl.ds(0, cols - 1)], outer_sem.at[0])
    await_bytes(chunk(6), wide_send)
    await_bytes(chunk(2), level_send)
    await_bytes(chunk(4), pass_send)
    await_bytes(weights.at[pl.ds(0, 3), pl.ds(0, 4)], mate_send)


def fast_body(
    tokens, w_value, w_first, w_second, w_gate, conv_taps, filter_embed, filter_freq, filter_proj,
    filter_decay, skip_gain, w_out,
):
    rows, cols = lax.axis_size("row"), lax.axis_size("col")
    tok_rows = tokens.shape[1]
    chan_col = w_value.shape[1]
    chans = chan_col // rows
    groups = chans // PACK
    length = tok_rows * rows
    block_q = tok_rows // LANES
    length_q = length // LANES
    width = tok_rows // cols
    depth = w_out.shape[1]
    emb, hid = filter_embed.shape
    half = length_q + 1

    flat = tokens.reshape(tok_rows, tokens.shape[2])
    bands = (emb - 1) // 2
    index = np.arange(length)
    spot = index.astype(np.float32) / np.float32(length - 1)
    phase = 2.0 * np.pi * (np.outer(np.arange(1, bands + 1), index) % length) / length
    features = np.concatenate([spot[None, :], np.cos(phase), np.sin(phase)])
    emb_pad = -(-emb // 8) * 8
    features = np.concatenate([features, np.zeros((emb_pad - emb, length))]).astype(np.float32).astype(np.float64)
    high, middle, least = host_split(features)
    features = np.concatenate([high, middle, high, least, middle, high]).astype(jnp.bfloat16.dtype)
    lanes = chan_col // LANES
    fproj = filter_proj.reshape(hid, 2, 2, lanes, LANES).transpose(0, 1, 3, 2, 4).reshape(hid * 4 * lanes, LANES)
    w_rows = w_out.reshape(rows, groups, PACK, depth)

    first, last, twist, ahead, back = dft_tables(length)
    size = groups * LANES
    tables = jnp.asarray(
        np.concatenate([first, last[:, :size], last[:, size:], ahead, back]).astype(np.float32)
    ).astype(jnp.bfloat16)
    operands = (
        flat, w_value, w_first, w_second, w_gate, w_rows, conv_taps, filter_embed, filter_freq.reshape(1, hid),
        fproj, filter_decay, skip_gain, jnp.asarray(features), tables, twist,
    )
    dma = pltpu.SemaphoreType.DMA
    f32, low = jnp.float32, jnp.bfloat16
    like = lambda array: pltpu.VMEM(array.shape, array.dtype)
    mixed = pl.pallas_call(
        functools.partial(mixer_kernel, rows, cols, width, emb),
        out_shape=pltpu.VMEM((width, depth), low),
        in_specs=[pl.BlockSpec(memory_space=pl.ANY)] * len(operands),
        out_specs=pl.BlockSpec(memory_space=pltpu.VMEM),
        scratch_shapes=[
            like(flat),
            pltpu.VMEM((4,) + w_value.shape, low),
            like(conv_taps),
            pltpu.VMEM((emb_pad, hid), f32),
            pltpu.VMEM((1, hid), f32),
            like(fproj),
            like(filter_decay),
            like(skip_gain),
            pltpu.VMEM(features.shape, low),
            like(tables),
            like(twist),
            pltpu.VMEM((2, rows, groups, block_q, PACK, LANES), low),
            pltpu.VMEM((2, rows, groups, block_q, PACK, LANES), low),
            pltpu.VMEM((2, 2, groups * half * PACK, LANES), f32),
            pltpu.VMEM((4, chans, length), low),
            pltpu.VMEM((16, chan_col), f32),
            pltpu.VMEM((8, groups, PACK, LANES), f32),
            pltpu.VMEM((lanes, tok_rows, LANES), f32),
            pltpu.VMEM((2, 8, chan_col), f32),
            pltpu.VMEM((2, 8, chan_col), f32),
            pltpu.VMEM((rows, block_q, groups, PACK, LANES), low),
            pltpu.VMEM((rows, block_q, groups, PACK, LANES), low),
            pltpu.VMEM((2, cols, width, LANES), low),
            pltpu.VMEM((2, cols, width, LANES), low),
            pltpu.VMEM((cols, rows, groups, PACK, depth), low),
            pltpu.VMEM((width, depth), f32),
            dma((len(operands) - 2,)),
            dma((2,)),
            dma((2,)),
            dma((2,)),
            dma((2,)),
            dma,
            dma((2,)),
            dma((3,)),
            dma,
            dma((3,)),
            dma,
            dma((2,)),
            dma,
            dma((2,)),
            dma,
            dma((2,)),
            pltpu.SemaphoreType.REGULAR,
        ],
        compiler_params=pltpu.CompilerParams(
            collective_id=0, has_side_effects=True, vmem_limit_bytes=40 * 1024 * 1024
        ),
        cost_estimate=pl.CostEstimate(flops=12_000_000_000, bytes_accessed=8_000_000, transcendentals=0),
    )(*[pltpu.with_memory_space_constraint(array, pltpu.HBM) for array in operands])
    return mixed[None]


def shaped_body(tokens, w_value, *rest):
    rows, cols = lax.axis_size("row"), lax.axis_size("col")
    seqs, tok_rows = tokens.shape[:2]
    chan_col = w_value.shape[1]
    chans = chan_col // rows
    width = tok_rows // cols
    fits = (
        seqs == 1
        and cols == 4
        and rows == 8
        and chans == 2 * PACK
        and tok_rows % LANES == 0
        and LANES == 2 * width
        and chan_col == 2 * LANES
        and rows * PACK == LANES
    )
    return (fast_body if fits else body)(tokens, w_value, *rest)


def solution(mesh):
    in_specs = (
        P(None, "row", None),
        P(None, "col"),
        P(None, "col"),
        P(None, "col"),
        P(None, "col"),
        P(None, None, "col"),
        P(),
        P(),
        P(None, None, None, "col"),
        P(None, None, "col"),
        P(None, "col"),
        P("col", None),
    )
    out_specs = P(None, ("row", "col"), None)
    return jax.shard_map(shaped_body, mesh=mesh, in_specs=in_specs, out_specs=out_specs, check_vma=False)
```

```python
import functools
import math

import jax
import jax.numpy as jnp
import numpy as np
from jax import lax
from jax.experimental import pallas as pl
from jax.experimental.pallas import tpu as pltpu
from jax.sharding import PartitionSpec as P

precise = lax.Precision.HIGHEST


def padded_2(array, sides, width):
    for axis, dim in sides:
        size, length = (lax.axis_size(axis), array.shape[dim])
        up = [(i, (i + 1) % size) for i in range(size - 1)]
        down = [(j, i) for i, j in up]
        last = lax.slice_in_dim(array, length - width, length, axis=dim)
        leading = lax.slice_in_dim(array, 0, width, axis=dim)
        before = lax.ppermute(last, axis, up)
        after = lax.ppermute(leading, axis, down)
        array = jnp.concatenate([before, array, after], axis=dim)
    return array


def split_length(total):
    factor = math.isqrt(total)
    while total % factor != 0:
        factor = factor - 1
    return (factor, total // factor)


def tables(outer, inner, total):
    first_index = jnp.arange(outer, dtype=jnp.int32)
    second_index = jnp.arange(inner, dtype=jnp.int32)
    scale = 2.0 * math.pi
    outer_angle = (first_index[:, None] * first_index[None, :] % outer).astype(jnp.float32) * (
        scale / outer
    )
    inner_angle = (second_index[:, None] * second_index[None, :] % inner).astype(jnp.float32) * (
        scale / inner
    )
    twist_angle = (first_index[:, None] * second_index[None, :] % total).astype(jnp.float32) * (
        scale / total
    )
    return (
        jnp.cos(outer_angle),
        jnp.sin(outer_angle),
        jnp.cos(inner_angle),
        jnp.sin(inner_angle),
        jnp.cos(twist_angle),
        jnp.sin(twist_angle),
    )


def forward_real(signal, table):
    outer_cos, outer_sin, inner_cos, inner_sin, twist_cos, twist_sin = table
    outer = outer_cos.shape[0]
    inner = inner_cos.shape[0]
    grid = signal.reshape(signal.shape[0], outer, inner)
    real_part = jnp.einsum("kq,cqp->ckp", outer_cos, grid, precision=precise)
    imag_part = -jnp.einsum("kq,cqp->ckp", outer_sin, grid, precision=precise)
    turned_real = real_part * twist_cos + imag_part * twist_sin
    turned_imag = imag_part * twist_cos - real_part * twist_sin
    spec_real = jnp.einsum("ckp,pj->ckj", turned_real, inner_cos, precision=precise) + jnp.einsum(
        "ckp,pj->ckj", turned_imag, inner_sin, precision=precise
    )
    spec_imag = jnp.einsum("ckp,pj->ckj", turned_imag, inner_cos, precision=precise) - jnp.einsum(
        "ckp,pj->ckj", turned_real, inner_sin, precision=precise
    )
    return (spec_real, spec_imag)


def inverse_real(spec_real, spec_imag, table):
    outer_cos, outer_sin, inner_cos, inner_sin, twist_cos, twist_sin = table
    total = outer_cos.shape[0] * inner_cos.shape[0]
    back_real = jnp.einsum("ckj,jp->ckp", spec_real, inner_cos, precision=precise) - jnp.einsum(
        "ckj,jp->ckp", spec_imag, inner_sin, precision=precise
    )
    back_imag = jnp.einsum("ckj,jp->ckp", spec_real, inner_sin, precision=precise) + jnp.einsum(
        "ckj,jp->ckp", spec_imag, inner_cos, precision=precise
    )
    turned_real = back_real * twist_cos - back_imag * twist_sin
    turned_imag = back_real * twist_sin + back_imag * twist_cos
    result = jnp.einsum("qk,ckp->cqp", outer_cos, turned_real, precision=precise) - jnp.einsum(
        "qk,ckp->cqp", outer_sin, turned_imag, precision=precise
    )
    return result.reshape(result.shape[0], total) / total


def channel_filters(
    length, row_index, chan_row, filter_embed, filter_freq, filter_proj, filter_decay
):
    bands = (filter_embed.shape[0] - 1) // 2
    index = jnp.arange(length, dtype=jnp.int32)
    spot = index.astype(jnp.float32) / (length - 1)
    freqs = jnp.arange(1, bands + 1, dtype=jnp.int32)
    phase = (index[:, None] * freqs[None, :] % length).astype(jnp.float32) * (
        2.0 * math.pi / length
    )
    features = jnp.concatenate([spot[:, None], jnp.cos(phase), jnp.sin(phase)], axis=1)
    hidden = jnp.sin(filter_freq[None, :] * jnp.dot(features, filter_embed, precision=precise))
    own_proj = lax.dynamic_slice_in_dim(filter_proj, row_index * chan_row, chan_row, 3)
    own_decay = lax.dynamic_slice_in_dim(filter_decay, row_index * chan_row, chan_row, 2)
    taps = jnp.dot(hidden, own_proj.reshape(own_proj.shape[0], 4 * chan_row), precision=precise)
    taps = jnp.transpose(taps).reshape(2, 2, chan_row, length)
    taps = taps * jnp.exp(-spot[None, None, None, :] * own_decay[:, :, :, None])
    cycles = []
    for order in range(2):
        behind = jnp.flip(taps[order, 1, :, 1:], axis=1)
        cycles.append(
            jnp.concatenate([taps[order, 0], jnp.zeros((chan_row, 1), jnp.float32), behind], axis=1)
        )
    return cycles


def body(
    tokens,
    w_value,
    w_first,
    w_second,
    w_gate,
    conv_taps,
    filter_embed,
    filter_freq,
    filter_proj,
    filter_decay,
    skip_gain,
    w_out,
):
    seq_count = tokens.shape[0]
    tok_rows = tokens.shape[1]
    chan_col = w_value.shape[1]
    row_count = lax.axis_size("row")
    chan_row = chan_col // row_count
    length = tok_rows * row_count
    row_index = lax.axis_index("row")
    proj = jnp.concatenate(
        [
            jnp.dot(tokens, w_value, preferred_element_type=jnp.float32),
            jnp.dot(tokens, w_first, preferred_element_type=jnp.float32),
            jnp.dot(tokens, w_second, preferred_element_type=jnp.float32),
        ],
        axis=2,
    ).astype(jnp.bfloat16)
    gate = jnp.dot(tokens, w_gate, preferred_element_type=jnp.float32).astype(jnp.bfloat16)
    padded = padded_2(proj, (("row", 1),), 1).astype(jnp.float32)
    weights = conv_taps.reshape(3, 3 * chan_col)
    short = padded[:, :-2] * weights[0] + padded[:, 1:-1] * weights[1] + padded[:, 2:] * weights[2]
    value_rows = jnp.transpose(short[:, :, :chan_col], (0, 2, 1))
    first_rows = jnp.transpose(short[:, :, chan_col : 2 * chan_col], (0, 2, 1))
    second_rows = jnp.transpose(short[:, :, 2 * chan_col :], (0, 2, 1))
    outer, inner = split_length(2 * length)
    table = tables(outer, inner, 2 * length)
    cycles = channel_filters(
        length, row_index, chan_row, filter_embed, filter_freq, filter_proj, filter_decay
    )
    spectra = [forward_real(cycle, table) for cycle in cycles]
    own_gain = lax.dynamic_slice_in_dim(skip_gain, row_index * chan_row, chan_row, 1)

    def convolve(signal, order):
        flat = signal.reshape(seq_count * chan_row, length)
        padded_signal = jnp.concatenate([flat, jnp.zeros_like(flat)], axis=1)
        sig_real, sig_imag = forward_real(padded_signal, table)
        sig_real = sig_real.reshape(seq_count, chan_row, outer, inner)
        sig_imag = sig_imag.reshape(seq_count, chan_row, outer, inner)
        filt_real, filt_imag = spectra[order]
        prod_real = sig_real * filt_real[None] - sig_imag * filt_imag[None]
        prod_imag = sig_real * filt_imag[None] + sig_imag * filt_real[None]
        result = inverse_real(
            prod_real.reshape(seq_count * chan_row, outer, inner),
            prod_imag.reshape(seq_count * chan_row, outer, inner),
            table,
        )[:, :length]
        return result.reshape(seq_count, chan_row, length) + own_gain[order][None, :, None] * signal

    value_chan, first_chan = (
        lax.all_to_all(value_rows, "row", split_axis=1, concat_axis=2, tiled=True),
        lax.all_to_all(first_rows, "row", split_axis=1, concat_axis=2, tiled=True),
    )
    inner_chan = first_chan * convolve(value_chan, 0)
    second_conv = lax.all_to_all(
        convolve(inner_chan, 1), "row", split_axis=2, concat_axis=1, tiled=True
    )
    outer_rows = (
        jnp.transpose(second_rows * second_conv, (0, 2, 1)) * jax.nn.silu(gate.astype(jnp.float32))
    ).astype(jnp.bfloat16)
    own_rows = tok_rows // lax.axis_size("col")
    flat_rows = jnp.transpose(outer_rows, (1, 0, 2)).reshape(tok_rows * seq_count, chan_col)
    summed = lax.psum_scatter(
        jnp.dot(flat_rows, w_out, preferred_element_type=jnp.float32).astype(jnp.bfloat16),
        "col",
        scatter_dimension=0,
        tiled=True,
    ).astype(jnp.float32)
    summed = jnp.transpose(summed.reshape(own_rows, seq_count, w_out.shape[1]), (1, 0, 2))
    return summed.astype(jnp.bfloat16)


LANES = 128
PACK = 16


def dft_tables(length):
    filled = length // LANES
    outer = 2 * filled
    total = outer * LANES
    half = filled + 1
    eye = np.eye(PACK)
    q, k, p = np.arange(filled), np.arange(half), np.arange(LANES)
    inside = k[1:-1]
    angle = 2.0 * np.pi * (np.outer(k, q) % outer) / outer
    first = np.concatenate([np.kron(np.cos(angle), eye), np.kron(-np.sin(angle)[inside], eye)], axis=0)
    weight = np.where((k == 0) | (k == filled), 1.0, 2.0) / total
    last = np.concatenate(
        [
            np.kron(np.cos(angle).T * weight, eye),
            np.kron((-np.sin(angle).T * weight)[:, inside], eye),
        ],
        axis=1,
    )
    turn = 2.0 * np.pi * np.outer(k, p) / total
    twist = np.stack([np.cos(turn), np.sin(turn)])[:, :, None, :]
    twist = np.broadcast_to(twist, (2, half, 8, LANES))
    angle = 2.0 * np.pi * (np.outer(p, p) % LANES) / LANES
    cos, sin = np.cos(angle), np.sin(angle)
    ahead = np.block([[cos, -sin], [sin, cos]])
    back = np.block([[cos, sin], [-sin, cos]])
    return first, last, jnp.asarray(twist.astype(np.float32)), ahead, back


def split_bf16(array):
    high = array.astype(jnp.bfloat16).astype(jnp.float32)
    middle = (array - high).astype(jnp.bfloat16).astype(jnp.float32)
    low = (array - high - middle).astype(jnp.bfloat16).astype(jnp.float32)
    return high, middle, low


def host_split(array):
    low_type = jnp.bfloat16.dtype
    high = array.astype(low_type).astype(np.float64)
    middle = (array - high).astype(low_type).astype(np.float64)
    low = (array - high - middle).astype(low_type).astype(np.float64)
    return high, middle, low


def flip(value, bits):
    bit = 1
    while bit <= bits:
        if bits & bit:
            value = value + bit - 2 * bit * lax.rem(lax.div(value, bit), 2)
        bit *= 2
    return value


def mixer_kernel(
    rows, cols, width, emb,
    tokens_hbm, w_value_hbm, w_first_hbm, w_second_hbm, w_gate_hbm, w_out_hbm, conv_hbm, embed_hbm, freq_hbm,
    proj_hbm, decay_hbm, gain_hbm, features_hbm, tables_hbm, twist_hbm,
    out_ref,
    tokens_ref, w_refs, conv_ref, embed_ref, freq_ref, fproj_ref, decay_ref, gain_ref, features_ref, tables_ref,
    twist_ref,
    send, recv, spectra, taps_ref, stack_ref, coef_ref, gated, edge_out, edge_in, back_send, back_in, outer_send, outer_in, weights, total,
    load_sem, row_send, row_recv, edge_send, edge_recv, piece_send, piece_recv, outer_sem,
    wide_send, wide_recv, level_send, level_recv, pass_send, pass_recv, mate_send, mate_recv, told,
):
    my_row = lax.axis_index("row")
    my_col = lax.axis_index("col")
    mesh_id = pl.DeviceIdType.MESH
    groups = recv.shape[2]
    chans = groups * PACK
    tok_rows = tokens_ref.shape[0]
    block_q = tok_rows // LANES
    length_q = rows * block_q
    length = tok_rows * rows
    half = length_q + 1
    hid = freq_ref.shape[1]
    depth = weights.shape[4]
    f32, low = jnp.float32, jnp.bfloat16

    def remote(src, dst, send_sem, recv_sem, row, col):
        return pltpu.make_async_remote_copy(
            src_ref=src, dst_ref=dst, send_sem=send_sem, recv_sem=recv_sem,
            device_id=(row, col), device_id_type=mesh_id,
        )

    side = lax.rem(my_row, 2)
    mate = flip(my_row, 1)
    low_row = my_row - side
    barrier = pltpu.get_barrier_semaphore()

    def greet(row, col):
        pl.semaphore_signal(barrier, inc=1, device_id=(row, col), device_id_type=mesh_id)

    near = (1, 2)
    greet(mate, my_col)
    for d in near:
        greet(low_row, flip(my_col, d))
    for d in range(1, rows // 2):
        greet(flip(low_row, 2 * d) + 1, my_col)

    def heard(own_side):
        others = 2 * len(near) + 1 if own_side == 0 else rows - 1

        @pl.when(side == own_side)
        def _():
            pl.semaphore_wait(barrier, others)
            pl.semaphore_signal(told, inc=1, device_id=(mate, my_col), device_id_type=mesh_id)

        @pl.when(side != own_side)
        def _():
            pl.semaphore_wait(told, 1)

    def await_bytes(ref, sem):
        pltpu.make_async_copy(ref, ref, sem).wait()

    token_sem, weight_sem, half_sem = load_sem.at[0], load_sem.at[1], load_sem.at[2]
    half_rows = lambda half: pl.ds(half * (rows // 2), rows // 2)
    own_rows = pltpu.make_async_copy(w_out_hbm.at[half_rows(side)], weights.at[0, half_rows(side)], half_sem)
    own_rows.start()
    pltpu.make_async_copy(tokens_hbm, tokens_ref, token_sem).start()
    pltpu.make_async_copy(w_value_hbm, w_refs.at[0], token_sem).start()
    loads = {}
    for name, src, dst in (
        ("embed", embed_hbm, embed_ref.at[pl.ds(0, emb)]),
        ("freq", freq_hbm, freq_ref),
        ("conv", conv_hbm, conv_ref),
        ("gain", gain_hbm, gain_ref),
        ("decay", decay_hbm, decay_ref),
        ("fproj", proj_hbm, fproj_ref),
        ("features", features_hbm, features_ref),
        ("tables", tables_hbm, tables_ref),
        ("twist", twist_hbm, twist_ref),
        ("w_out", w_out_hbm.at[half_rows(1 - side)], weights.at[0, half_rows(1 - side)]),
    ):
        loads[name] = pltpu.make_async_copy(src, dst, load_sem.at[3 + len(loads)])
    for role, w_hbm in ((2, w_second_hbm), (1, w_first_hbm), (3, w_gate_hbm)):
        pltpu.make_async_copy(w_hbm, w_refs.at[role], weight_sem).start()
    for copy in loads.values():
        copy.start()

    plane = lax.rem(lax.div(my_row, 2), 2)
    subs = rows // 2
    row_of = lambda sub: side * subs + sub

    def wide_copy(group, d, sub):
        return remote(
            weights.at[0, row_of(sub)], weights.at[d, row_of(sub)],
            wide_send, wide_recv.at[group], my_row, flip(my_col, d),
        )

    wide = {
        (d, sub): wide_copy(group, d, sub + plane if group == 0 else sub)
        for group, d, sub in ((0, 1, 0), (0, 2, 2), (1, 1, 3), (1, 2, 0), (2, 1, 2), (2, 2, 1))
    }

    def there(part, send_sem, recv_sem, row):
        return remote(part, part, send_sem, recv_sem, row, my_col)

    def level_copy(index, d, group, start, count):
        part = weights.at[d, row_of(2 * d - 2 + plane), group, pl.ds(0, PACK), pl.ds(start, count)]
        return there(part, level_send, level_recv.at[index], flip(my_row, 2))

    ahead_of = depth // 2
    early = [level_copy(0, 1, pl.ds(0, groups), 0, depth), level_copy(1, 2, pl.ds(0, 1), 0, ahead_of)]
    late = [
        level_copy(1, 2, pl.ds(0, 1), ahead_of, depth - ahead_of),
        level_copy(1, 2, pl.ds(1, groups - 1), 0, depth),
    ]

    def pass_copy(index, d, sub):
        return remote(
            weights.at[d, row_of(sub)], weights.at[3, row_of(sub)],
            pass_send, pass_recv.at[index], my_row, flip(my_col, 3 - d),
        )

    passed = {(d, sub): pass_copy(index, d, sub) for index, d, sub in ((0, 1, 3), (0, 2, 0), (1, 1, 2), (1, 2, 1))}

    def to_mate(d, sub):
        there(weights.at[d, row_of(sub)], mate_send, mate_recv.at[d // 3], mate).start()

    def chunk(count):
        return weights.at[0, pl.ds(0, count)]

    def wide_arrived(group, keys):
        await_bytes(chunk(len(keys)), wide_recv.at[group])
        for d, sub in keys:
            if (d, sub) in passed:
                passed[d, sub].start()
            to_mate(d, sub + plane if group == 0 else sub)

    far_first = sorted(range(1, rows), key=lambda d: -(d & (rows // 2)))

    def row_copies(role):
        return [
            remote(
                send.at[role, flip(my_row, d)], recv.at[role, my_row],
                row_send.at[role], row_recv.at[role], flip(my_row, d), my_col,
            )
            for d in far_first
        ]

    def project(role):
        return jnp.dot(tokens_ref[...], w_refs[role], preferred_element_type=f32)

    def project_turned(role):
        result = project(role).T
        for q in range(block_q):
            send[role, :, :, q] = (
                result[:, q * LANES : (q + 1) * LANES].reshape(rows, groups, PACK, LANES).astype(low)
            )

    value_copies, first_copies = row_copies(0), row_copies(1)

    heard(0)
    own_rows.wait()
    for copy in wide.values():
        copy.start()
    await_bytes(w_refs.at[pl.ds(0, 2)], token_sem)
    project_turned(0)
    heard(1)
    for copy in value_copies:
        copy.start()
    recv[0, my_row] = send[0, my_row]

    await_bytes(w_refs.at[pl.ds(1, 3)], weight_sem)
    second = project(2).astype(low).astype(f32)
    edge_out[0] = jnp.broadcast_to(second[tok_rows - 1 :], edge_out.shape[1:])
    edge_out[1] = jnp.broadcast_to(second[:1], edge_out.shape[1:])
    def edge_copy(index, step):
        return remote(edge_out.at[index], edge_in.at[index], edge_send.at[index], edge_recv.at[index], my_row + step, my_col)

    has_above, has_below = my_row > 0, my_row < rows - 1

    @pl.when(has_below)
    def _():
        edge_copy(0, 1).start()

    @pl.when(has_above)
    def _():
        edge_copy(1, -1).start()

    project_turned(1)
    for copy in first_copies:
        copy.start()
    recv[1, my_row] = send[1, my_row]
    gate = project(3).astype(low).astype(f32)
    loads["conv"].wait()

    loads["gain"].wait()
    loads["decay"].wait()
    stack_ref[...] = jnp.zeros_like(stack_ref)
    for j in range(3):
        stack_ref[j : j + 1] = conv_ref[j, 0:1]
        stack_ref[3 + j : 4 + j] = conv_ref[j, 1:2]
    stack_ref[6:8] = gain_ref[...]
    stack_ref[8:10] = decay_ref[0]
    stack_ref[10:12] = decay_ref[1]
    shape = (chans, stack_ref.shape[1])
    picks = lax.broadcasted_iota(jnp.int32, shape, 1) == lax.broadcasted_iota(jnp.int32, shape, 0) + my_row * chans
    picks = jnp.where(picks, 1.0, 0.0)
    contract_last = (((1,), (1,)), ((), ()))
    own = lax.dot_general(picks, stack_ref[...], contract_last, precision=precise, preferred_element_type=f32)
    for k in range(8):
        coef_ref[k] = jnp.broadcast_to(own[:, k : k + 1], (chans, LANES)).reshape(groups, PACK, LANES)

    loads["embed"].wait()
    loads["freq"].wait()
    embed = embed_ref[...] * (freq_ref[...] * (1.0 / math.pi))
    embed = jnp.where(lax.broadcasted_iota(jnp.int32, embed.shape, 0) < emb, embed, 0.0)
    high, middle, least = split_bf16(embed)
    stacked = jnp.concatenate([high, high, middle, high, middle, least], axis=0).astype(low)
    loads["features"].wait()
    turns = lax.dot_general(stacked, features_ref[...], (((0,), (0,)), ((), ())), preferred_element_type=f32)
    whole = jnp.floor(turns + 0.5)
    rest = turns - whole
    sign = 1.0 - 2.0 * (whole - 2.0 * jnp.floor(whole * 0.5))
    square = rest * rest
    series = jnp.full_like(square, -(math.pi**11) / math.factorial(11))
    for n in (9, 7, 5, 3, 1):
        series = series * square + (-1) ** (n // 2) * math.pi**n / math.factorial(n)
    hidden = (series * (rest * sign)).astype(low)
    loads["fproj"].wait()
    pieces = []
    picks_low = picks.astype(low)
    halves = 2
    for od in range(4):
        parts = [
            fproj_ref[pl.ds((od // 2) * 2 * halves + j * 2 + od % 2, hid, stride=4 * halves), :]
            for j in range(halves)
        ]
        block = jnp.concatenate(parts, axis=1).astype(low)
        pieces.append(lax.dot_general(picks_low, block, contract_last, preferred_element_type=f32).astype(low))
    taps = jnp.dot(jnp.concatenate(pieces, axis=0), hidden, preferred_element_type=f32)
    lag = lax.broadcasted_iota(jnp.int32, (1, length), 1)
    spot = lag.astype(f32) / (length - 1)
    for od in range(4):
        block = taps[od * chans : (od + 1) * chans] * jnp.exp(-own[:, 8 + od : 9 + od] * spot)
        if od % 2 == 1:
            block = jnp.where(lag == 0, 0.0, block)
        taps_ref[od] = block.astype(low)

    size = LANES * groups
    first_ref, last_ref, ahead_ref, back_ref = (
        tables_ref.at[pl.ds(start * size, count * size)]
        for start, count in ((0, 2), (2, 2), (4, 1), (5, 1))
    )

    def wide_twist(index):
        return twist_ref[index].reshape(half, 1, 8, LANES)

    def ahead(signal):
        mid = jnp.dot(first_ref[...], signal, preferred_element_type=f32)
        blank = jnp.zeros((PACK, LANES), f32)
        blocks = []
        for g in range(groups):
            lanes = slice(g * LANES, (g + 1) * LANES)
            real = mid[: half * PACK, lanes].reshape(half, 2, 8, LANES)
            imag = jnp.concatenate([blank, mid[half * PACK :, lanes], blank], axis=0).reshape(half, 2, 8, LANES)
            cos, sin = wide_twist(0), wide_twist(1)
            blocks.append(
                jnp.concatenate(
                    [
                        (real * cos + imag * sin).reshape(half * PACK, LANES),
                        (imag * cos - real * sin).reshape(half * PACK, LANES),
                    ],
                    axis=1,
                ).astype(low)
            )
        return jnp.dot(jnp.concatenate(blocks, axis=0), ahead_ref[...], preferred_element_type=f32)

    def convolve(signal, order):
        spec = ahead(signal.astype(low))
        real, imag = spec[:, :LANES], spec[:, LANES:]
        filt_real, filt_imag = spectra[order, 0], spectra[order, 1]
        prod = jnp.concatenate(
            [real * filt_real - imag * filt_imag, real * filt_imag + imag * filt_real], axis=1
        ).astype(low)
        mid = jnp.dot(prod, back_ref[...], preferred_element_type=f32)
        blocks = []
        for g in range(groups):
            span = slice(g * half * PACK, (g + 1) * half * PACK)
            real = mid[span, :LANES].reshape(half, 2, 8, LANES)
            imag = mid[span, LANES:].reshape(half, 2, 8, LANES)
            cos, sin = wide_twist(0), wide_twist(1)
            turned_real = (real * cos - imag * sin).reshape(half * PACK, LANES)
            turned_imag = (real * sin + imag * cos)[1:-1].reshape((half - 2) * PACK, LANES)
            blocks.append(jnp.concatenate([turned_real, turned_imag], axis=0).astype(low))
        last = jnp.concatenate([last_ref[:size], last_ref[size:]], axis=1)
        result = jnp.dot(last, jnp.concatenate(blocks, axis=1), preferred_element_type=f32)
        gain = jnp.concatenate([coef_ref[6 + order, g] for g in range(groups)], axis=1)
        shape = (length_q, PACK, groups * LANES)
        return (result.reshape(shape) + gain[None] * signal.reshape(shape)).reshape(signal.shape)

    loads["tables"].wait()
    loads["twist"].wait()
    for order in range(2):
        for direction in range(2):
            od = 2 * order + direction
            signal = jnp.concatenate(
                [
                    jnp.concatenate(
                        [
                            taps_ref[od, g * PACK : (g + 1) * PACK, q * LANES : (q + 1) * LANES]
                            for q in range(length_q)
                        ],
                        axis=0,
                    )
                    for g in range(groups)
                ],
                axis=1,
            )
            spec = ahead(signal)
            if direction == 0:
                spectra[order, 0] = spec[:, :LANES]
                spectra[order, 1] = spec[:, LANES:]
            else:
                spectra[order, 0] += spec[:, :LANES]
                spectra[order, 1] -= spec[:, LANES:]

    wide_arrived(0, ((1, 0), (2, 2)))
    for copy in early:
        copy.start()


    @pl.when(has_above)
    def _():
        await_bytes(edge_in.at[0], edge_recv.at[0])

    @pl.when(has_below)
    def _():
        await_bytes(edge_in.at[1], edge_recv.at[1])

    line = lax.broadcasted_iota(jnp.int32, second.shape, 0)
    above = jnp.where(has_above, edge_in[0, 0:1], 0.0)
    below = jnp.where(has_below, edge_in[1, 0:1], 0.0)
    before = jnp.where(line == 0, above, pltpu.roll(second, 1, 0))
    after = jnp.where(line == tok_rows - 1, below, pltpu.roll(second, tok_rows - 1, 0))
    short_second = before * conv_ref[0, 2:3] + second * conv_ref[1, 2:3] + after * conv_ref[2, 2:3]
    both = short_second * (gate / (1.0 + jnp.exp(-gate)))
    for tile in range(halves):
        gated[tile] = both[:, tile * LANES : (tile + 1) * LANES]

    def short(role):
        blocks = []
        for g in range(groups):
            here = recv[role, :, g].reshape(length_q * PACK, LANES).astype(f32)
            size = here.shape[0]
            lane = lax.broadcasted_iota(jnp.int32, here.shape, 1)
            blank = jnp.zeros((PACK, LANES), f32)
            before = pltpu.roll(here, 1, 1)
            before = jnp.where(lane == 0, jnp.concatenate([blank, before[: size - PACK]], axis=0), before)
            after = pltpu.roll(here, LANES - 1, 1)
            after = jnp.where(lane == LANES - 1, jnp.concatenate([after[PACK:], blank], axis=0), after)
            shape = (length_q, PACK, LANES)
            w = lambda j: coef_ref[3 * role + j, g][None]
            result = before.reshape(shape) * w(0) + here.reshape(shape) * w(1) + after.reshape(shape) * w(2)
            blocks.append(result.reshape(size, LANES))
        return jnp.concatenate(blocks, axis=1)

    others = pl.ds(0, rows - 1)
    await_bytes(recv.at[0, others], row_recv.at[0])
    conv = convolve(short(0), 0)

    wide_arrived(1, ((1, 3), (2, 0)))
    await_bytes(recv.at[1, others], row_recv.at[1])
    conv = convolve(short(1) * conv, 1)

    for g in range(groups):
        back_send[:, :, g] = (
            conv[:, g * LANES : (g + 1) * LANES].reshape(rows, block_q, PACK, LANES).astype(low)
        )
    for d in far_first:
        peer = flip(my_row, d)
        remote(back_send.at[peer], back_in.at[my_row], piece_send, piece_recv.at[2 * d // rows], peer, my_col).start()
    for copy in late:
        copy.start()
    back_in[my_row] = back_send[my_row]

    wide_arrived(2, ((1, 2), (2, 1)))

    per_tile = rows // halves
    near_tile = lax.div(my_row, per_tile)

    def finish(tile, far):
        count = per_tile if far else per_tile - 1
        await_bytes(back_in.at[pl.ds(0, count)], piece_recv.at[far])
        for q in range(block_q):
            block = back_in[pl.ds(tile * per_tile, per_tile), q].reshape(LANES, LANES).astype(f32).T
            block = (block * gated[tile, q * LANES : (q + 1) * LANES]).astype(low)
            spots = LANES // width
            outer_send[far, q * spots : (q + 1) * spots] = block.reshape(spots, width, LANES)
        for d in (3, 1, 2):
            peer = flip(my_col, d)
            remote(
                outer_send.at[far, peer], outer_in.at[far, d], outer_sem.at[0], outer_sem.at[1 + far], my_row, peer
            ).start()
        outer_in[far, 0] = outer_send[far, my_col]

    def share(tile, far):
        await_bytes(outer_in.at[far, pl.ds(1, cols - 1)], outer_sem.at[1 + far])
        left = jnp.concatenate([outer_in[far, d] for d in range(cols)], axis=1)
        right = jnp.concatenate(
            [weights[d, pl.ds(tile * per_tile, per_tile)].reshape(LANES, depth) for d in range(cols)], axis=0
        )
        return jnp.dot(left, right, preferred_element_type=f32)

    finish(near_tile, 0)
    await_bytes(chunk(2), pass_recv.at[0])
    to_mate(3, 0)
    to_mate(3, 3)
    await_bytes(chunk(1), level_recv.at[0])
    to_mate(1, 1 - plane)
    finish(1 - near_tile, 1)
    await_bytes(chunk(2), pass_recv.at[1])
    to_mate(3, 2)
    to_mate(3, 1)
    await_bytes(chunk(1), level_recv.at[1])
    to_mate(2, 3 - plane)

    loads["w_out"].wait()
    await_bytes(weights.at[0], mate_recv.at[0])
    await_bytes(chunk(subs), mate_recv.at[1])
    total[...] = share(near_tile, 0)
    out_ref[...] = (total[...] + share(1 - near_tile, 1)).astype(low)

    for role in range(2):
        await_bytes(send.at[role, others], row_send.at[role])

    @pl.when(has_below)
    def _():
        await_bytes(edge_out.at[0], edge_send.at[0])

    @pl.when(has_above)
    def _():
        await_bytes(edge_out.at[1], edge_send.at[1])

    await_bytes(back_send.at[others], piece_send)
    await_bytes(outer_send.at[pl.ds(0, 2), pl.ds(0, cols - 1)], outer_sem.at[0])
    await_bytes(chunk(6), wide_send)
    await_bytes(chunk(2), level_send)
    await_bytes(chunk(4), pass_send)
    await_bytes(weights.at[pl.ds(0, 3), pl.ds(0, 4)], mate_send)


def fast_body(
    tokens, w_value, w_first, w_second, w_gate, conv_taps, filter_embed, filter_freq, filter_proj,
    filter_decay, skip_gain, w_out,
):
    rows, cols = lax.axis_size("row"), lax.axis_size("col")
    tok_rows = tokens.shape[1]
    chan_col = w_value.shape[1]
    chans = chan_col // rows
    groups = chans // PACK
    length = tok_rows * rows
    block_q = tok_rows // LANES
    length_q = length // LANES
    width = tok_rows // cols
    depth = w_out.shape[1]
    emb, hid = filter_embed.shape
    half = length_q + 1

    flat = tokens.reshape(tok_rows, tokens.shape[2])
    bands = (emb - 1) // 2
    index = np.arange(length)
    spot = index.astype(np.float32) / np.float32(length - 1)
    phase = 2.0 * np.pi * (np.outer(np.arange(1, bands + 1), index) % length) / length
    features = np.concatenate([spot[None, :], np.cos(phase), np.sin(phase)])
    emb_pad = -(-emb // 8) * 8
    features = np.concatenate([features, np.zeros((emb_pad - emb, length))]).astype(np.float32).astype(np.float64)
    high, middle, least = host_split(features)
    features = np.concatenate([high, middle, high, least, middle, high]).astype(jnp.bfloat16.dtype)
    lanes = chan_col // LANES
    fproj = filter_proj.reshape(hid, 2, 2, lanes, LANES).transpose(0, 1, 3, 2, 4).reshape(hid * 4 * lanes, LANES)
    w_rows = w_out.reshape(rows, groups, PACK, depth)

    first, last, twist, ahead, back = dft_tables(length)
    size = groups * LANES
    tables = jnp.asarray(
        np.concatenate([first, last[:, :size], last[:, size:], ahead, back]).astype(np.float32)
    ).astype(jnp.bfloat16)
    operands = (
        flat, w_value, w_first, w_second, w_gate, w_rows, conv_taps, filter_embed, filter_freq.reshape(1, hid),
        fproj, filter_decay, skip_gain, jnp.asarray(features), tables, twist,
    )
    dma = pltpu.SemaphoreType.DMA
    f32, low = jnp.float32, jnp.bfloat16
    like = lambda array: pltpu.VMEM(array.shape, array.dtype)
    mixed = pl.pallas_call(
        functools.partial(mixer_kernel, rows, cols, width, emb),
        out_shape=pltpu.VMEM((width, depth), low),
        in_specs=[pl.BlockSpec(memory_space=pl.ANY)] * len(operands),
        out_specs=pl.BlockSpec(memory_space=pltpu.VMEM),
        scratch_shapes=[
            like(flat),
            pltpu.VMEM((4,) + w_value.shape, low),
            like(conv_taps),
            pltpu.VMEM((emb_pad, hid), f32),
            pltpu.VMEM((1, hid), f32),
            like(fproj),
            like(filter_decay),
            like(skip_gain),
            pltpu.VMEM(features.shape, low),
            like(tables),
            like(twist),
            pltpu.VMEM((2, rows, groups, block_q, PACK, LANES), low),
            pltpu.VMEM((2, rows, groups, block_q, PACK, LANES), low),
            pltpu.VMEM((2, 2, groups * half * PACK, LANES), f32),
            pltpu.VMEM((4, chans, length), low),
            pltpu.VMEM((16, chan_col), f32),
            pltpu.VMEM((8, groups, PACK, LANES), f32),
            pltpu.VMEM((lanes, tok_rows, LANES), f32),
            pltpu.VMEM((2, 8, chan_col), f32),
            pltpu.VMEM((2, 8, chan_col), f32),
            pltpu.VMEM((rows, block_q, groups, PACK, LANES), low),
            pltpu.VMEM((rows, block_q, groups, PACK, LANES), low),
            pltpu.VMEM((2, cols, width, LANES), low),
            pltpu.VMEM((2, cols, width, LANES), low),
            pltpu.VMEM((cols, rows, groups, PACK, depth), low),
            pltpu.VMEM((width, depth), f32),
            dma((len(operands) - 2,)),
            dma((2,)),
            dma((2,)),
            dma((2,)),
            dma((2,)),
            dma,
            dma((2,)),
            dma((3,)),
            dma,
            dma((3,)),
            dma,
            dma((2,)),
            dma,
            dma((2,)),
            dma,
            dma((2,)),
            pltpu.SemaphoreType.REGULAR,
        ],
        compiler_params=pltpu.CompilerParams(
            collective_id=0, has_side_effects=True, vmem_limit_bytes=40 * 1024 * 1024
        ),
        cost_estimate=pl.CostEstimate(flops=12_000_000_000, bytes_accessed=8_000_000, transcendentals=0),
    )(*[pltpu.with_memory_space_constraint(array, pltpu.HBM) for array in operands])
    return mixed[None]


def shaped_body(tokens, w_value, *rest):
    rows, cols = lax.axis_size("row"), lax.axis_size("col")
    seqs, tok_rows = tokens.shape[:2]
    chan_col = w_value.shape[1]
    chans = chan_col // rows
    width = tok_rows // cols
    fits = (
        seqs == 1
        and cols == 4
        and rows == 8
        and chans == 2 * PACK
        and tok_rows % LANES == 0
        and LANES == 2 * width
        and chan_col == 2 * LANES
        and rows * PACK == LANES
    )
    return (fast_body if fits else body)(tokens, w_value, *rest)


def solution(mesh):
    in_specs = (
        P(None, "row", None),
        P(None, "col"),
        P(None, "col"),
        P(None, "col"),
        P(None, "col"),
        P(None, None, "col"),
        P(),
        P(),
        P(None, None, None, "col"),
        P(None, None, "col"),
        P(None, "col"),
        P("col", None),
    )
    out_specs = P(None, ("row", "col"), None)
    return jax.shard_map(shaped_body, mesh=mesh, in_specs=in_specs, out_specs=out_specs, check_vma=False)
```

```python
import functools
import math

import jax
import jax.numpy as jnp
import numpy as np
from jax import lax
from jax.experimental import pallas as pl
from jax.experimental.pallas import tpu as pltpu
from jax.sharding import PartitionSpec as P

precise = lax.Precision.HIGHEST


def padded_2(array, sides, width):
    for axis, dim in sides:
        size, length = (lax.axis_size(axis), array.shape[dim])
        up = [(i, (i + 1) % size) for i in range(size - 1)]
        down = [(j, i) for i, j in up]
        last = lax.slice_in_dim(array, length - width, length, axis=dim)
        leading = lax.slice_in_dim(array, 0, width, axis=dim)
        before = lax.ppermute(last, axis, up)
        after = lax.ppermute(leading, axis, down)
        array = jnp.concatenate([before, array, after], axis=dim)
    return array


def split_length(total):
    factor = math.isqrt(total)
    while total % factor != 0:
        factor = factor - 1
    return (factor, total // factor)


def tables(outer, inner, total):
    first_index = jnp.arange(outer, dtype=jnp.int32)
    second_index = jnp.arange(inner, dtype=jnp.int32)
    scale = 2.0 * math.pi
    outer_angle = (first_index[:, None] * first_index[None, :] % outer).astype(jnp.float32) * (
        scale / outer
    )
    inner_angle = (second_index[:, None] * second_index[None, :] % inner).astype(jnp.float32) * (
        scale / inner
    )
    twist_angle = (first_index[:, None] * second_index[None, :] % total).astype(jnp.float32) * (
        scale / total
    )
    return (
        jnp.cos(outer_angle),
        jnp.sin(outer_angle),
        jnp.cos(inner_angle),
        jnp.sin(inner_angle),
        jnp.cos(twist_angle),
        jnp.sin(twist_angle),
    )


def forward_real(signal, table):
    outer_cos, outer_sin, inner_cos, inner_sin, twist_cos, twist_sin = table
    outer = outer_cos.shape[0]
    inner = inner_cos.shape[0]
    grid = signal.reshape(signal.shape[0], outer, inner)
    real_part = jnp.einsum("kq,cqp->ckp", outer_cos, grid, precision=precise)
    imag_part = -jnp.einsum("kq,cqp->ckp", outer_sin, grid, precision=precise)
    turned_real = real_part * twist_cos + imag_part * twist_sin
    turned_imag = imag_part * twist_cos - real_part * twist_sin
    spec_real = jnp.einsum("ckp,pj->ckj", turned_real, inner_cos, precision=precise) + jnp.einsum(
        "ckp,pj->ckj", turned_imag, inner_sin, precision=precise
    )
    spec_imag = jnp.einsum("ckp,pj->ckj", turned_imag, inner_cos, precision=precise) - jnp.einsum(
        "ckp,pj->ckj", turned_real, inner_sin, precision=precise
    )
    return (spec_real, spec_imag)


def inverse_real(spec_real, spec_imag, table):
    outer_cos, outer_sin, inner_cos, inner_sin, twist_cos, twist_sin = table
    total = outer_cos.shape[0] * inner_cos.shape[0]
    back_real = jnp.einsum("ckj,jp->ckp", spec_real, inner_cos, precision=precise) - jnp.einsum(
        "ckj,jp->ckp", spec_imag, inner_sin, precision=precise
    )
    back_imag = jnp.einsum("ckj,jp->ckp", spec_real, inner_sin, precision=precise) + jnp.einsum(
        "ckj,jp->ckp", spec_imag, inner_cos, precision=precise
    )
    turned_real = back_real * twist_cos - back_imag * twist_sin
    turned_imag = back_real * twist_sin + back_imag * twist_cos
    result = jnp.einsum("qk,ckp->cqp", outer_cos, turned_real, precision=precise) - jnp.einsum(
        "qk,ckp->cqp", outer_sin, turned_imag, precision=precise
    )
    return result.reshape(result.shape[0], total) / total


def channel_filters(
    length, row_index, chan_row, filter_embed, filter_freq, filter_proj, filter_decay
):
    bands = (filter_embed.shape[0] - 1) // 2
    index = jnp.arange(length, dtype=jnp.int32)
    spot = index.astype(jnp.float32) / (length - 1)
    freqs = jnp.arange(1, bands + 1, dtype=jnp.int32)
    phase = (index[:, None] * freqs[None, :] % length).astype(jnp.float32) * (
        2.0 * math.pi / length
    )
    features = jnp.concatenate([spot[:, None], jnp.cos(phase), jnp.sin(phase)], axis=1)
    hidden = jnp.sin(filter_freq[None, :] * jnp.dot(features, filter_embed, precision=precise))
    own_proj = lax.dynamic_slice_in_dim(filter_proj, row_index * chan_row, chan_row, 3)
    own_decay = lax.dynamic_slice_in_dim(filter_decay, row_index * chan_row, chan_row, 2)
    taps = jnp.dot(hidden, own_proj.reshape(own_proj.shape[0], 4 * chan_row), precision=precise)
    taps = jnp.transpose(taps).reshape(2, 2, chan_row, length)
    taps = taps * jnp.exp(-spot[None, None, None, :] * own_decay[:, :, :, None])
    cycles = []
    for order in range(2):
        behind = jnp.flip(taps[order, 1, :, 1:], axis=1)
        cycles.append(
            jnp.concatenate([taps[order, 0], jnp.zeros((chan_row, 1), jnp.float32), behind], axis=1)
        )
    return cycles


def body(
    tokens,
    w_value,
    w_first,
    w_second,
    w_gate,
    conv_taps,
    filter_embed,
    filter_freq,
    filter_proj,
    filter_decay,
    skip_gain,
    w_out,
):
    seq_count = tokens.shape[0]
    tok_rows = tokens.shape[1]
    chan_col = w_value.shape[1]
    row_count = lax.axis_size("row")
    chan_row = chan_col // row_count
    length = tok_rows * row_count
    row_index = lax.axis_index("row")
    proj = jnp.concatenate(
        [
            jnp.dot(tokens, w_value, preferred_element_type=jnp.float32),
            jnp.dot(tokens, w_first, preferred_element_type=jnp.float32),
            jnp.dot(tokens, w_second, preferred_element_type=jnp.float32),
        ],
        axis=2,
    ).astype(jnp.bfloat16)
    gate = jnp.dot(tokens, w_gate, preferred_element_type=jnp.float32).astype(jnp.bfloat16)
    padded = padded_2(proj, (("row", 1),), 1).astype(jnp.float32)
    weights = conv_taps.reshape(3, 3 * chan_col)
    short = padded[:, :-2] * weights[0] + padded[:, 1:-1] * weights[1] + padded[:, 2:] * weights[2]
    value_rows = jnp.transpose(short[:, :, :chan_col], (0, 2, 1))
    first_rows = jnp.transpose(short[:, :, chan_col : 2 * chan_col], (0, 2, 1))
    second_rows = jnp.transpose(short[:, :, 2 * chan_col :], (0, 2, 1))
    outer, inner = split_length(2 * length)
    table = tables(outer, inner, 2 * length)
    cycles = channel_filters(
        length, row_index, chan_row, filter_embed, filter_freq, filter_proj, filter_decay
    )
    spectra = [forward_real(cycle, table) for cycle in cycles]
    own_gain = lax.dynamic_slice_in_dim(skip_gain, row_index * chan_row, chan_row, 1)

    def convolve(signal, order):
        flat = signal.reshape(seq_count * chan_row, length)
        padded_signal = jnp.concatenate([flat, jnp.zeros_like(flat)], axis=1)
        sig_real, sig_imag = forward_real(padded_signal, table)
        sig_real = sig_real.reshape(seq_count, chan_row, outer, inner)
        sig_imag = sig_imag.reshape(seq_count, chan_row, outer, inner)
        filt_real, filt_imag = spectra[order]
        prod_real = sig_real * filt_real[None] - sig_imag * filt_imag[None]
        prod_imag = sig_real * filt_imag[None] + sig_imag * filt_real[None]
        result = inverse_real(
            prod_real.reshape(seq_count * chan_row, outer, inner),
            prod_imag.reshape(seq_count * chan_row, outer, inner),
            table,
        )[:, :length]
        return result.reshape(seq_count, chan_row, length) + own_gain[order][None, :, None] * signal

    value_chan, first_chan = (
        lax.all_to_all(value_rows, "row", split_axis=1, concat_axis=2, tiled=True),
        lax.all_to_all(first_rows, "row", split_axis=1, concat_axis=2, tiled=True),
    )
    inner_chan = first_chan * convolve(value_chan, 0)
    second_conv = lax.all_to_all(
        convolve(inner_chan, 1), "row", split_axis=2, concat_axis=1, tiled=True
    )
    outer_rows = (
        jnp.transpose(second_rows * second_conv, (0, 2, 1)) * jax.nn.silu(gate.astype(jnp.float32))
    ).astype(jnp.bfloat16)
    own_rows = tok_rows // lax.axis_size("col")
    flat_rows = jnp.transpose(outer_rows, (1, 0, 2)).reshape(tok_rows * seq_count, chan_col)
    summed = lax.psum_scatter(
        jnp.dot(flat_rows, w_out, preferred_element_type=jnp.float32).astype(jnp.bfloat16),
        "col",
        scatter_dimension=0,
        tiled=True,
    ).astype(jnp.float32)
    summed = jnp.transpose(summed.reshape(own_rows, seq_count, w_out.shape[1]), (1, 0, 2))
    return summed.astype(jnp.bfloat16)


LANES = 128
PACK = 16


def dft_tables(length):
    filled = length // LANES
    outer = 2 * filled
    total = outer * LANES
    half = filled + 1
    eye = np.eye(PACK)
    q, k, p = np.arange(filled), np.arange(half), np.arange(LANES)
    inside = k[1:-1]
    angle = 2.0 * np.pi * (np.outer(k, q) % outer) / outer
    first = np.concatenate([np.kron(np.cos(angle), eye), np.kron(-np.sin(angle)[inside], eye)], axis=0)
    weight = np.where((k == 0) | (k == filled), 1.0, 2.0) / total
    last = np.concatenate(
        [
            np.kron(np.cos(angle).T * weight, eye),
            np.kron((-np.sin(angle).T * weight)[:, inside], eye),
        ],
        axis=1,
    )
    turn = 2.0 * np.pi * np.outer(k, p) / total
    twist = np.stack([np.cos(turn), np.sin(turn)])[:, :, None, :]
    twist = np.broadcast_to(twist, (2, half, 8, LANES))
    angle = 2.0 * np.pi * (np.outer(p, p) % LANES) / LANES
    cos, sin = np.cos(angle), np.sin(angle)
    ahead = np.block([[cos, -sin], [sin, cos]])
    back = np.block([[cos, sin], [-sin, cos]])
    return first, last, jnp.asarray(twist.astype(np.float32)), ahead, back


def split_bf16(array):
    high = array.astype(jnp.bfloat16).astype(jnp.float32)
    middle = (array - high).astype(jnp.bfloat16).astype(jnp.float32)
    low = (array - high - middle).astype(jnp.bfloat16).astype(jnp.float32)
    return high, middle, low


def host_split(array):
    low_type = jnp.bfloat16.dtype
    high = array.astype(low_type).astype(np.float64)
    middle = (array - high).astype(low_type).astype(np.float64)
    low = (array - high - middle).astype(low_type).astype(np.float64)
    return high, middle, low


def flip(value, bits):
    bit = 1
    while bit <= bits:
        if bits & bit:
            value = value + bit - 2 * bit * lax.rem(lax.div(value, bit), 2)
        bit *= 2
    return value


def mixer_kernel(
    rows, cols, width, emb,
    tokens_hbm, w_value_hbm, w_first_hbm, w_second_hbm, w_gate_hbm, w_out_hbm, conv_hbm, embed_hbm, freq_hbm,
    proj_hbm, decay_hbm, gain_hbm, features_hbm, tables_hbm, twist_hbm,
    out_ref,
    tokens_ref, w_refs, conv_ref, embed_ref, freq_ref, fproj_ref, decay_ref, gain_ref, features_ref, tables_ref,
    twist_ref,
    send, recv, spectra, taps_ref, stack_ref, coef_ref, gated, edge_out, edge_in, back_send, back_in, outer_send, outer_in, weights, total,
    load_sem, row_send, row_recv, edge_send, edge_recv, piece_send, piece_recv, outer_sem,
    wide_send, wide_recv, level_send, level_recv, pass_send, pass_recv, mate_send, mate_recv, told,
):
    my_row = lax.axis_index("row")
    my_col = lax.axis_index("col")
    mesh_id = pl.DeviceIdType.MESH
    groups = recv.shape[2]
    chans = groups * PACK
    tok_rows = tokens_ref.shape[0]
    block_q = tok_rows // LANES
    length_q = rows * block_q
    length = tok_rows * rows
    half = length_q + 1
    hid = freq_ref.shape[1]
    depth = weights.shape[4]
    f32, low = jnp.float32, jnp.bfloat16

    def remote(src, dst, send_sem, recv_sem, row, col):
        return pltpu.make_async_remote_copy(
            src_ref=src, dst_ref=dst, send_sem=send_sem, recv_sem=recv_sem,
            device_id=(row, col), device_id_type=mesh_id,
        )

    side = lax.rem(my_row, 2)
    mate = flip(my_row, 1)
    low_row = my_row - side
    barrier = pltpu.get_barrier_semaphore()

    def greet(row, col):
        pl.semaphore_signal(barrier, inc=1, device_id=(row, col), device_id_type=mesh_id)

    near = (1, 2)
    greet(mate, my_col)
    for d in near:
        greet(low_row, flip(my_col, d))
    for d in range(1, rows // 2):
        greet(flip(low_row, 2 * d) + 1, my_col)

    def heard(own_side):
        others = 2 * len(near) + 1 if own_side == 0 else rows - 1

        @pl.when(side == own_side)
        def _():
            pl.semaphore_wait(barrier, others)
            pl.semaphore_signal(told, inc=1, device_id=(mate, my_col), device_id_type=mesh_id)

        @pl.when(side != own_side)
        def _():
            pl.semaphore_wait(told, 1)

    def await_bytes(ref, sem):
        pltpu.make_async_copy(ref, ref, sem).wait()

    token_sem, weight_sem, half_sem = load_sem.at[0], load_sem.at[1], load_sem.at[2]
    half_rows = lambda half: pl.ds(half * (rows // 2), rows // 2)
    own_rows = pltpu.make_async_copy(w_out_hbm.at[half_rows(side)], weights.at[0, half_rows(side)], half_sem)
    own_rows.start()
    pltpu.make_async_copy(tokens_hbm, tokens_ref, token_sem).start()
    pltpu.make_async_copy(w_value_hbm, w_refs.at[0], token_sem).start()
    loads = {}
    for name, src, dst in (
        ("embed", embed_hbm, embed_ref.at[pl.ds(0, emb)]),
        ("freq", freq_hbm, freq_ref),
        ("conv", conv_hbm, conv_ref),
        ("gain", gain_hbm, gain_ref),
        ("decay", decay_hbm, decay_ref),
        ("fproj", proj_hbm, fproj_ref),
        ("features", features_hbm, features_ref),
        ("tables", tables_hbm, tables_ref),
        ("twist", twist_hbm, twist_ref),
        ("w_out", w_out_hbm.at[half_rows(1 - side)], weights.at[0, half_rows(1 - side)]),
    ):
        loads[name] = pltpu.make_async_copy(src, dst, load_sem.at[3 + len(loads)])
    for role, w_hbm in ((2, w_second_hbm), (1, w_first_hbm), (3, w_gate_hbm)):
        pltpu.make_async_copy(w_hbm, w_refs.at[role], weight_sem).start()
    for copy in loads.values():
        copy.start()

    plane = lax.rem(lax.div(my_row, 2), 2)
    subs = rows // 2
    row_of = lambda sub: side * subs + sub

    def wide_copy(group, d, sub):
        return remote(
            weights.at[0, row_of(sub)], weights.at[d, row_of(sub)],
            wide_send, wide_recv.at[group], my_row, flip(my_col, d),
        )

    wide = {
        (d, sub): wide_copy(group, d, sub + plane if group == 0 else sub)
        for group, d, sub in ((0, 1, 0), (0, 2, 2), (1, 1, 3), (1, 2, 0), (2, 1, 2), (2, 2, 1))
    }

    def there(part, send_sem, recv_sem, row):
        return remote(part, part, send_sem, recv_sem, row, my_col)

    def level_copy(index, d, group, start, count):
        part = weights.at[d, row_of(2 * d - 2 + plane), group, pl.ds(0, PACK), pl.ds(start, count)]
        return there(part, level_send, level_recv.at[index], flip(my_row, 2))

    ahead_of = depth // 2
    early = [level_copy(0, 1, pl.ds(0, groups), 0, depth), level_copy(1, 2, pl.ds(0, 1), 0, ahead_of)]
    late = [
        level_copy(1, 2, pl.ds(0, 1), ahead_of, depth - ahead_of),
        level_copy(1, 2, pl.ds(1, groups - 1), 0, depth),
    ]

    def pass_copy(index, d, sub):
        return remote(
            weights.at[d, row_of(sub)], weights.at[3, row_of(sub)],
            pass_send, pass_recv.at[index], my_row, flip(my_col, 3 - d),
        )

    passed = {(d, sub): pass_copy(index, d, sub) for index, d, sub in ((0, 1, 3), (0, 2, 0), (1, 1, 2), (1, 2, 1))}

    def to_mate(d, sub):
        there(weights.at[d, row_of(sub)], mate_send, mate_recv.at[d // 3], mate).start()

    def chunk(count):
        return weights.at[0, pl.ds(0, count)]

    def wide_arrived(group, keys):
        await_bytes(chunk(len(keys)), wide_recv.at[group])
        for d, sub in keys:
            if (d, sub) in passed:
                passed[d, sub].start()
            to_mate(d, sub + plane if group == 0 else sub)

    far_first = sorted(range(1, rows), key=lambda d: -(d & (rows // 2)))

    def row_copies(role):
        return [
            remote(
                send.at[role, flip(my_row, d)], recv.at[role, my_row],
                row_send.at[role], row_recv.at[role], flip(my_row, d), my_col,
            )
            for d in far_first
        ]

    def project(role):
        return jnp.dot(tokens_ref[...], w_refs[role], preferred_element_type=f32)

    def project_turned(role):
        result = project(role).T
        for q in range(block_q):
            send[role, :, :, q] = (
                result[:, q * LANES : (q + 1) * LANES].reshape(rows, groups, PACK, LANES).astype(low)
            )

    value_copies, first_copies = row_copies(0), row_copies(1)

    heard(0)
    own_rows.wait()
    for copy in wide.values():
        copy.start()
    await_bytes(w_refs.at[pl.ds(0, 2)], token_sem)
    project_turned(0)
    heard(1)
    for copy in value_copies:
        copy.start()
    recv[0, my_row] = send[0, my_row]

    await_bytes(w_refs.at[pl.ds(1, 3)], weight_sem)
    project_turned(1)
    for copy in first_copies:
        copy.start()
    recv[1, my_row] = send[1, my_row]
    second = project(2).astype(low).astype(f32)
    edge_out[0] = jnp.broadcast_to(second[tok_rows - 1 :], edge_out.shape[1:])
    edge_out[1] = jnp.broadcast_to(second[:1], edge_out.shape[1:])
    def edge_copy(index, step):
        return remote(edge_out.at[index], edge_in.at[index], edge_send.at[index], edge_recv.at[index], my_row + step, my_col)

    has_above, has_below = my_row > 0, my_row < rows - 1

    @pl.when(has_below)
    def _():
        edge_copy(0, 1).start()

    @pl.when(has_above)
    def _():
        edge_copy(1, -1).start()

    gate = project(3).astype(low).astype(f32)
    loads["conv"].wait()

    loads["gain"].wait()
    loads["decay"].wait()
    stack_ref[...] = jnp.zeros_like(stack_ref)
    for j in range(3):
        stack_ref[j : j + 1] = conv_ref[j, 0:1]
        stack_ref[3 + j : 4 + j] = conv_ref[j, 1:2]
    stack_ref[6:8] = gain_ref[...]
    stack_ref[8:10] = decay_ref[0]
    stack_ref[10:12] = decay_ref[1]
    shape = (chans, stack_ref.shape[1])
    picks = lax.broadcasted_iota(jnp.int32, shape, 1) == lax.broadcasted_iota(jnp.int32, shape, 0) + my_row * chans
    picks = jnp.where(picks, 1.0, 0.0)
    contract_last = (((1,), (1,)), ((), ()))
    own = lax.dot_general(picks, stack_ref[...], contract_last, precision=precise, preferred_element_type=f32)
    for k in range(8):
        coef_ref[k] = jnp.broadcast_to(own[:, k : k + 1], (chans, LANES)).reshape(groups, PACK, LANES)

    loads["embed"].wait()
    loads["freq"].wait()
    embed = embed_ref[...] * (freq_ref[...] * (1.0 / math.pi))
    embed = jnp.where(lax.broadcasted_iota(jnp.int32, embed.shape, 0) < emb, embed, 0.0)
    high, middle, least = split_bf16(embed)
    stacked = jnp.concatenate([high, high, middle, high, middle, least], axis=0).astype(low)
    loads["features"].wait()
    turns = lax.dot_general(stacked, features_ref[...], (((0,), (0,)), ((), ())), preferred_element_type=f32)
    whole = jnp.floor(turns + 0.5)
    rest = turns - whole
    sign = 1.0 - 2.0 * (whole - 2.0 * jnp.floor(whole * 0.5))
    square = rest * rest
    series = jnp.full_like(square, -(math.pi**11) / math.factorial(11))
    for n in (9, 7, 5, 3, 1):
        series = series * square + (-1) ** (n // 2) * math.pi**n / math.factorial(n)
    hidden = (series * (rest * sign)).astype(low)
    loads["fproj"].wait()
    pieces = []
    picks_low = picks.astype(low)
    halves = 2
    for od in range(4):
        parts = [
            fproj_ref[pl.ds((od // 2) * 2 * halves + j * 2 + od % 2, hid, stride=4 * halves), :]
            for j in range(halves)
        ]
        block = jnp.concatenate(parts, axis=1).astype(low)
        pieces.append(lax.dot_general(picks_low, block, contract_last, preferred_element_type=f32).astype(low))
    taps = jnp.dot(jnp.concatenate(pieces, axis=0), hidden, preferred_element_type=f32)
    lag = lax.broadcasted_iota(jnp.int32, (1, length), 1)
    spot = lag.astype(f32) / (length - 1)
    for od in range(4):
        block = taps[od * chans : (od + 1) * chans] * jnp.exp(-own[:, 8 + od : 9 + od] * spot)
        if od % 2 == 1:
            block = jnp.where(lag == 0, 0.0, block)
        taps_ref[od] = block.astype(low)

    size = LANES * groups
    first_ref, last_ref, ahead_ref, back_ref = (
        tables_ref.at[pl.ds(start * size, count * size)]
        for start, count in ((0, 2), (2, 2), (4, 1), (5, 1))
    )

    def wide_twist(index):
        return twist_ref[index].reshape(half, 1, 8, LANES)

    def ahead(signal):
        mid = jnp.dot(first_ref[...], signal, preferred_element_type=f32)
        blank = jnp.zeros((PACK, LANES), f32)
        blocks = []
        for g in range(groups):
            lanes = slice(g * LANES, (g + 1) * LANES)
            real = mid[: half * PACK, lanes].reshape(half, 2, 8, LANES)
            imag = jnp.concatenate([blank, mid[half * PACK :, lanes], blank], axis=0).reshape(half, 2, 8, LANES)
            cos, sin = wide_twist(0), wide_twist(1)
            blocks.append(
                jnp.concatenate(
                    [
                        (real * cos + imag * sin).reshape(half * PACK, LANES),
                        (imag * cos - real * sin).reshape(half * PACK, LANES),
                    ],
                    axis=1,
                ).astype(low)
            )
        return jnp.dot(jnp.concatenate(blocks, axis=0), ahead_ref[...], preferred_element_type=f32)

    def convolve(signal, order):
        spec = ahead(signal.astype(low))
        real, imag = spec[:, :LANES], spec[:, LANES:]
        filt_real, filt_imag = spectra[order, 0], spectra[order, 1]
        prod = jnp.concatenate(
            [real * filt_real - imag * filt_imag, real * filt_imag + imag * filt_real], axis=1
        ).astype(low)
        mid = jnp.dot(prod, back_ref[...], preferred_element_type=f32)
        blocks = []
        for g in range(groups):
            span = slice(g * half * PACK, (g + 1) * half * PACK)
            real = mid[span, :LANES].reshape(half, 2, 8, LANES)
            imag = mid[span, LANES:].reshape(half, 2, 8, LANES)
            cos, sin = wide_twist(0), wide_twist(1)
            turned_real = (real * cos - imag * sin).reshape(half * PACK, LANES)
            turned_imag = (real * sin + imag * cos)[1:-1].reshape((half - 2) * PACK, LANES)
            blocks.append(jnp.concatenate([turned_real, turned_imag], axis=0).astype(low))
        last = jnp.concatenate([last_ref[:size], last_ref[size:]], axis=1)
        result = jnp.dot(last, jnp.concatenate(blocks, axis=1), preferred_element_type=f32)
        gain = jnp.concatenate([coef_ref[6 + order, g] for g in range(groups)], axis=1)
        shape = (length_q, PACK, groups * LANES)
        return (result.reshape(shape) + gain[None] * signal.reshape(shape)).reshape(signal.shape)

    loads["tables"].wait()
    loads["twist"].wait()
    for order in range(2):
        for direction in range(2):
            od = 2 * order + direction
            signal = jnp.concatenate(
                [
                    jnp.concatenate(
                        [
                            taps_ref[od, g * PACK : (g + 1) * PACK, q * LANES : (q + 1) * LANES]
                            for q in range(length_q)
                        ],
                        axis=0,
                    )
                    for g in range(groups)
                ],
                axis=1,
            )
            spec = ahead(signal)
            if direction == 0:
                spectra[order, 0] = spec[:, :LANES]
                spectra[order, 1] = spec[:, LANES:]
            else:
                spectra[order, 0] += spec[:, :LANES]
                spectra[order, 1] -= spec[:, LANES:]

    wide_arrived(0, ((1, 0), (2, 2)))
    for copy in early:
        copy.start()

    def short(role):
        blocks = []
        for g in range(groups):
            here = recv[role, :, g].reshape(length_q * PACK, LANES).astype(f32)
            size = here.shape[0]
            lane = lax.broadcasted_iota(jnp.int32, here.shape, 1)
            blank = jnp.zeros((PACK, LANES), f32)
            before = pltpu.roll(here, 1, 1)
            before = jnp.where(lane == 0, jnp.concatenate([blank, before[: size - PACK]], axis=0), before)
            after = pltpu.roll(here, LANES - 1, 1)
            after = jnp.where(lane == LANES - 1, jnp.concatenate([after[PACK:], blank], axis=0), after)
            shape = (length_q, PACK, LANES)
            w = lambda j: coef_ref[3 * role + j, g][None]
            result = before.reshape(shape) * w(0) + here.reshape(shape) * w(1) + after.reshape(shape) * w(2)
            blocks.append(result.reshape(size, LANES))
        return jnp.concatenate(blocks, axis=1)

    others = pl.ds(0, rows - 1)
    await_bytes(recv.at[0, others], row_recv.at[0])
    conv = convolve(short(0), 0)

    wide_arrived(1, ((1, 3), (2, 0)))
    await_bytes(recv.at[1, others], row_recv.at[1])
    conv = convolve(short(1) * conv, 1)

    for g in range(groups):
        back_send[:, :, g] = (
            conv[:, g * LANES : (g + 1) * LANES].reshape(rows, block_q, PACK, LANES).astype(low)
        )
    for d in far_first:
        peer = flip(my_row, d)
        remote(back_send.at[peer], back_in.at[my_row], piece_send, piece_recv.at[2 * d // rows], peer, my_col).start()
    for copy in late:
        copy.start()
    back_in[my_row] = back_send[my_row]

    wide_arrived(2, ((1, 2), (2, 1)))


    @pl.when(has_above)
    def _():
        await_bytes(edge_in.at[0], edge_recv.at[0])

    @pl.when(has_below)
    def _():
        await_bytes(edge_in.at[1], edge_recv.at[1])

    line = lax.broadcasted_iota(jnp.int32, second.shape, 0)
    above = jnp.where(has_above, edge_in[0, 0:1], 0.0)
    below = jnp.where(has_below, edge_in[1, 0:1], 0.0)
    before = jnp.where(line == 0, above, pltpu.roll(second, 1, 0))
    after = jnp.where(line == tok_rows - 1, below, pltpu.roll(second, tok_rows - 1, 0))
    short_second = before * conv_ref[0, 2:3] + second * conv_ref[1, 2:3] + after * conv_ref[2, 2:3]
    both = short_second * (gate / (1.0 + jnp.exp(-gate)))
    for tile in range(halves):
        gated[tile] = both[:, tile * LANES : (tile + 1) * LANES]


    per_tile = rows // halves
    near_tile = lax.div(my_row, per_tile)

    def finish(tile, far):
        count = per_tile if far else per_tile - 1
        await_bytes(back_in.at[pl.ds(0, count)], piece_recv.at[far])
        for q in range(block_q):
            block = back_in[pl.ds(tile * per_tile, per_tile), q].reshape(LANES, LANES).astype(f32).T
            block = (block * gated[tile, q * LANES : (q + 1) * LANES]).astype(low)
            spots = LANES // width
            outer_send[far, q * spots : (q + 1) * spots] = block.reshape(spots, width, LANES)
        for d in (3, 1, 2):
            peer = flip(my_col, d)
            remote(
                outer_send.at[far, peer], outer_in.at[far, d], outer_sem.at[0], outer_sem.at[1 + far], my_row, peer
            ).start()
        outer_in[far, 0] = outer_send[far, my_col]

    def share(tile, far):
        await_bytes(outer_in.at[far, pl.ds(1, cols - 1)], outer_sem.at[1 + far])
        left = jnp.concatenate([outer_in[far, d] for d in range(cols)], axis=1)
        right = jnp.concatenate(
            [weights[d, pl.ds(tile * per_tile, per_tile)].reshape(LANES, depth) for d in range(cols)], axis=0
        )
        return jnp.dot(left, right, preferred_element_type=f32)

    finish(near_tile, 0)
    await_bytes(chunk(2), pass_recv.at[0])
    to_mate(3, 0)
    to_mate(3, 3)
    await_bytes(chunk(1), level_recv.at[0])
    to_mate(1, 1 - plane)
    finish(1 - near_tile, 1)
    await_bytes(chunk(2), pass_recv.at[1])
    to_mate(3, 2)
    to_mate(3, 1)
    await_bytes(chunk(1), level_recv.at[1])
    to_mate(2, 3 - plane)

    loads["w_out"].wait()
    await_bytes(weights.at[0], mate_recv.at[0])
    await_bytes(chunk(subs), mate_recv.at[1])
    total[...] = share(near_tile, 0)
    out_ref[...] = (total[...] + share(1 - near_tile, 1)).astype(low)

    for role in range(2):
        await_bytes(send.at[role, others], row_send.at[role])

    @pl.when(has_below)
    def _():
        await_bytes(edge_out.at[0], edge_send.at[0])

    @pl.when(has_above)
    def _():
        await_bytes(edge_out.at[1], edge_send.at[1])

    await_bytes(back_send.at[others], piece_send)
    await_bytes(outer_send.at[pl.ds(0, 2), pl.ds(0, cols - 1)], outer_sem.at[0])
    await_bytes(chunk(6), wide_send)
    await_bytes(chunk(2), level_send)
    await_bytes(chunk(4), pass_send)
    await_bytes(weights.at[pl.ds(0, 3), pl.ds(0, 4)], mate_send)


def fast_body(
    tokens, w_value, w_first, w_second, w_gate, conv_taps, filter_embed, filter_freq, filter_proj,
    filter_decay, skip_gain, w_out,
):
    rows, cols = lax.axis_size("row"), lax.axis_size("col")
    tok_rows = tokens.shape[1]
    chan_col = w_value.shape[1]
    chans = chan_col // rows
    groups = chans // PACK
    length = tok_rows * rows
    block_q = tok_rows // LANES
    length_q = length // LANES
    width = tok_rows // cols
    depth = w_out.shape[1]
    emb, hid = filter_embed.shape
    half = length_q + 1

    flat = tokens.reshape(tok_rows, tokens.shape[2])
    bands = (emb - 1) // 2
    index = np.arange(length)
    spot = index.astype(np.float32) / np.float32(length - 1)
    phase = 2.0 * np.pi * (np.outer(np.arange(1, bands + 1), index) % length) / length
    features = np.concatenate([spot[None, :], np.cos(phase), np.sin(phase)])
    emb_pad = -(-emb // 8) * 8
    features = np.concatenate([features, np.zeros((emb_pad - emb, length))]).astype(np.float32).astype(np.float64)
    high, middle, least = host_split(features)
    features = np.concatenate([high, middle, high, least, middle, high]).astype(jnp.bfloat16.dtype)
    lanes = chan_col // LANES
    fproj = filter_proj.reshape(hid, 2, 2, lanes, LANES).transpose(0, 1, 3, 2, 4).reshape(hid * 4 * lanes, LANES)
    w_rows = w_out.reshape(rows, groups, PACK, depth)

    first, last, twist, ahead, back = dft_tables(length)
    size = groups * LANES
    tables = jnp.asarray(
        np.concatenate([first, last[:, :size], last[:, size:], ahead, back]).astype(np.float32)
    ).astype(jnp.bfloat16)
    operands = (
        flat, w_value, w_first, w_second, w_gate, w_rows, conv_taps, filter_embed, filter_freq.reshape(1, hid),
        fproj, filter_decay, skip_gain, jnp.asarray(features), tables, twist,
    )
    dma = pltpu.SemaphoreType.DMA
    f32, low = jnp.float32, jnp.bfloat16
    like = lambda array: pltpu.VMEM(array.shape, array.dtype)
    mixed = pl.pallas_call(
        functools.partial(mixer_kernel, rows, cols, width, emb),
        out_shape=pltpu.VMEM((width, depth), low),
        in_specs=[pl.BlockSpec(memory_space=pl.ANY)] * len(operands),
        out_specs=pl.BlockSpec(memory_space=pltpu.VMEM),
        scratch_shapes=[
            like(flat),
            pltpu.VMEM((4,) + w_value.shape, low),
            like(conv_taps),
            pltpu.VMEM((emb_pad, hid), f32),
            pltpu.VMEM((1, hid), f32),
            like(fproj),
            like(filter_decay),
            like(skip_gain),
            pltpu.VMEM(features.shape, low),
            like(tables),
            like(twist),
            pltpu.VMEM((2, rows, groups, block_q, PACK, LANES), low),
            pltpu.VMEM((2, rows, groups, block_q, PACK, LANES), low),
            pltpu.VMEM((2, 2, groups * half * PACK, LANES), f32),
            pltpu.VMEM((4, chans, length), low),
            pltpu.VMEM((16, chan_col), f32),
            pltpu.VMEM((8, groups, PACK, LANES), f32),
            pltpu.VMEM((lanes, tok_rows, LANES), f32),
            pltpu.VMEM((2, 8, chan_col), f32),
            pltpu.VMEM((2, 8, chan_col), f32),
            pltpu.VMEM((rows, block_q, groups, PACK, LANES), low),
            pltpu.VMEM((rows, block_q, groups, PACK, LANES), low),
            pltpu.VMEM((2, cols, width, LANES), low),
            pltpu.VMEM((2, cols, width, LANES), low),
            pltpu.VMEM((cols, rows, groups, PACK, depth), low),
            pltpu.VMEM((width, depth), f32),
            dma((len(operands) - 2,)),
            dma((2,)),
            dma((2,)),
            dma((2,)),
            dma((2,)),
            dma,
            dma((2,)),
            dma((3,)),
            dma,
            dma((3,)),
            dma,
            dma((2,)),
            dma,
            dma((2,)),
            dma,
            dma((2,)),
            pltpu.SemaphoreType.REGULAR,
        ],
        compiler_params=pltpu.CompilerParams(
            collective_id=0, has_side_effects=True, vmem_limit_bytes=40 * 1024 * 1024
        ),
        cost_estimate=pl.CostEstimate(flops=12_000_000_000, bytes_accessed=8_000_000, transcendentals=0),
    )(*[pltpu.with_memory_space_constraint(array, pltpu.HBM) for array in operands])
    return mixed[None]


def shaped_body(tokens, w_value, *rest):
    rows, cols = lax.axis_size("row"), lax.axis_size("col")
    seqs, tok_rows = tokens.shape[:2]
    chan_col = w_value.shape[1]
    chans = chan_col // rows
    width = tok_rows // cols
    fits = (
        seqs == 1
        and cols == 4
        and rows == 8
        and chans == 2 * PACK
        and tok_rows % LANES == 0
        and LANES == 2 * width
        and chan_col == 2 * LANES
        and rows * PACK == LANES
    )
    return (fast_body if fits else body)(tokens, w_value, *rest)


def solution(mesh):
    in_specs = (
        P(None, "row", None),
        P(None, "col"),
        P(None, "col"),
        P(None, "col"),
        P(None, "col"),
        P(None, None, "col"),
        P(),
        P(),
        P(None, None, None, "col"),
        P(None, None, "col"),
        P(None, "col"),
        P("col", None),
    )
    out_specs = P(None, ("row", "col"), None)
    return jax.shard_map(shaped_body, mesh=mesh, in_specs=in_specs, out_specs=out_specs, check_vma=False)
```
